32 devices in a mesh: sp: 8 (over z, y), tp: 4 (over x, core).
Axes of the slice: x: 2, y: 2, z: 4, core: 2. Of those that a mesh axis runs over, the one named last changes fastest.
Arguments:
- skip_stream_vector: bfloat16 [8192, 2048], P(('sp', 'tp')), may hold values from -6 to 6
- probe_preactivation: bfloat16 [8192, 1024], P('sp', 'tp'), may hold values from -6 to 6
- retention_preactivation: bfloat16 [8192, 1024], P('sp', 'tp'), may hold values from -4.5 to 4.5
- content_vector: bfloat16 [8192, 1024], P('sp', 'tp'), may hold values from -6 to 6
- emission_preactivation: bfloat16 [8192, 1024], P('sp', 'tp'), may hold values from -6 to 6
- retention_slack: float32 [1024], P('tp'), may hold values from 0 to 0.12
- surge_rate: float32 [8192, 1024], P('sp', 'tp'), may hold values from -1.2 to 0
- subspace_scaling_factor: float32 [1024], P('tp'), may hold values from 0.1 to 1.9
- emission_matrix: bfloat16 [1024, 2048], replicated, may hold values from -0.1875 to 0.1875
- mlp_scaling_factor: float32 [2048], replicated, may hold values from 0.1 to 1.9
- switch_matrix: bfloat16 [2048, 5632], P('sp', 'tp'), may hold values from -0.125 to 0.125
- expansion_matrix: bfloat16 [2048, 5632], P('sp', 'tp'), may hold values from -0.125 to 0.125
- contraction_matrix: bfloat16 [5632, 2048], P('tp', 'sp'), may hold values from -0.078125 to 0.078125
Outputs:
- stream_out: bfloat16 [8192, 2048], P(('sp', 'tp'))
The draws below stay inside these ranges and needn't reach their ends.
All inputs are finite; a program needn't handle non-finite values.
Results may differ from the reference program's by a relative error of at most 0.017.
Values may be sent and summed in bfloat16 or wider, within the bound.
A program may use at most 128 MiB of HBM per device.

```python
import jax
import jax.numpy as jnp
from jax import lax

D = 2048
HEADS = 8
HEAD_DIM = 128
FF = 5632
BLOCK = 64
TOK_DEV = 1024
D_HGRN = 1024
TOKENS = 8192
N_TP = 4


def draw_retention_slack(key, part):
    first_key, second_key, third_key = jax.random.split(jax.random.fold_in(key, 11), 3)
    ranking = jax.random.permutation(first_key, HEADS)
    slow_heads = ranking < HEADS // 2
    slow_gap = jnp.exp(jax.random.uniform(second_key, (HEADS, HEAD_DIM), jnp.float32, jnp.log(0.2), jnp.log(0.8))) / TOKENS
    fast_gap = jnp.exp(jax.random.uniform(third_key, (HEADS, HEAD_DIM), jnp.float32, jnp.log(0.04), jnp.log(0.12)))
    chosen = jnp.where(slow_heads[:, None], slow_gap, fast_gap)
    return jnp.minimum(chosen, 0.12).reshape(HEADS * HEAD_DIM)


def draw_retention_preactivation(key, part):
    first_key, second_key = jax.random.split(jax.random.fold_in(key, 21))
    noise = jnp.clip(0.8 * jax.random.normal(first_key, (TOKENS, HEADS * HEAD_DIM), jnp.float32), -3.0, 3.0)
    offsets = jax.random.uniform(second_key, (TOKENS // TOK_DEV, HEADS), jnp.float32, -1.2, 1.2)
    spread_rows = jnp.repeat(jnp.repeat(offsets, TOK_DEV, axis=0), HEAD_DIM, axis=1)
    return (noise + spread_rows).astype(jnp.bfloat16)


def draw_surge_rate(key, part):
    first_key, second_key = jax.random.split(jax.random.fold_in(key, 31))
    positions = jax.random.randint(first_key, (2, HEADS), 0, TOKENS)
    strength = jnp.log(jax.random.uniform(second_key, (2, HEADS), jnp.float32, 0.55, 0.8))
    places = jnp.arange(TOKENS, dtype=jnp.int32)[:, None, None]
    hits = jnp.sum(jnp.where(places == positions[None, :, :], strength[None, :, :], 0.0), axis=1)
    return jnp.repeat(hits, HEAD_DIM, axis=1)


def levels(rng, shape, pieces, low, largest):
    loudness, own = 1.0, jax.random.fold_in(rng, 6)
    for position, shards_of in pieces:
        draws = jnp.exp(jax.random.uniform(jax.random.fold_in(own, position), (shards_of,), jnp.float32, low / len(pieces), largest / len(pieces)))
        loudness = loudness * jnp.repeat(draws, shape[position] // shards_of).reshape([-1 if axis == position else 1 for axis in range(len(shape))])
    return loudness


def normal_values(own_key, extent, width, limit, shards=(), kind=jnp.bfloat16):
    drawn = width * jax.random.normal(own_key, extent, jnp.float32)
    if shards:
        drawn = drawn * levels(own_key, extent, shards, -0.22, 0.18)
    return jnp.clip(drawn, -limit, limit).astype(kind)


def setup_inputs(seed: int = 0) -> dict:
    key_of = jax.random.split(jax.random.key(seed), 14)
    return {
        "skip_stream_vector": normal_values(key_of[0], (TOKENS, D), 1.0, 6.0, ((0, 32),)),
        "probe_preactivation": normal_values(key_of[1], (TOKENS, D_HGRN), 1.0, 6.0, ((0, 8), (1, 4))),
        "retention_preactivation": draw_retention_preactivation(jax.random.fold_in(key_of[13], 71), 0),
        "content_vector": normal_values(key_of[3], (TOKENS, D_HGRN), 1.0, 6.0, ((0, 8), (1, 4))),
        "emission_preactivation": normal_values(key_of[4], (TOKENS, D_HGRN), 1.0, 6.0, ((0, 8), (1, 4))),
        "retention_slack": draw_retention_slack(jax.random.fold_in(key_of[13], 71), 0),
        "surge_rate": draw_surge_rate(jax.random.fold_in(key_of[13], 71), 0),
        "subspace_scaling_factor": jnp.clip(1.0 + 0.18 * jax.random.normal(key_of[7], (D_HGRN,), jnp.float32), 0.1, 1.9),
        "emission_matrix": normal_values(key_of[8], (D_HGRN, D), D_HGRN ** -0.5, 0.1875),
        "mlp_scaling_factor": jnp.clip(1.0 + 0.18 * jax.random.normal(key_of[9], (D,), jnp.float32), 0.1, 1.9),
        "switch_matrix": normal_values(key_of[10], (D, FF), D ** -0.5, 0.125, ((0, 8), (1, 4))),
        "expansion_matrix": normal_values(key_of[11], (D, FF), D ** -0.5, 0.125, ((0, 8), (1, 4))),
        "contraction_matrix": normal_values(key_of[12], (FF, D), FF ** -0.5, 0.078125, ((0, 4), (1, 8))),
    }


EPSILON = 1e-06
TOP_PRECISION = lax.Precision.HIGHEST

def block_step(carry, inputs):
    memory_state, offsets = carry
    query_block, input_gate_block, value_block, log_blk = inputs
    cumulative_decay = jnp.cumsum(log_blk, axis=1)
    length = log_blk.shape[1]
    carried_share = jnp.einsum('eia,eax->eix', query_block * jnp.exp(cumulative_decay), memory_state, precision=TOP_PRECISION)
    middle = cumulative_decay[:, length // 2, :][:, None, :]
    left_side = query_block * jnp.exp(cumulative_decay - middle)
    right_side = input_gate_block * jnp.exp(middle - cumulative_decay)
    causal = (jnp.arange(length)[:, None] >= jnp.arange(length)[None, :])[None, :, :]
    scores = jnp.einsum('htk,hsk->hts', left_side, right_side, precision=TOP_PRECISION)
    scores = jnp.where(causal, scores, 0.0)
    outputs = carried_share + jnp.einsum('hts,hsv->htv', scores, value_block, precision=TOP_PRECISION)
    closing_log_decay = cumulative_decay[:, -1, :]
    updated_memory_state = jnp.exp(closing_log_decay)[:, :, None] * memory_state + jnp.einsum('qnj,qnl->qjl', input_gate_block * jnp.exp(closing_log_decay[:, None, :] - cumulative_decay), value_block, precision=TOP_PRECISION)
    return ((updated_memory_state, offsets + closing_log_decay), (outputs, cumulative_decay + offsets[:, None, :]))

def split_blocks(values, heads_here):
    count = values.shape[0]
    return values.reshape(count // BLOCK, BLOCK, heads_here, HEAD_DIM).transpose(0, 2, 1, 3)

def admission_source_matrix(probe_preactivation, retention_preactivation, content_vector, retention_slack, surge_rate):
    query_act = jax.nn.silu(probe_preactivation.astype(jnp.float32))
    admission_factor = retention_slack[None, :] * jax.nn.sigmoid(-retention_preactivation.astype(jnp.float32))
    retention_logarithm = jnp.log1p(-admission_factor) + surge_rate
    return (query_act, admission_factor, content_vector.astype(jnp.float32), retention_logarithm)

def head_output(outputs, subspace_scaling_factor, emission_preactivation):
    count, heads_here = (outputs.shape[0], outputs.shape[1])
    squares = lax.optimization_barrier(jnp.mean(outputs * outputs, axis=-1, keepdims=True))
    scaled = outputs * lax.rsqrt(squares + EPSILON) * subspace_scaling_factor.reshape(heads_here, HEAD_DIM)
    scaled = scaled.reshape(count, heads_here * HEAD_DIM)
    return (scaled * jax.nn.silu(emission_preactivation.astype(jnp.float32))).astype(jnp.bfloat16)

def row_norm(stream, mlp_scaling_factor):
    streamf = stream.astype(jnp.float32)
    squares = lax.optimization_barrier(jnp.mean(streamf * streamf, axis=-1, keepdims=True))
    return (streamf * lax.rsqrt(squares + EPSILON) * mlp_scaling_factor).astype(jnp.bfloat16)

def reference(skip_stream_vector, probe_preactivation, retention_preactivation, content_vector, emission_preactivation, retention_slack, surge_rate, subspace_scaling_factor, emission_matrix, mlp_scaling_factor, switch_matrix, expansion_matrix, contraction_matrix):
    arranged_sources = admission_source_matrix(probe_preactivation, retention_preactivation, content_vector, retention_slack, surge_rate)
    block_list = tuple((split_blocks(item, HEADS) for item in arranged_sources))
    start_carry = (jnp.zeros((HEADS, HEAD_DIM, HEAD_DIM), jnp.float32), jnp.zeros((HEADS, HEAD_DIM), jnp.float32))
    _, (outputs, _) = lax.scan(block_step, start_carry, block_list)
    outputs = outputs.transpose(0, 2, 1, 3).reshape(TOKENS, HEADS, HEAD_DIM)
    mixed = head_output(outputs, subspace_scaling_factor, emission_preactivation)
    projected = jnp.dot(mixed, emission_matrix, preferred_element_type=jnp.float32)
    stream = (skip_stream_vector.astype(jnp.float32) + projected).astype(jnp.bfloat16)
    normed = row_norm(stream, mlp_scaling_factor)
    gate_proj = jnp.dot(normed, switch_matrix, preferred_element_type=jnp.float32)
    up_proj = jnp.dot(normed, expansion_matrix, preferred_element_type=jnp.float32)
    hidden = (jax.nn.silu(gate_proj) * up_proj).astype(jnp.bfloat16)
    slice_width = FF // N_TP
    summed = jnp.zeros((TOKENS, D), jnp.float32)
    for member in range(N_TP):
        lower = member * slice_width
        partial_sum = jnp.dot(hidden[:, lower:lower + slice_width], contraction_matrix[lower:lower + slice_width], preferred_element_type=jnp.float32)
        summed = summed + partial_sum.astype(jnp.bfloat16).astype(jnp.float32)
    return (stream.astype(jnp.float32) + summed).astype(jnp.bfloat16)
```

```python
import functools

import jax
import jax.numpy as jnp
from jax import lax
from jax.experimental import pallas as pl
from jax.experimental.pallas import tpu as pltpu
from jax.sharding import PartitionSpec as P

HEAD_DIM = 128
BLOCK = 64
STATE_ROWS = HEAD_DIM + 16
EPSILON = 1e-06
MESH = pl.DeviceIdType.MESH
F32, BF16 = jnp.float32, jnp.bfloat16
LAST = (((1,), (1,)), ((), ()))
FIRST = (((0,), (0,)), ((), ()))


def weight_plan(n, me):
    out = []
    if n != 8:
        for tensor in range(3):
            for d in range(1, n):
                to, source = lax.rem(me + d, n), lax.rem(me + n - d, n)
                out.append((0, tensor, ("D", d, tensor), True, me, to, True, source, None))
        return out
    ny, nz = 2, n // 2
    z, y = me // ny, lax.rem(me, ny)

    def at(place, flip):
        return jnp.clip(place, 0, nz - 1) * ny + (1 - y if flip else y)

    def crossed(place, tensor, way):
        first, last = (1, nz - 1) if way > 0 else (nz - 2, 0)
        return (place == first) | (place == last) if tensor == 0 else place == first

    def inside(place):
        return (place >= 0) & (place < nz)

    for tensor in range(3):
        late = 1 if tensor == 2 else 0
        out.append((0, tensor, ("Y", 0, tensor), True, me, at(z, 1), True, at(z, 1), None))
        for way in (1, -1):
            for k in range(1, nz):
                to, unit = z + way, z + way - way * k
                name, above = (way, k, tensor), (way, k - 1, tensor)
                stage = 0 if k == 1 else k - 1 + late
                out.append(
                    (stage, tensor, name, inside(to) & inside(unit), at(unit, 0), at(to, 0),
                     inside(z - way * k), at(z - way * k, 0), None if k == 1 else above)
                )
                held = inside(z - way * k)
                if k == 1:
                    held = held & jnp.logical_not(crossed(z, tensor, way))
                out.append(
                    (k + late, tensor, ("Y", way * k, tensor), held, at(z - way * k, 0), at(z, 1),
                     held, at(z - way * k, 1), name)
                )
            out.append(
                (2, tensor, ("X", way, tensor), inside(z + way) & crossed(z + way, tensor, way), at(z, 1),
                 at(z + way, 0), crossed(z, tensor, way), at(z - way, 1), ("Y", 0, tensor))
            )
    return out


def kernel(
    n,
    m,
    skip_ref,
    query_ref,
    forget_ref,
    value_ref,
    emission_ref,
    slack_ref,
    surge_ref,
    gain_ref,
    projection_ref,
    row_gain_ref,
    switch_ref,
    expansion_ref,
    contraction_ref,
    out_ref,
    switch_all,
    expansion_all,
    contraction_all,
    projection,
    stream,
    normed,
    hidden,
    mixed,
    outputs,
    decayed_query,
    state,
    offset,
    state_out,
    state_in,
    part,
    from_buddy,
    cross_out,
    cross_in,
    local_sem,
    weight_send,
    weight_recv,
    skip_send,
    skip_recv,
    mixed_send,
    mixed_recv,
    state_send,
    state_recv,
    buddy_send,
    buddy_recv,
    cross_send,
    cross_recv,
):
    sp, tp = lax.axis_index("sp"), lax.axis_index("tp")
    tokens, width = query_ref.shape
    rows, model = skip_ref.shape
    depth, units = switch_ref.shape
    heads = width // HEAD_DIM
    pairs = m // 2

    barrier = pltpu.get_barrier_semaphore()
    for d in range(1, n):
        pl.semaphore_signal(barrier, inc=1, device_id=(lax.rem(sp + d, n), tp), device_id_type=MESH)
    for d in range(1, m):
        pl.semaphore_signal(barrier, inc=1, device_id=(sp, lax.rem(tp + d, m)), device_id_type=MESH)
    pl.semaphore_wait(barrier, n - 1 + m - 1)

    def remote(src, dst, send, recv, device):
        return pltpu.make_async_remote_copy(
            src_ref=src, dst_ref=dst, send_sem=send, recv_sem=recv, device_id=device, device_id_type=MESH
        )

    own_units = (switch_ref, expansion_ref, contraction_ref)

    def unit(tensor, owner):
        if tensor == 2:
            return contraction_all.at[owner]
        held = (switch_all, expansion_all)[tensor]
        return held.at[pl.ds(pl.multiple_of(owner * depth, depth), depth)]

    messages = {}
    for index, (stage, tensor, name, sent, owner, target, arrives, arriving, after) in enumerate(
        weight_plan(n, sp)
    ):
        src = own_units[tensor] if stage == 0 else unit(tensor, owner)
        args = (weight_send.at[index], weight_recv.at[index], (target, tp))
        send = remote(src, unit(tensor, owner), *args)
        arrival = remote(unit(tensor, arriving), unit(tensor, arriving), *args)
        messages[name] = (stage, sent, send, arrives, arrival, after)
    arrived = set()

    def where(condition, action):
        if condition is True:
            action()
        else:
            pl.when(condition)(action)

    def await_unit(name):
        if name not in arrived:
            arrived.add(name)
            where(messages[name][3], messages[name][4].wait_recv)

    def run_stage(wanted):
        for name, (stage, sent, send, _, _, after) in messages.items():
            if stage == wanted:
                if after is not None:
                    await_unit(after)
                where(sent, send.start)

    run_stage(0)

    def rows_of(owner):
        return pl.ds(pl.multiple_of(owner * rows, rows), rows)

    skip_sends, skip_arrivals, mixed_sends, mixed_arrivals = [], [], [], []
    for d in range(1, m):
        source, target = lax.rem(tp + m - d, m), (sp, lax.rem(tp + d, m))
        sems = (skip_send.at[d - 1], skip_recv.at[d - 1], target)
        skip_sends.append(remote(skip_ref, stream.at[rows_of(tp)], *sems))
        skip_arrivals.append(remote(stream.at[rows_of(source)], stream.at[rows_of(source)], *sems))
        sems = (mixed_send.at[d - 1], mixed_recv.at[d - 1], target)
        mixed_sends.append(remote(mixed.at[tp], mixed.at[tp], *sems))
        mixed_arrivals.append(remote(mixed.at[source], mixed.at[source], *sems))
    for copy in skip_sends:
        copy.start()
    local = [
        pltpu.make_async_copy(skip_ref, stream.at[rows_of(tp)], local_sem.at[0]),
        pltpu.make_async_copy(projection_ref, projection, local_sem.at[1]),
    ] + [pltpu.make_async_copy(own_units[t], unit(t, sp), local_sem.at[2 + t]) for t in range(3)]
    for copy in local:
        copy.start()

    state[...] = jnp.zeros_like(state)
    offset[...] = jnp.zeros_like(offset)
    before = lax.broadcasted_iota(jnp.int32, (BLOCK, BLOCK), 0) >= lax.broadcasted_iota(
        jnp.int32, (BLOCK, BLOCK), 1
    )
    lower = before.astype(F32)

    @pl.loop(0, tokens // BLOCK)
    def _(block):
        here = pl.ds(pl.multiple_of(block * BLOCK, BLOCK), BLOCK)
        raw = query_ref[here, :].astype(F32)
        query = raw * jax.nn.sigmoid(raw)
        gate = slack_ref[...] * jax.nn.sigmoid(-forget_ref[here, :].astype(F32))
        log_forget = jnp.log1p(-gate) + surge_ref[here, :]
        total = jnp.dot(lower, log_forget, precision=lax.Precision.HIGHEST, preferred_element_type=F32)
        middle, last = total[BLOCK // 2 : BLOCK // 2 + 1, :], total[BLOCK - 1 :, :]
        left = (query * jnp.exp(total - middle)).astype(BF16)
        right = (gate * jnp.exp(middle - total)).astype(BF16)
        carried = (query * jnp.exp(total)).astype(BF16)
        kept = (gate * jnp.exp(last - total)).astype(BF16)
        decayed_query[here, :] = (query * jnp.exp(total + offset[...])).astype(BF16)
        closing = jnp.exp(last)
        for head in range(heads):
            lanes = slice(head * HEAD_DIM, (head + 1) * HEAD_DIM)
            value = value_ref[here, lanes]
            scores = lax.dot_general(left[:, lanes], right[:, lanes], LAST, preferred_element_type=F32)
            scores = jnp.where(before, scores, 0.0).astype(BF16)
            held = state[head]
            outputs[here, lanes] = jnp.dot(
                scores, value, preferred_element_type=F32
            ) + lax.dot_general(carried[:, lanes], held.astype(BF16), LAST, preferred_element_type=F32)
            state[head] = closing[:, lanes] * held + lax.dot_general(
                value, kept[:, lanes], FIRST, preferred_element_type=F32
            )
        offset[...] += last

    for head in range(heads):
        lanes = slice(head * HEAD_DIM, (head + 1) * HEAD_DIM)
        state_out[head, :HEAD_DIM, :] = state[head].astype(BF16)
        decay = jnp.exp(offset[:, lanes])
        state_out[head, HEAD_DIM:, :] = jnp.broadcast_to(decay, (16, HEAD_DIM)).astype(BF16)
    state_copies = []
    for d in range(1, n):
        copy = remote(
            state_out,
            state_in.at[d - 1],
            state_send.at[d - 1],
            state_recv.at[d - 1],
            (lax.rem(sp + d, n), tp),
        )
        state_copies.append(copy)
        pl.when(sp + d < n)(copy.start)

    run_stage(1)

    for d in range(1, n):
        pl.when(sp >= d)(state_copies[d - 1].wait_recv)
    state[...] = jnp.zeros_like(state)

    @pl.loop(0, sp)
    def _(earlier):
        slot = sp - earlier - 1
        for head in range(heads):
            item = state_in[slot, head].astype(F32)
            state[head] = item[HEAD_DIM : HEAD_DIM + 1, :] * state[head] + item[:HEAD_DIM, :]

    tile = min(256, tokens)

    @pl.loop(0, tokens // tile)
    def _(turn):
        here = pl.ds(pl.multiple_of(turn * tile, tile), tile)
        for head in range(heads):
            lanes = slice(head * HEAD_DIM, (head + 1) * HEAD_DIM)
            full = outputs[here, lanes] + lax.dot_general(
                decayed_query[here, lanes], state[head].astype(BF16), LAST, preferred_element_type=F32
            )
            squares = jnp.mean(full * full, axis=-1, keepdims=True)
            raw = emission_ref[here, lanes].astype(F32)
            scaled = full * lax.rsqrt(squares + EPSILON) * gain_ref[:, lanes]
            mixed[tp, here, lanes] = (scaled * (raw * jax.nn.sigmoid(raw))).astype(BF16)

    for copy in mixed_sends:
        copy.start()
    run_stage(2)
    for copy in local:
        copy.wait()
    for copy in skip_arrivals:
        copy.wait_recv()
    for copy in mixed_arrivals:
        copy.wait_recv()

    @pl.loop(0, tokens // tile)
    def _(turn):
        here = pl.ds(pl.multiple_of(turn * tile, tile), tile)
        total = stream[here, :].astype(F32)
        for source in range(m):
            total += jnp.dot(
                mixed[source, here, :],
                projection[source * width : (source + 1) * width, :],
                preferred_element_type=F32,
            )
        rounded = total.astype(BF16)
        stream[here, :] = rounded
        total = rounded.astype(F32)
        squares = jnp.mean(total * total, axis=-1, keepdims=True)
        normed[here, :] = (total * lax.rsqrt(squares + EPSILON) * row_gain_ref[...]).astype(BF16)

    run_stage(3)
    for name in messages:
        if name[2] < 2:
            await_unit(name)

    core, pair = lax.rem(tp, 2), tp // 2
    buddy = (sp, pair * 2 + 1 - core)

    def half(number, which):
        return part.at[number, pl.ds(pl.multiple_of(which * rows, rows), rows)]

    def gate_and_up(number, owner):
        inputs = pl.ds(pl.multiple_of(owner * 2 * rows, 2 * rows), 2 * rows)

        def columns(lanes):
            value = normed[inputs, :]
            gate = jnp.dot(value, switch_all[:, lanes], preferred_element_type=F32)
            up = jnp.dot(value, expansion_all[:, lanes], preferred_element_type=F32)
            hidden[number, :, lanes] = (gate * jax.nn.sigmoid(gate) * up).astype(BF16)

        @pl.loop(0, units // 256)
        def _(turn):
            columns(pl.ds(pl.multiple_of(turn * 256, 256), 256))

        if units % 256:
            columns(slice(units // 256 * 256, units))

    def down(number):
        @pl.loop(0, n)
        def _(turn):
            lanes = pl.ds(pl.multiple_of(turn * depth, depth), depth)
            part[number, :, lanes] = jnp.dot(
                hidden[number], contraction_all[turn], preferred_element_type=F32
            ).astype(BF16)

        copy = remote(
            half(number, 1 - core),
            from_buddy.at[number],
            buddy_send.at[number],
            buddy_recv.at[number],
            buddy,
        )
        copy.start()
        return copy

    for d in [*range(1, pairs), 0]:
        gate_and_up(d, lax.rem(pair + d, pairs))
    run_stage(4)
    for name in messages:
        await_unit(name)
    tail = []
    for d in range(1, pairs):
        owner = lax.rem(pair + d, pairs)
        copy = down(d)
        copy.wait_recv()
        cross_out[d - 1] = (half(d, core)[...].astype(F32) + from_buddy[d].astype(F32)).astype(BF16)
        cross = remote(
            cross_out.at[d - 1],
            cross_in.at[d - 1],
            cross_send.at[d - 1],
            cross_recv.at[d - 1],
            (sp, owner * 2 + core),
        )
        cross.start()
        tail += [copy, cross]
    copy = down(0)
    copy.wait_recv()
    total = half(0, core)[...].astype(F32) + from_buddy[0].astype(F32) + stream[rows_of(tp), :].astype(F32)
    for d in range(1, pairs):
        tail[2 * d - 1].wait_recv()
        total += cross_in[d - 1].astype(F32)
    out_ref[...] = total.astype(BF16)

    for copy in tail + [copy] + skip_sends + mixed_sends:
        copy.wait_send()
    for _, sent, send, _, _, _ in messages.values():
        where(sent, send.wait_send)
    for d in range(1, n):
        pl.when(sp + d < n)(state_copies[d - 1].wait_send)


def on_device(n, m, *arrays):
    (skip, query, forget, value, emission, slack, surge, gain, projection, row_gain, switch, expansion, contraction) = arrays
    tokens, width = query.shape
    rows, model = skip.shape
    depth, units = switch.shape
    heads, pairs = width // HEAD_DIM, m // 2
    count = 3 * (3 * n // 2 + 3) if n == 8 else 3 * (n - 1)
    vmem, anywhere = pl.BlockSpec(memory_space=pltpu.VMEM), pl.BlockSpec(memory_space=pl.ANY)
    dma = pltpu.SemaphoreType.DMA
    return pl.pallas_call(
        functools.partial(kernel, n, m),
        out_shape=jax.ShapeDtypeStruct((rows, model), BF16),
        in_specs=[anywhere] + [vmem] * 7 + [anywhere, vmem] + [anywhere] * 3,
        out_specs=vmem,
        scratch_shapes=[
            pltpu.VMEM((model, units), BF16),
            pltpu.VMEM((model, units), BF16),
            pltpu.VMEM((n, units, depth), BF16),
            pltpu.VMEM(projection.shape, BF16),
            pltpu.VMEM((tokens, model), BF16),
            pltpu.VMEM((tokens, model), BF16),
            pltpu.VMEM((pairs, 2 * rows, units), BF16),
            pltpu.VMEM((m, tokens, width), BF16),
            pltpu.VMEM((tokens, width), F32),
            pltpu.VMEM((tokens, width), BF16),
            pltpu.VMEM((heads, HEAD_DIM, HEAD_DIM), F32),
            pltpu.VMEM((1, width), F32),
            pltpu.VMEM((heads, STATE_ROWS, HEAD_DIM), BF16),
            pltpu.VMEM((n - 1, heads, STATE_ROWS, HEAD_DIM), BF16),
            pltpu.VMEM((pairs, 2 * rows, model), BF16),
            pltpu.VMEM((pairs, rows, model), BF16),
            pltpu.VMEM((pairs - 1, rows, model), BF16),
            pltpu.VMEM((pairs - 1, rows, model), BF16),
            dma((5,)),
            dma((count,)),
            dma((count,)),
            dma((m - 1,)),
            dma((m - 1,)),
            dma((m - 1,)),
            dma((m - 1,)),
            dma((n - 1,)),
            dma((n - 1,)),
            dma((pairs,)),
            dma((pairs,)),
            dma((pairs - 1,)),
            dma((pairs - 1,)),
        ],
        compiler_params=pltpu.CompilerParams(
            collective_id=0, has_side_effects=True, vmem_limit_bytes=63_000_000
        ),
    )(
        skip,
        query,
        forget,
        value,
        emission,
        slack.reshape(1, width),
        surge,
        gain.reshape(1, width),
        projection,
        row_gain.reshape(1, model),
        switch,
        expansion,
        contraction,
    )


def paired_kernel(
    n,
    m,
    skip_ref,
    query_ref,
    forget_ref,
    value_ref,
    emission_ref,
    slack_ref,
    surge_ref,
    gain_ref,
    projection_ref,
    row_gain_ref,
    switch_ref,
    expansion_ref,
    contraction_ref,
    out_ref,
    switch_half,
    expansion_half,
    contraction_half,
    projection,
    stream,
    normed,
    hidden,
    mixed,
    outputs,
    decayed_query,
    state,
    offset,
    state_out,
    state_in,
    chain_out,
    chain_in,
    part,
    from_buddy,
    cross_out,
    cross_in,
    plane_out,
    plane_in,
    local_sem,
    weight_send,
    weight_recv,
    skip_sem,
    state_sem,
    chain_sem,
    mixed_send,
    mixed_recv,
    normed_send,
    normed_recv,
    buddy_send,
    buddy_recv,
    cross_send,
    cross_recv,
    plane_send,
    plane_recv,
):
    sp, tp = lax.axis_index("sp"), lax.axis_index("tp")
    tokens, width = query_ref.shape
    rows, model = skip_ref.shape
    depth, units = switch_ref.shape
    heads = width // HEAD_DIM
    few = units // 256 * 128
    many = units - few
    z, y = sp // 2, lax.rem(sp, 2)
    x, core = tp // 2, lax.rem(tp, 2)
    planes = {0: z, 1: z + 1 - 2 * lax.rem(z, 2), 2: lax.rem(z + 2, 4), 3: 3 - z}
    outer = (z == 0) | (z == 3)
    beside = (z * 2 + 1 - y, tp)
    across = (sp, (1 - x) * 2 + core)
    buddy = (sp, x * 2 + 1 - core)
    paired = (planes[1] * 2 + y, tp)

    barrier = pltpu.get_barrier_semaphore()
    for d in range(1, n):
        pl.semaphore_signal(barrier, inc=1, device_id=(lax.rem(sp + d, n), tp), device_id_type=MESH)
    for d in range(1, m):
        pl.semaphore_signal(barrier, inc=1, device_id=(sp, lax.rem(tp + d, m)), device_id_type=MESH)
    pl.semaphore_wait(barrier, n - 1 + m - 1)

    def remote(src, dst, send, recv, device):
        return pltpu.make_async_remote_copy(
            src_ref=src, dst_ref=dst, send_sem=send, recv_sem=recv, device_id=device, device_id_type=MESH
        )

    sends = []

    def start(copy):
        copy.start()
        sends.append(copy)

    def by_kind(action):
        pl.when(outer)(lambda: action(False))
        pl.when(jnp.logical_not(outer))(lambda: action(True))

    def own(tensor, big):
        span = pl.ds(few, many) if big else pl.ds(0, few)
        if tensor == 2:
            return contraction_ref.at[span]
        return (switch_ref, expansion_ref)[tensor].at[:, span]

    def held(tensor, owner, big):
        span = pl.ds(0, many if big else few)
        if tensor == 2:
            return contraction_half.at[owner, span]
        place = pl.ds(pl.multiple_of(owner * depth, depth), depth)
        return (switch_half, expansion_half)[tensor].at[place, span]

    def weight(tensor, kind, big):
        sems = (weight_send.at[tensor * 7 + kind], weight_recv.at[tensor * 7 + kind])
        if kind == 0:
            return remote(own(tensor, big), held(tensor, sp, big), *sems, beside)
        if kind <= 3:
            wanted = big if kind == 3 else not big
            return remote(own(tensor, wanted), held(tensor, sp, wanted), *sems, (planes[kind] * 2 + y, tp))
        unit = held(tensor, planes[kind - 3] * 2 + y, big)
        return remote(unit, unit, *sems, beside)

    def weight_arrival(tensor, kind, big):
        sems = (weight_send.at[tensor * 7 + kind], weight_recv.at[tensor * 7 + kind])
        if kind == 0:
            owner = z * 2 + 1 - y
        elif kind <= 3:
            owner = planes[kind] * 2 + y
        else:
            owner = planes[kind - 3] * 2 + 1 - y
        unit = held(tensor, owner, big)
        return remote(unit, unit, *sems, beside)

    def local_weight(tensor, big):
        return pltpu.make_async_copy(own(tensor, big), held(tensor, sp, big), local_sem.at[2 + tensor])

    def send_weights(*pairs):
        def action(big):
            for tensor, kind in pairs:
                weight(tensor, kind, big).start()

        by_kind(action)

    def await_weights(*pairs):
        def action(big):
            for tensor, kind in pairs:
                weight_arrival(tensor, kind, big).wait_recv()

        by_kind(action)

    def relay(tensor, kind):
        def action(big):
            weight_arrival(tensor, kind, big).wait_recv()
            weight(tensor, kind + 3, big).start()

        by_kind(action)

    send_weights((0, 0), (0, 1), (0, 3), (0, 2), (1, 0))
    start(remote(skip_ref, stream.at[1], skip_sem.at[0], skip_sem.at[1], across))
    local = [
        pltpu.make_async_copy(skip_ref, stream.at[0], local_sem.at[0]),
        pltpu.make_async_copy(projection_ref, projection, local_sem.at[1]),
    ]
    for copy in local:
        copy.start()

    def prepare(big):
        for tensor in range(3):
            local_weight(tensor, big).start()
        if not big and many > few:
            switch_half[:, few:] = jnp.zeros((model, many - few), BF16)
            expansion_half[:, few:] = jnp.zeros((model, many - few), BF16)
            for owner in range(n):
                contraction_half[owner, few:, :] = jnp.zeros((many - few, depth), BF16)

    by_kind(prepare)

    state[...] = jnp.zeros_like(state)
    offset[...] = jnp.zeros_like(offset)
    before = lax.broadcasted_iota(jnp.int32, (BLOCK, BLOCK), 0) >= lax.broadcasted_iota(
        jnp.int32, (BLOCK, BLOCK), 1
    )
    lower = before.astype(F32)

    def recur(block):
        here = pl.ds(pl.multiple_of(block * BLOCK, BLOCK), BLOCK)
        raw = query_ref[here, :].astype(F32)
        query = raw * jax.nn.sigmoid(raw)
        gate = slack_ref[...] * jax.nn.sigmoid(-forget_ref[here, :].astype(F32))
        log_forget = jnp.log1p(-gate) + surge_ref[here, :]
        total = jnp.dot(lower, log_forget, precision=lax.Precision.HIGHEST, preferred_element_type=F32)
        middle, last = total[BLOCK // 2 : BLOCK // 2 + 1, :], total[BLOCK - 1 :, :]
        left = (query * jnp.exp(total - middle)).astype(BF16)
        right = (gate * jnp.exp(middle - total)).astype(BF16)
        carried = (query * jnp.exp(total)).astype(BF16)
        kept = (gate * jnp.exp(last - total)).astype(BF16)
        decayed_query[here, :] = (query * jnp.exp(total + offset[...])).astype(BF16)
        closing = jnp.exp(last)
        for head in range(heads):
            lanes = slice(head * HEAD_DIM, (head + 1) * HEAD_DIM)
            value = value_ref[here, lanes]
            scores = lax.dot_general(left[:, lanes], right[:, lanes], LAST, preferred_element_type=F32)
            scores = jnp.where(before, scores, 0.0).astype(BF16)
            kept_state = state[head]
            outputs[here, lanes] = jnp.dot(
                scores, value, preferred_element_type=F32
            ) + lax.dot_general(carried[:, lanes], kept_state.astype(BF16), LAST, preferred_element_type=F32)
            state[head] = closing[:, lanes] * kept_state + lax.dot_general(
                value, kept[:, lanes], FIRST, preferred_element_type=F32
            )
        offset[...] += last

    blocks = tokens // BLOCK
    pl.loop(0, blocks * 5 // 8)(recur)
    relay(0, 1)
    pl.loop(blocks * 5 // 8, blocks)(recur)

    for head in range(heads):
        lanes = slice(head * HEAD_DIM, (head + 1) * HEAD_DIM)
        state_out[head, :HEAD_DIM, :] = state[head].astype(BF16)
        decay = jnp.exp(offset[:, lanes])
        state_out[head, HEAD_DIM:, :] = jnp.broadcast_to(decay, (16, HEAD_DIM)).astype(BF16)
    exchange = remote(state_out, state_in, state_sem.at[0], state_sem.at[1], beside)
    start(exchange)
    chain = remote(chain_out, chain_in, chain_sem.at[0], chain_sem.at[1], ((z + 1) * 2 + y, tp))
    chain_arrival = remote(chain_in, chain_in, chain_sem.at[0], chain_sem.at[1], beside)
    exchange.wait_recv()

    @pl.when(z > 0)
    def _():
        chain_arrival.wait_recv()

    @pl.when(z == 0)
    def _():
        chain_in[...] = jnp.zeros_like(chain_in)

    for head in range(heads):
        lanes = slice(head * HEAD_DIM, (head + 1) * HEAD_DIM)
        decay = jnp.exp(offset[:, lanes])
        other = state_in[head, :HEAD_DIM, :].astype(F32)
        other_decay = state_in[head, HEAD_DIM : HEAD_DIM + 1, :].astype(F32)
        prefix, mine = chain_in[head].astype(F32), state[head]

        @pl.when(y == 0)
        def _():
            chain_out[head] = (other_decay * (decay * prefix + mine) + other).astype(BF16)
            state[head] = prefix

        @pl.when(y == 1)
        def _():
            middle = other_decay * prefix + other
            chain_out[head] = (decay * middle + mine).astype(BF16)
            state[head] = middle

    pl.when(z < 3)(chain.start)
    send_weights((1, 1), (1, 3), (1, 2))
    relay(0, 3)
    relay(0, 2)

    def mixed_copy(slot, source, block, kind, device):
        place = mixed.at[source, block]
        index = kind * 2 + slot
        return remote(place, place, mixed_send.at[index], mixed_recv.at[index], device)

    for j in range(2):
        side = 1 - x if j else x
        for r in range(2):
            target = 1 - core if r else core
            block = side * 2 + target
            here = pl.ds(pl.multiple_of(block * rows, rows), rows)
            for head in range(heads):
                lanes = slice(head * HEAD_DIM, (head + 1) * HEAD_DIM)
                full = outputs[here, lanes] + lax.dot_general(
                    decayed_query[here, lanes], state[head].astype(BF16), LAST, preferred_element_type=F32
                )
                squares = jnp.mean(full * full, axis=-1, keepdims=True)
                raw = emission_ref[here, lanes].astype(F32)
                scaled = full * lax.rsqrt(squares + EPSILON) * gain_ref[:, lanes]
                mixed[tp, block, :, lanes] = (scaled * (raw * jax.nn.sigmoid(raw))).astype(BF16)
            start(mixed_copy(1 - j, tp, block, r, (sp, (1 - x) * 2 + target)))
            if r:
                start(mixed_copy(j, tp, block, 2, buddy))

    relay(1, 1)
    for copy in local:
        copy.wait()
    remote(stream.at[1], stream.at[1], skip_sem.at[0], skip_sem.at[1], across).wait_recv()

    half = rows // 2

    def place_of(plane, side, which):
        return (which * 4 + plane * 2 + side) * rows

    def normed_copy(index, plane, side, which, device, piece=None):
        first, count = place_of(plane, side, which), rows
        target = place_of(1, side, which) if index < 2 else first
        if piece is not None:
            first, target, count = first + piece * half, target + piece * half, half
        return remote(
            normed.at[pl.ds(pl.multiple_of(first, half), count)],
            normed.at[pl.ds(pl.multiple_of(target, half), count)],
            normed_send.at[index],
            normed_recv.at[index],
            device,
        )

    def normed_arrival(index, plane, side, which, piece=None):
        first, count = place_of(plane, side, which), rows
        if piece is not None:
            first, count = first + piece * half, half
        block = normed.at[pl.ds(pl.multiple_of(first, half), count)]
        return remote(block, block, normed_send.at[index], normed_recv.at[index], beside)

    for j in range(2):
        side = 1 - x if j else x
        block = side * 2 + core
        mixed_copy(j, (1 - x) * 2 + core, block, 0, across).wait_recv()
        mixed_copy(j, (1 - x) * 2 + 1 - core, block, 1, across).wait_recv()
        mixed_copy(j, x * 2 + 1 - core, block, 2, across).wait_recv()
        first = place_of(0, side, core)
        for piece in range(2):
            here = slice(piece * half, (piece + 1) * half)
            total = stream[j, here, :].astype(F32)
            for source in range(m):
                total += jnp.dot(
                    mixed[source, block, here, :],
                    projection[source * width : (source + 1) * width, :],
                    preferred_element_type=F32,
                )
            rounded = total.astype(BF16)
            stream[j, here, :] = rounded
            total = rounded.astype(F32)
            squares = jnp.mean(total * total, axis=-1, keepdims=True)
            normed[pl.ds(pl.multiple_of(first + piece * half, half), half), :] = (
                total * lax.rsqrt(squares + EPSILON) * row_gain_ref[...]
            ).astype(BF16)
            if j == 0:
                start(normed_copy(piece, 0, side, core, paired, piece))
        start(normed_copy(2 + j, 0, side, core, buddy))

    send_weights((2, 1), (2, 3), (2, 2))
    relay(1, 3)
    relay(1, 2)
    send_weights((2, 0))

    def tiles(plane, action):
        @pl.loop(0, 2)
        def _(which):
            here = pl.ds(pl.multiple_of(which * 4 * rows + plane * 2 * rows, 2 * rows), 2 * rows)

            @pl.loop(0, many // 256)
            def _(turn):
                action(here, pl.ds(pl.multiple_of(turn * 256, 256), 256))

            if many % 256:
                action(here, slice(many // 256 * 256, many))

    def gate(here, lanes):
        value = jnp.dot(normed[here, :], switch_half[:, lanes], preferred_element_type=F32)
        hidden[here, lanes] = (value * jax.nn.sigmoid(value)).astype(BF16)

    def up(here, lanes):
        value = jnp.dot(normed[here, :], expansion_half[:, lanes], preferred_element_type=F32)
        hidden[here, lanes] = (hidden[here, lanes].astype(F32) * value).astype(BF16)

    for j in range(2):
        normed_arrival(2 + j, 0, 1 - x if j else x, 1 - core).wait_recv()

    def await_local(big):
        for tensor in range(3):
            local_weight(tensor, big).wait()

    by_kind(await_local)
    await_weights((0, 0), (0, 4), (0, 6), (0, 5))
    tiles(0, gate)
    for piece in range(2):
        normed_arrival(piece, 1, x, core, piece).wait_recv()
        start(normed_copy(4 + piece, 1, x, core, across, piece))
        start(normed_copy(6 + piece, 1, x, core, buddy, piece))
    await_weights((1, 0), (1, 4), (1, 6), (1, 5))
    tiles(0, up)
    for piece in range(2):
        normed_arrival(4 + piece, 1, 1 - x, core, piece).wait_recv()
        start(normed_copy(8 + piece, 1, 1 - x, core, buddy, piece))
    relay(2, 1)
    for piece in range(2):
        normed_arrival(6 + piece, 1, x, 1 - core, piece).wait_recv()
    for piece in range(2):
        normed_arrival(8 + piece, 1, 1 - x, 1 - core, piece).wait_recv()
    tiles(1, gate)
    tiles(1, up)

    base = z // 2

    def owner_of(turn):
        group, even = turn // 2, lax.rem(turn, 2)
        pair = base + (group // 2) * (1 - 2 * base)
        return (pair * 2 + even) * 2 + y + lax.rem(group, 2) * (1 - 2 * y)

    mine = pl.multiple_of(core * 4 * rows, 4 * rows)
    theirs = pl.multiple_of((1 - core) * 4 * rows, 4 * rows)

    def buddy_copy(turn):
        return remote(
            part.at[turn, pl.ds(theirs, 4 * rows)],
            from_buddy.at[turn],
            buddy_send.at[turn],
            buddy_recv.at[turn],
            buddy,
        )

    def cross_copy(turn):
        return remote(cross_out.at[turn], cross_in.at[turn], cross_send.at[turn], cross_recv.at[turn], across)

    def plane_copy(turn):
        return remote(plane_out.at[turn], plane_in.at[turn], plane_send.at[turn], plane_recv.at[turn], paired)

    def share(turn, plane, side):
        place = (plane * 2 + side) * rows
        local_part = part[turn, pl.ds(pl.multiple_of(mine + place, rows), rows), :].astype(F32)
        return local_part + from_buddy[turn, pl.ds(pl.multiple_of(place, rows), rows), :].astype(F32)

    lag_cross, lag_plane = 3, 5

    @pl.loop(0, n + lag_plane)
    def _(step):
        @pl.when(step == 1)
        def _():
            relay(2, 3)

        @pl.when(step == 2)
        def _():
            await_weights((2, 0), (2, 4))
            relay(2, 2)

        @pl.when(step == 6)
        def _():
            await_weights((2, 5), (2, 6))

        @pl.when(step < n)
        def _():
            unit = contraction_half.at[owner_of(step)]

            @pl.loop(0, 4)
            def _(turn):
                here = pl.ds(pl.multiple_of(turn * 2 * rows, 2 * rows), 2 * rows)
                part[step, here, :] = jnp.dot(
                    hidden[here, :], unit[...], preferred_element_type=F32
                ).astype(BF16)

            buddy_copy(step).start()

        @pl.when((step >= 1) & (step < n + 1))
        def _():
            turn = step - 1
            buddy_copy(turn).wait_recv()
            for plane in range(2):
                cross_out[turn, plane] = share(turn, plane, 1 - x).astype(BF16)
            cross_copy(turn).start()

        @pl.when((step >= lag_cross) & (step < n + lag_cross))
        def _():
            turn = step - lag_cross
            cross_copy(turn).wait_recv()
            plane_out[turn] = (share(turn, 1, x) + cross_in[turn, 1].astype(F32)).astype(BF16)
            plane_copy(turn).start()

        @pl.when(step >= lag_plane)
        def _():
            turn = step - lag_plane
            plane_copy(turn).wait_recv()
            lanes = pl.ds(pl.multiple_of(owner_of(turn) * depth, depth), depth)
            total = stream[0, :, lanes].astype(F32) + share(turn, 0, x)
            total += cross_in[turn, 0].astype(F32) + plane_in[turn].astype(F32)
            out_ref[:, lanes] = total.astype(BF16)

    @pl.loop(0, n)
    def _(turn):
        buddy_copy(turn).wait_send()
        cross_copy(turn).wait_send()
        plane_copy(turn).wait_send()

    for copy in sends:
        copy.wait_send()

    def await_weight_sends(big):
        for tensor in range(3):
            for kind in range(7):
                weight(tensor, kind, big).wait_send()

    by_kind(await_weight_sends)
    pl.when(z < 3)(chain.wait_send)


def on_device_paired(n, m, *arrays):
    (skip, query, forget, value, emission, slack, surge, gain, projection, row_gain, switch, expansion, contraction) = arrays
    tokens, width = query.shape
    rows, model = skip.shape
    depth, units = switch.shape
    heads = width // HEAD_DIM
    many = units - units // 256 * 128
    vmem, anywhere = pl.BlockSpec(memory_space=pltpu.VMEM), pl.BlockSpec(memory_space=pl.ANY)
    dma = pltpu.SemaphoreType.DMA
    return pl.pallas_call(
        functools.partial(paired_kernel, n, m),
        out_shape=jax.ShapeDtypeStruct((rows, model), BF16),
        in_specs=[anywhere] + [vmem] * 7 + [anywhere, vmem] + [anywhere] * 3,
        out_specs=vmem,
        scratch_shapes=[
            pltpu.VMEM((model, many), BF16),
            pltpu.VMEM((model, many), BF16),
            pltpu.VMEM((n, many, depth), BF16),
            pltpu.VMEM(projection.shape, BF16),
            pltpu.VMEM((2, rows, model), BF16),
            pltpu.VMEM((2 * tokens, model), BF16),
            pltpu.VMEM((2 * tokens, many), BF16),
            pltpu.VMEM((m, m, rows, width), BF16),
            pltpu.VMEM((tokens, width), F32),
            pltpu.VMEM((tokens, width), BF16),
            pltpu.VMEM((heads, HEAD_DIM, HEAD_DIM), F32),
            pltpu.VMEM((1, width), F32),
            pltpu.VMEM((heads, STATE_ROWS, HEAD_DIM), BF16),
            pltpu.VMEM((heads, STATE_ROWS, HEAD_DIM), BF16),
            pltpu.VMEM((heads, HEAD_DIM, HEAD_DIM), BF16),
            pltpu.VMEM((heads, HEAD_DIM, HEAD_DIM), BF16),
            pltpu.VMEM((n, 2 * tokens, depth), BF16),
            pltpu.VMEM((n, tokens, depth), BF16),
            pltpu.VMEM((n, 2, rows, depth), BF16),
            pltpu.VMEM((n, 2, rows, depth), BF16),
            pltpu.VMEM((n, rows, depth), BF16),
            pltpu.VMEM((n, rows, depth), BF16),
            dma((5,)),
            dma((21,)),
            dma((21,)),
            dma((2,)),
            dma((2,)),
            dma((2,)),
            dma((6,)),
            dma((6,)),
            dma((10,)),
            dma((10,)),
            dma((n,)),
            dma((n,)),
            dma((n,)),
            dma((n,)),
            dma((n,)),
            dma((n,)),
        ],
        compiler_params=pltpu.CompilerParams(
            collective_id=0, has_side_effects=True, vmem_limit_bytes=64_000_000
        ),
    )(
        skip,
        query,
        forget,
        value,
        emission,
        slack.reshape(1, width),
        surge,
        gain.reshape(1, width),
        projection,
        row_gain.reshape(1, model),
        switch,
        expansion,
        contraction,
    )


def solution(mesh):
    in_specs = (
        P(("sp", "tp"), None),
        P("sp", "tp"),
        P("sp", "tp"),
        P("sp", "tp"),
        P("sp", "tp"),
        P("tp"),
        P("sp", "tp"),
        P("tp"),
        P(),
        P(),
        P("sp", "tp"),
        P("sp", "tp"),
        P("tp", "sp"),
    )
    n, m = mesh.shape["sp"], mesh.shape["tp"]
    return jax.shard_map(
        functools.partial(on_device_paired if (n, m) == (8, 4) else on_device, n, m),
        mesh=mesh,
        in_specs=in_specs,
        out_specs=P(("sp", "tp"), None),
        check_vma=False,
    )
```

```python
import functools

import jax
import jax.numpy as jnp
from jax import lax
from jax.experimental import pallas as pl
from jax.experimental.pallas import tpu as pltpu
from jax.sharding import PartitionSpec as P

HEAD_DIM = 128
BLOCK = 64
STATE_ROWS = HEAD_DIM + 16
EPSILON = 1e-06
MESH = pl.DeviceIdType.MESH
F32, BF16 = jnp.float32, jnp.bfloat16
LAST = (((1,), (1,)), ((), ()))
FIRST = (((0,), (0,)), ((), ()))


def weight_plan(n, me):
    out = []
    if n != 8:
        for tensor in range(3):
            for d in range(1, n):
                to, source = lax.rem(me + d, n), lax.rem(me + n - d, n)
                out.append((0, tensor, ("D", d, tensor), True, me, to, True, source, None))
        return out
    ny, nz = 2, n // 2
    z, y = me // ny, lax.rem(me, ny)

    def at(place, flip):
        return jnp.clip(place, 0, nz - 1) * ny + (1 - y if flip else y)

    def crossed(place, tensor, way):
        first, last = (1, nz - 1) if way > 0 else (nz - 2, 0)
        return (place == first) | (place == last) if tensor == 0 else place == first

    def inside(place):
        return (place >= 0) & (place < nz)

    for tensor in range(3):
        late = 1 if tensor == 2 else 0
        out.append((0, tensor, ("Y", 0, tensor), True, me, at(z, 1), True, at(z, 1), None))
        for way in (1, -1):
            for k in range(1, nz):
                to, unit = z + way, z + way - way * k
                name, above = (way, k, tensor), (way, k - 1, tensor)
                stage = 0 if k == 1 else k - 1 + late
                out.append(
                    (stage, tensor, name, inside(to) & inside(unit), at(unit, 0), at(to, 0),
                     inside(z - way * k), at(z - way * k, 0), None if k == 1 else above)
                )
                held = inside(z - way * k)
                if k == 1:
                    held = held & jnp.logical_not(crossed(z, tensor, way))
                out.append(
                    (k + late, tensor, ("Y", way * k, tensor), held, at(z - way * k, 0), at(z, 1),
                     held, at(z - way * k, 1), name)
                )
            out.append(
                (2, tensor, ("X", way, tensor), inside(z + way) & crossed(z + way, tensor, way), at(z, 1),
                 at(z + way, 0), crossed(z, tensor, way), at(z - way, 1), ("Y", 0, tensor))
            )
    return out


def kernel(
    n,
    m,
    skip_ref,
    query_ref,
    forget_ref,
    value_ref,
    emission_ref,
    slack_ref,
    surge_ref,
    gain_ref,
    projection_ref,
    row_gain_ref,
    switch_ref,
    expansion_ref,
    contraction_ref,
    out_ref,
    switch_all,
    expansion_all,
    contraction_all,
    projection,
    stream,
    normed,
    hidden,
    mixed,
    outputs,
    decayed_query,
    state,
    offset,
    state_out,
    state_in,
    part,
    from_buddy,
    cross_out,
    cross_in,
    local_sem,
    weight_send,
    weight_recv,
    skip_send,
    skip_recv,
    mixed_send,
    mixed_recv,
    state_send,
    state_recv,
    buddy_send,
    buddy_recv,
    cross_send,
    cross_recv,
):
    sp, tp = lax.axis_index("sp"), lax.axis_index("tp")
    tokens, width = query_ref.shape
    rows, model = skip_ref.shape
    depth, units = switch_ref.shape
    heads = width // HEAD_DIM
    pairs = m // 2

    barrier = pltpu.get_barrier_semaphore()
    for d in range(1, n):
        pl.semaphore_signal(barrier, inc=1, device_id=(lax.rem(sp + d, n), tp), device_id_type=MESH)
    for d in range(1, m):
        pl.semaphore_signal(barrier, inc=1, device_id=(sp, lax.rem(tp + d, m)), device_id_type=MESH)
    pl.semaphore_wait(barrier, n - 1 + m - 1)

    def remote(src, dst, send, recv, device):
        return pltpu.make_async_remote_copy(
            src_ref=src, dst_ref=dst, send_sem=send, recv_sem=recv, device_id=device, device_id_type=MESH
        )

    own_units = (switch_ref, expansion_ref, contraction_ref)

    def unit(tensor, owner):
        if tensor == 2:
            return contraction_all.at[owner]
        held = (switch_all, expansion_all)[tensor]
        return held.at[pl.ds(pl.multiple_of(owner * depth, depth), depth)]

    messages = {}
    for index, (stage, tensor, name, sent, owner, target, arrives, arriving, after) in enumerate(
        weight_plan(n, sp)
    ):
        src = own_units[tensor] if stage == 0 else unit(tensor, owner)
        args = (weight_send.at[index], weight_recv.at[index], (target, tp))
        send = remote(src, unit(tensor, owner), *args)
        arrival = remote(unit(tensor, arriving), unit(tensor, arriving), *args)
        messages[name] = (stage, sent, send, arrives, arrival, after)
    arrived = set()

    def where(condition, action):
        if condition is True:
            action()
        else:
            pl.when(condition)(action)

    def await_unit(name):
        if name not in arrived:
            arrived.add(name)
            where(messages[name][3], messages[name][4].wait_recv)

    def run_stage(wanted):
        for name, (stage, sent, send, _, _, after) in messages.items():
            if stage == wanted:
                if after is not None:
                    await_unit(after)
                where(sent, send.start)

    run_stage(0)

    def rows_of(owner):
        return pl.ds(pl.multiple_of(owner * rows, rows), rows)

    skip_sends, skip_arrivals, mixed_sends, mixed_arrivals = [], [], [], []
    for d in range(1, m):
        source, target = lax.rem(tp + m - d, m), (sp, lax.rem(tp + d, m))
        sems = (skip_send.at[d - 1], skip_recv.at[d - 1], target)
        skip_sends.append(remote(skip_ref, stream.at[rows_of(tp)], *sems))
        skip_arrivals.append(remote(stream.at[rows_of(source)], stream.at[rows_of(source)], *sems))
        sems = (mixed_send.at[d - 1], mixed_recv.at[d - 1], target)
        mixed_sends.append(remote(mixed.at[tp], mixed.at[tp], *sems))
        mixed_arrivals.append(remote(mixed.at[source], mixed.at[source], *sems))
    for copy in skip_sends:
        copy.start()
    local = [
        pltpu.make_async_copy(skip_ref, stream.at[rows_of(tp)], local_sem.at[0]),
        pltpu.make_async_copy(projection_ref, projection, local_sem.at[1]),
    ] + [pltpu.make_async_copy(own_units[t], unit(t, sp), local_sem.at[2 + t]) for t in range(3)]
    for copy in local:
        copy.start()

    state[...] = jnp.zeros_like(state)
    offset[...] = jnp.zeros_like(offset)
    before = lax.broadcasted_iota(jnp.int32, (BLOCK, BLOCK), 0) >= lax.broadcasted_iota(
        jnp.int32, (BLOCK, BLOCK), 1
    )
    lower = before.astype(F32)

    @pl.loop(0, tokens // BLOCK)
    def _(block):
        here = pl.ds(pl.multiple_of(block * BLOCK, BLOCK), BLOCK)
        raw = query_ref[here, :].astype(F32)
        query = raw * jax.nn.sigmoid(raw)
        gate = slack_ref[...] * jax.nn.sigmoid(-forget_ref[here, :].astype(F32))
        log_forget = jnp.log1p(-gate) + surge_ref[here, :]
        total = jnp.dot(lower, log_forget, precision=lax.Precision.HIGHEST, preferred_element_type=F32)
        middle, last = total[BLOCK // 2 : BLOCK // 2 + 1, :], total[BLOCK - 1 :, :]
        left = (query * jnp.exp(total - middle)).astype(BF16)
        right = (gate * jnp.exp(middle - total)).astype(BF16)
        carried = (query * jnp.exp(total)).astype(BF16)
        kept = (gate * jnp.exp(last - total)).astype(BF16)
        decayed_query[here, :] = (query * jnp.exp(total + offset[...])).astype(BF16)
        closing = jnp.exp(last)
        for head in range(heads):
            lanes = slice(head * HEAD_DIM, (head + 1) * HEAD_DIM)
            value = value_ref[here, lanes]
            scores = lax.dot_general(left[:, lanes], right[:, lanes], LAST, preferred_element_type=F32)
            scores = jnp.where(before, scores, 0.0).astype(BF16)
            held = state[head]
            outputs[here, lanes] = jnp.dot(
                scores, value, preferred_element_type=F32
            ) + lax.dot_general(carried[:, lanes], held.astype(BF16), LAST, preferred_element_type=F32)
            state[head] = closing[:, lanes] * held + lax.dot_general(
                value, kept[:, lanes], FIRST, preferred_element_type=F32
            )
        offset[...] += last

    for head in range(heads):
        lanes = slice(head * HEAD_DIM, (head + 1) * HEAD_DIM)
        state_out[head, :HEAD_DIM, :] = state[head].astype(BF16)
        decay = jnp.exp(offset[:, lanes])
        state_out[head, HEAD_DIM:, :] = jnp.broadcast_to(decay, (16, HEAD_DIM)).astype(BF16)
    state_copies = []
    for d in range(1, n):
        copy = remote(
            state_out,
            state_in.at[d - 1],
            state_send.at[d - 1],
            state_recv.at[d - 1],
            (lax.rem(sp + d, n), tp),
        )
        state_copies.append(copy)
        pl.when(sp + d < n)(copy.start)

    run_stage(1)

    for d in range(1, n):
        pl.when(sp >= d)(state_copies[d - 1].wait_recv)
    state[...] = jnp.zeros_like(state)

    @pl.loop(0, sp)
    def _(earlier):
        slot = sp - earlier - 1
        for head in range(heads):
            item = state_in[slot, head].astype(F32)
            state[head] = item[HEAD_DIM : HEAD_DIM + 1, :] * state[head] + item[:HEAD_DIM, :]

    tile = min(256, tokens)

    @pl.loop(0, tokens // tile)
    def _(turn):
        here = pl.ds(pl.multiple_of(turn * tile, tile), tile)
        for head in range(heads):
            lanes = slice(head * HEAD_DIM, (head + 1) * HEAD_DIM)
            full = outputs[here, lanes] + lax.dot_general(
                decayed_query[here, lanes], state[head].astype(BF16), LAST, preferred_element_type=F32
            )
            squares = jnp.mean(full * full, axis=-1, keepdims=True)
            raw = emission_ref[here, lanes].astype(F32)
            scaled = full * lax.rsqrt(squares + EPSILON) * gain_ref[:, lanes]
            mixed[tp, here, lanes] = (scaled * (raw * jax.nn.sigmoid(raw))).astype(BF16)

    for copy in mixed_sends:
        copy.start()
    run_stage(2)
    for copy in local:
        copy.wait()
    for copy in skip_arrivals:
        copy.wait_recv()
    for copy in mixed_arrivals:
        copy.wait_recv()

    @pl.loop(0, tokens // tile)
    def _(turn):
        here = pl.ds(pl.multiple_of(turn * tile, tile), tile)
        total = stream[here, :].astype(F32)
        for source in range(m):
            total += jnp.dot(
                mixed[source, here, :],
                projection[source * width : (source + 1) * width, :],
                preferred_element_type=F32,
            )
        rounded = total.astype(BF16)
        stream[here, :] = rounded
        total = rounded.astype(F32)
        squares = jnp.mean(total * total, axis=-1, keepdims=True)
        normed[here, :] = (total * lax.rsqrt(squares + EPSILON) * row_gain_ref[...]).astype(BF16)

    run_stage(3)
    for name in messages:
        if name[2] < 2:
            await_unit(name)

    core, pair = lax.rem(tp, 2), tp // 2
    buddy = (sp, pair * 2 + 1 - core)

    def half(number, which):
        return part.at[number, pl.ds(pl.multiple_of(which * rows, rows), rows)]

    def gate_and_up(number, owner):
        inputs = pl.ds(pl.multiple_of(owner * 2 * rows, 2 * rows), 2 * rows)

        def columns(lanes):
            value = normed[inputs, :]
            gate = jnp.dot(value, switch_all[:, lanes], preferred_element_type=F32)
            up = jnp.dot(value, expansion_all[:, lanes], preferred_element_type=F32)
            hidden[number, :, lanes] = (gate * jax.nn.sigmoid(gate) * up).astype(BF16)

        @pl.loop(0, units // 256)
        def _(turn):
            columns(pl.ds(pl.multiple_of(turn * 256, 256), 256))

        if units % 256:
            columns(slice(units // 256 * 256, units))

    def down(number):
        @pl.loop(0, n)
        def _(turn):
            lanes = pl.ds(pl.multiple_of(turn * depth, depth), depth)
            part[number, :, lanes] = jnp.dot(
                hidden[number], contraction_all[turn], preferred_element_type=F32
            ).astype(BF16)

        copy = remote(
            half(number, 1 - core),
            from_buddy.at[number],
            buddy_send.at[number],
            buddy_recv.at[number],
            buddy,
        )
        copy.start()
        return copy

    for d in [*range(1, pairs), 0]:
        gate_and_up(d, lax.rem(pair + d, pairs))
    run_stage(4)
    for name in messages:
        await_unit(name)
    tail = []
    for d in range(1, pairs):
        owner = lax.rem(pair + d, pairs)
        copy = down(d)
        copy.wait_recv()
        cross_out[d - 1] = (half(d, core)[...].astype(F32) + from_buddy[d].astype(F32)).astype(BF16)
        cross = remote(
            cross_out.at[d - 1],
            cross_in.at[d - 1],
            cross_send.at[d - 1],
            cross_recv.at[d - 1],
            (sp, owner * 2 + core),
        )
        cross.start()
        tail += [copy, cross]
    copy = down(0)
    copy.wait_recv()
    total = half(0, core)[...].astype(F32) + from_buddy[0].astype(F32) + stream[rows_of(tp), :].astype(F32)
    for d in range(1, pairs):
        tail[2 * d - 1].wait_recv()
        total += cross_in[d - 1].astype(F32)
    out_ref[...] = total.astype(BF16)

    for copy in tail + [copy] + skip_sends + mixed_sends:
        copy.wait_send()
    for _, sent, send, _, _, _ in messages.values():
        where(sent, send.wait_send)
    for d in range(1, n):
        pl.when(sp + d < n)(state_copies[d - 1].wait_send)


def on_device(n, m, *arrays):
    (skip, query, forget, value, emission, slack, surge, gain, projection, row_gain, switch, expansion, contraction) = arrays
    tokens, width = query.shape
    rows, model = skip.shape
    depth, units = switch.shape
    heads, pairs = width // HEAD_DIM, m // 2
    count = 3 * (3 * n // 2 + 3) if n == 8 else 3 * (n - 1)
    vmem, anywhere = pl.BlockSpec(memory_space=pltpu.VMEM), pl.BlockSpec(memory_space=pl.ANY)
    dma = pltpu.SemaphoreType.DMA
    return pl.pallas_call(
        functools.partial(kernel, n, m),
        out_shape=jax.ShapeDtypeStruct((rows, model), BF16),
        in_specs=[anywhere] + [vmem] * 7 + [anywhere, vmem] + [anywhere] * 3,
        out_specs=vmem,
        scratch_shapes=[
            pltpu.VMEM((model, units), BF16),
            pltpu.VMEM((model, units), BF16),
            pltpu.VMEM((n, units, depth), BF16),
            pltpu.VMEM(projection.shape, BF16),
            pltpu.VMEM((tokens, model), BF16),
            pltpu.VMEM((tokens, model), BF16),
            pltpu.VMEM((pairs, 2 * rows, units), BF16),
            pltpu.VMEM((m, tokens, width), BF16),
            pltpu.VMEM((tokens, width), F32),
            pltpu.VMEM((tokens, width), BF16),
            pltpu.VMEM((heads, HEAD_DIM, HEAD_DIM), F32),
            pltpu.VMEM((1, width), F32),
            pltpu.VMEM((heads, STATE_ROWS, HEAD_DIM), BF16),
            pltpu.VMEM((n - 1, heads, STATE_ROWS, HEAD_DIM), BF16),
            pltpu.VMEM((pairs, 2 * rows, model), BF16),
            pltpu.VMEM((pairs, rows, model), BF16),
            pltpu.VMEM((pairs - 1, rows, model), BF16),
            pltpu.VMEM((pairs - 1, rows, model), BF16),
            dma((5,)),
            dma((count,)),
            dma((count,)),
            dma((m - 1,)),
            dma((m - 1,)),
            dma((m - 1,)),
            dma((m - 1,)),
            dma((n - 1,)),
            dma((n - 1,)),
            dma((pairs,)),
            dma((pairs,)),
            dma((pairs - 1,)),
            dma((pairs - 1,)),
        ],
        compiler_params=pltpu.CompilerParams(
            collective_id=0, has_side_effects=True, vmem_limit_bytes=63_000_000
        ),
    )(
        skip,
        query,
        forget,
        value,
        emission,
        slack.reshape(1, width),
        surge,
        gain.reshape(1, width),
        projection,
        row_gain.reshape(1, model),
        switch,
        expansion,
        contraction,
    )


def paired_kernel(
    n,
    m,
    skip_ref,
    query_ref,
    forget_ref,
    value_ref,
    emission_ref,
    slack_ref,
    surge_ref,
    gain_ref,
    projection_ref,
    row_gain_ref,
    switch_ref,
    expansion_ref,
    contraction_ref,
    out_ref,
    switch_half,
    expansion_half,
    contraction_half,
    projection,
    stream,
    normed,
    hidden,
    mixed,
    outputs,
    decayed_query,
    state,
    offset,
    state_out,
    state_in,
    chain_out,
    chain_in,
    part,
    from_buddy,
    cross_out,
    cross_in,
    plane_out,
    plane_in,
    local_sem,
    weight_send,
    weight_recv,
    skip_sem,
    state_sem,
    chain_sem,
    mixed_send,
    mixed_recv,
    normed_send,
    normed_recv,
    buddy_send,
    buddy_recv,
    cross_send,
    cross_recv,
    plane_send,
    plane_recv,
):
    sp, tp = lax.axis_index("sp"), lax.axis_index("tp")
    tokens, width = query_ref.shape
    rows, model = skip_ref.shape
    depth, units = switch_ref.shape
    heads = width // HEAD_DIM
    few = units // 256 * 128
    many = units - few
    z, y = sp // 2, lax.rem(sp, 2)
    x, core = tp // 2, lax.rem(tp, 2)
    planes = {0: z, 1: z + 1 - 2 * lax.rem(z, 2), 2: lax.rem(z + 2, 4), 3: 3 - z}
    outer = (z == 0) | (z == 3)
    beside = (z * 2 + 1 - y, tp)
    across = (sp, (1 - x) * 2 + core)
    buddy = (sp, x * 2 + 1 - core)
    paired = (planes[1] * 2 + y, tp)

    barrier = pltpu.get_barrier_semaphore()
    for d in range(1, n):
        pl.semaphore_signal(barrier, inc=1, device_id=(lax.rem(sp + d, n), tp), device_id_type=MESH)
    for d in range(1, m):
        pl.semaphore_signal(barrier, inc=1, device_id=(sp, lax.rem(tp + d, m)), device_id_type=MESH)
    def remote(src, dst, send, recv, device):
        return pltpu.make_async_remote_copy(
            src_ref=src, dst_ref=dst, send_sem=send, recv_sem=recv, device_id=device, device_id_type=MESH
        )

    sends = []

    def start(copy):
        copy.start()
        sends.append(copy)

    def by_kind(action):
        pl.when(outer)(lambda: action(False))
        pl.when(jnp.logical_not(outer))(lambda: action(True))

    def own(tensor, big):
        span = pl.ds(few, many) if big else pl.ds(0, few)
        if tensor == 2:
            return contraction_ref.at[span]
        return (switch_ref, expansion_ref)[tensor].at[:, span]

    def held(tensor, owner, big):
        span = pl.ds(0, many if big else few)
        if tensor == 2:
            return contraction_half.at[owner, span]
        place = pl.ds(pl.multiple_of(owner * depth, depth), depth)
        return (switch_half, expansion_half)[tensor].at[place, span]

    def weight(tensor, kind, big):
        sems = (weight_send.at[tensor * 8 + kind], weight_recv.at[tensor * 8 + kind])
        if kind == 0:
            return remote(own(tensor, big), held(tensor, sp, big), *sems, beside)
        if kind <= 3:
            wanted = big if kind == 3 else not big
            return remote(own(tensor, wanted), held(tensor, sp, wanted), *sems, (planes[kind] * 2 + y, tp))
        unit = held(tensor, planes[1 if kind == 7 else kind - 3] * 2 + y, big)
        if kind == 7:
            return remote(unit, unit, sems[0], weight_recv.at[tensor * 8 + 2], (planes[3] * 2 + y, tp))
        return remote(unit, unit, *sems, beside)

    def weight_arrival(tensor, kind, big):
        sems = (weight_send.at[tensor * 8 + kind], weight_recv.at[tensor * 8 + kind])
        if kind == 0:
            owner = z * 2 + 1 - y
        elif kind <= 3:
            owner = planes[kind] * 2 + y
        else:
            owner = planes[kind - 3] * 2 + 1 - y
        unit = held(tensor, owner, big)
        return remote(unit, unit, *sems, beside)

    def local_weight(tensor, big):
        return pltpu.make_async_copy(own(tensor, big), held(tensor, sp, big), local_sem.at[2 + tensor])

    def send_weights(*pairs):
        def action(big):
            for tensor, kind in pairs:
                if big or kind != 2:
                    weight(tensor, kind, big).start()

        by_kind(action)

    def await_weights(*pairs):
        def action(big):
            for tensor, kind in pairs:
                weight_arrival(tensor, kind, big).wait_recv()

        by_kind(action)

    def relay(tensor, kind):
        def action(big):
            weight_arrival(tensor, kind, big).wait_recv()
            weight(tensor, kind + 3, big).start()

        by_kind(action)

    local = [
        pltpu.make_async_copy(skip_ref, stream.at[0], local_sem.at[0]),
        pltpu.make_async_copy(projection_ref, projection, local_sem.at[1]),
    ]
    for copy in local:
        copy.start()

    def prepare(big):
        for tensor in range(3):
            local_weight(tensor, big).start()
        if not big and many > few:
            switch_half[:, few:] = jnp.zeros((model, many - few), BF16)
            expansion_half[:, few:] = jnp.zeros((model, many - few), BF16)
            for owner in range(n):
                contraction_half[owner, few:, :] = jnp.zeros((many - few, depth), BF16)

    by_kind(prepare)

    state[...] = jnp.zeros_like(state)
    offset[...] = jnp.zeros_like(offset)
    before = lax.broadcasted_iota(jnp.int32, (BLOCK, BLOCK), 0) >= lax.broadcasted_iota(
        jnp.int32, (BLOCK, BLOCK), 1
    )
    lower = before.astype(F32)

    def recur(block):
        here = pl.ds(pl.multiple_of(block * BLOCK, BLOCK), BLOCK)
        raw = query_ref[here, :].astype(F32)
        query = raw * jax.nn.sigmoid(raw)
        gate = slack_ref[...] * jax.nn.sigmoid(-forget_ref[here, :].astype(F32))
        log_forget = jnp.log1p(-gate) + surge_ref[here, :]
        total = jnp.dot(lower, log_forget, precision=lax.Precision.HIGHEST, preferred_element_type=F32)
        middle, last = total[BLOCK // 2 : BLOCK // 2 + 1, :], total[BLOCK - 1 :, :]
        left = (query * jnp.exp(total - middle)).astype(BF16)
        right = (gate * jnp.exp(middle - total)).astype(BF16)
        carried = (query * jnp.exp(total)).astype(BF16)
        kept = (gate * jnp.exp(last - total)).astype(BF16)
        decayed_query[here, :] = (query * jnp.exp(total + offset[...])).astype(BF16)
        closing = jnp.exp(last)
        for head in range(heads):
            lanes = slice(head * HEAD_DIM, (head + 1) * HEAD_DIM)
            value = value_ref[here, lanes]
            scores = lax.dot_general(left[:, lanes], right[:, lanes], LAST, preferred_element_type=F32)
            scores = jnp.where(before, scores, 0.0).astype(BF16)
            kept_state = state[head]
            outputs[here, lanes] = jnp.dot(
                scores, value, preferred_element_type=F32
            ) + lax.dot_general(carried[:, lanes], kept_state.astype(BF16), LAST, preferred_element_type=F32)
            state[head] = closing[:, lanes] * kept_state + lax.dot_general(
                value, kept[:, lanes], FIRST, preferred_element_type=F32
            )
        offset[...] += last

    blocks = tokens // BLOCK
    early = blocks // 4
    pl.loop(0, early)(recur)
    pl.semaphore_wait(barrier, n - 1 + m - 1)
    send_weights((0, 0), (0, 1))
    pl.when(z > 0)(lambda: send_weights((0, 3)))

    @pl.when(z > 1)
    def _():
        send_weights((0, 2))

    @pl.when(z == 3)
    def _():
        send_weights((1, 1), (1, 3))

    start(remote(skip_ref, stream.at[1], skip_sem.at[0], skip_sem.at[1], across))
    pl.loop(early, blocks)(recur)

    for head in range(heads):
        lanes = slice(head * HEAD_DIM, (head + 1) * HEAD_DIM)
        state_out[head, :HEAD_DIM, :] = state[head].astype(BF16)
        decay = jnp.exp(offset[:, lanes])
        state_out[head, HEAD_DIM:, :] = jnp.broadcast_to(decay, (16, HEAD_DIM)).astype(BF16)
    exchange = remote(state_out, state_in, state_sem.at[0], state_sem.at[1], beside)
    start(exchange)
    chain = remote(chain_out, chain_in, chain_sem.at[0], chain_sem.at[1], ((z + 1) * 2 + y, tp))
    chain_arrival = remote(chain_in, chain_in, chain_sem.at[0], chain_sem.at[1], beside)
    relay(0, 1)
    exchange.wait_recv()

    def forward(tensor):
        pl.when(jnp.logical_not(outer))(lambda: weight(tensor, 7, True).start())

    pl.when(z == 2)(lambda: forward(0))

    def advance(prefixes):
        for head in range(heads):
            lanes = slice(head * HEAD_DIM, (head + 1) * HEAD_DIM)
            decay = jnp.exp(offset[:, lanes])
            other = state_in[head, :HEAD_DIM, :].astype(F32)
            other_decay = state_in[head, HEAD_DIM : HEAD_DIM + 1, :].astype(F32)
            prefix, mine = prefixes(head), state[head]

            @pl.when(y == 0)
            def _():
                chain_out[head] = (other_decay * (decay * prefix + mine) + other).astype(BF16)
                state[head] = prefix

            @pl.when(y == 1)
            def _():
                middle = other_decay * prefix + other
                chain_out[head] = (decay * middle + mine).astype(BF16)
                state[head] = middle

    @pl.when(z == 0)
    def _():
        advance(lambda head: jnp.zeros((HEAD_DIM, HEAD_DIM), F32))
        chain.start()
        send_weights((0, 3), (1, 1), (1, 3))

    @pl.when((z == 1) | (z == 2))
    def _():
        pl.when(z == 1)(lambda: send_weights((1, 1)))
        pl.when(z == 2)(lambda: send_weights((1, 3), (1, 2)))

    relay(0, 3)

    @pl.when(z > 0)
    def _():
        chain_arrival.wait_recv()
        advance(lambda head: chain_in[head].astype(F32))

    pl.when((z > 0) & (z < 3))(chain.start)

    @pl.when(z == 1)
    def _():
        send_weights((0, 2))
        forward(0)
        send_weights((1, 3), (1, 2))

    pl.when(z == 2)(lambda: send_weights((1, 1)))
    send_weights((1, 0))

    def mixed_copy(slot, source, block, kind, device):
        place = mixed.at[source, block]
        index = kind * 2 + slot
        return remote(place, place, mixed_send.at[index], mixed_recv.at[index], device)

    for j in range(2):
        side = 1 - x if j else x
        for r in range(2):
            target = 1 - core if r else core
            block = side * 2 + target
            here = pl.ds(pl.multiple_of(block * rows, rows), rows)
            for head in range(heads):
                lanes = slice(head * HEAD_DIM, (head + 1) * HEAD_DIM)
                full = outputs[here, lanes] + lax.dot_general(
                    decayed_query[here, lanes], state[head].astype(BF16), LAST, preferred_element_type=F32
                )
                squares = jnp.mean(full * full, axis=-1, keepdims=True)
                raw = emission_ref[here, lanes].astype(F32)
                scaled = full * lax.rsqrt(squares + EPSILON) * gain_ref[:, lanes]
                mixed[tp, block, :, lanes] = (scaled * (raw * jax.nn.sigmoid(raw))).astype(BF16)
            start(mixed_copy(1 - j, tp, block, r, (sp, (1 - x) * 2 + target)))
            if r:
                start(mixed_copy(j, tp, block, 2, buddy))

    for copy in local:
        copy.wait()
    remote(stream.at[1], stream.at[1], skip_sem.at[0], skip_sem.at[1], across).wait_recv()

    pieces = 4
    fine = rows // pieces

    def place_of(plane, side, which):
        return (which * 4 + plane * 2 + side) * rows

    def normed_rows(plane, side, which, piece):
        first, count = place_of(plane, side, which), rows
        if piece is not None:
            first, count = first + piece * fine, fine
        return normed.at[pl.ds(pl.multiple_of(first, fine), count)]

    def normed_copy(index, device, plane, side, which, piece=None, target=None):
        return remote(
            normed_rows(plane, side, which, piece),
            normed_rows(plane if target is None else target, side, which, piece),
            normed_send.at[index],
            normed_recv.at[index],
            device,
        )

    for j in range(2):
        side = 1 - x if j else x
        block = side * 2 + core
        mixed_copy(j, (1 - x) * 2 + core, block, 0, across).wait_recv()
        mixed_copy(j, (1 - x) * 2 + 1 - core, block, 1, across).wait_recv()
        mixed_copy(j, x * 2 + 1 - core, block, 2, across).wait_recv()
        first = place_of(0, side, core)
        for piece in range(2):
            here = slice(piece * rows // 2, (piece + 1) * rows // 2)
            total = stream[j, here, :].astype(F32)
            for source in range(m):
                total += jnp.dot(
                    mixed[source, block, here, :],
                    projection[source * width : (source + 1) * width, :],
                    preferred_element_type=F32,
                )
            rounded = total.astype(BF16)
            stream[j, here, :] = rounded
            total = rounded.astype(F32)
            squares = jnp.mean(total * total, axis=-1, keepdims=True)
            normed[pl.ds(pl.multiple_of(first + piece * rows // 2, rows // 2), rows // 2), :] = (
                total * lax.rsqrt(squares + EPSILON) * row_gain_ref[...]
            ).astype(BF16)
            if j == 0:
                for part_of in range(piece * pieces // 2, (piece + 1) * pieces // 2):
                    start(normed_copy(2 + part_of, paired, 0, side, core, part_of, 1))
        start(normed_copy(j, buddy, 0, side, core))

    relay(0, 2)
    relay(1, 1)
    forward(1)
    relay(1, 3)

    def tiles(plane, action):
        @pl.loop(0, 2)
        def _(which):
            here = pl.ds(pl.multiple_of(which * 4 * rows + plane * 2 * rows, 2 * rows), 2 * rows)

            @pl.loop(0, many // 256)
            def _(turn):
                action(here, pl.ds(pl.multiple_of(turn * 256, 256), 256))

            if many % 256:
                action(here, slice(many // 256 * 256, many))

    def gate(here, lanes):
        value = jnp.dot(normed[here, :], switch_half[:, lanes], preferred_element_type=F32)
        hidden[here, lanes] = (value * jax.nn.sigmoid(value)).astype(BF16)

    def up(here, lanes):
        value = jnp.dot(normed[here, :], expansion_half[:, lanes], preferred_element_type=F32)
        hidden[here, lanes] = (hidden[here, lanes].astype(F32) * value).astype(BF16)

    def normed_arrives(index, plane, side, which, piece=None):
        normed_copy(index, buddy, plane, side, which, piece).wait_recv()

    for j in range(2):
        normed_arrives(j, 0, 1 - x if j else x, 1 - core)

    def await_local(big):
        for tensor in range(3):
            local_weight(tensor, big).wait()

    by_kind(await_local)
    await_weights((0, 0), (0, 4), (0, 6), (0, 5))
    tiles(0, gate)
    relay(1, 2)
    for piece in range(pieces):
        normed_arrives(2 + piece, 1, x, core, piece)
        start(normed_copy(6 + piece, across, 1, x, core, piece))
        start(normed_copy(10 + piece, buddy, 1, x, core, piece))
    send_weights((2, 0), (2, 1), (2, 3), (2, 2))
    await_weights((1, 0), (1, 4), (1, 6), (1, 5))
    tiles(0, up)
    for piece in range(pieces):
        normed_arrives(6 + piece, 1, 1 - x, core, piece)
        start(normed_copy(14 + piece, buddy, 1, 1 - x, core, piece))
    relay(2, 1)
    forward(2)
    for piece in range(pieces):
        normed_arrives(10 + piece, 1, x, 1 - core, piece)
        normed_arrives(14 + piece, 1, 1 - x, 1 - core, piece)
    tiles(1, gate)
    tiles(1, up)

    base = z // 2

    def owner_of(turn):
        group, even = turn // 2, lax.rem(turn, 2)
        pair = base + (group // 2) * (1 - 2 * base)
        return (pair * 2 + even) * 2 + y + lax.rem(group, 2) * (1 - 2 * y)

    mine = pl.multiple_of(core * 4 * rows, 4 * rows)
    theirs = pl.multiple_of((1 - core) * 4 * rows, 4 * rows)

    def buddy_copy(turn):
        return remote(
            part.at[turn, pl.ds(theirs, 4 * rows)],
            from_buddy.at[turn],
            buddy_send.at[turn],
            buddy_recv.at[turn],
            buddy,
        )

    def partner(odd):
        return (sp + (paired[0] - sp) * odd, across[1] + (tp - across[1]) * odd)

    def cross_copy(turn):
        sems = (cross_send.at[turn], cross_recv.at[turn])
        return remote(cross_out.at[turn], cross_in.at[turn], *sems, partner(lax.rem(turn, 2)))

    def plane_copy(turn):
        sems = (plane_send.at[turn], plane_recv.at[turn])
        return remote(plane_out.at[turn], plane_in.at[turn], *sems, partner(1 - lax.rem(turn, 2)))

    def share(turn, plane, side):
        place = (plane * 2 + side) * rows
        local_part = part[turn, pl.ds(pl.multiple_of(mine + place, rows), rows), :].astype(F32)
        return local_part + from_buddy[turn, pl.ds(pl.multiple_of(place, rows), rows), :].astype(F32)

    lag_cross, lag_plane = 3, 5

    @pl.loop(0, n + lag_plane)
    def _(step):
        @pl.when(step == 1)
        def _():
            relay(2, 3)

        @pl.when(step == 2)
        def _():
            await_weights((2, 0), (2, 4))
            relay(2, 2)

        @pl.when(step == 6)
        def _():
            await_weights((2, 5), (2, 6))

        @pl.when(step < n)
        def _():
            unit = contraction_half.at[owner_of(step)]

            @pl.loop(0, 4)
            def _(turn):
                here = pl.ds(pl.multiple_of(turn * 2 * rows, 2 * rows), 2 * rows)
                part[step, here, :] = jnp.dot(
                    hidden[here, :], unit[...], preferred_element_type=F32
                ).astype(BF16)

            buddy_copy(step).start()

        @pl.when((step >= 1) & (step < n + 1))
        def _():
            turn = step - 1
            buddy_copy(turn).wait_recv()
            odd = lax.rem(turn, 2)
            cross_out[turn, 0] = share(turn, odd, 1 - x + (2 * x - 1) * odd).astype(BF16)
            cross_out[turn, 1] = share(turn, 1, 1 - x).astype(BF16)
            cross_copy(turn).start()

        @pl.when((step >= lag_cross) & (step < n + lag_cross))
        def _():
            turn = step - lag_cross
            cross_copy(turn).wait_recv()
            odd = lax.rem(turn, 2)
            total = share(turn, 1 - odd, x + (1 - 2 * x) * odd) + cross_in[turn, 1].astype(F32)
            plane_out[turn] = total.astype(BF16)
            plane_copy(turn).start()

        @pl.when(step >= lag_plane)
        def _():
            turn = step - lag_plane
            plane_copy(turn).wait_recv()
            lanes = pl.ds(pl.multiple_of(owner_of(turn) * depth, depth), depth)
            total = stream[0, :, lanes].astype(F32) + share(turn, 0, x)
            total += cross_in[turn, 0].astype(F32) + plane_in[turn].astype(F32)
            out_ref[:, lanes] = total.astype(BF16)

    @pl.loop(0, n)
    def _(turn):
        buddy_copy(turn).wait_send()
        cross_copy(turn).wait_send()
        plane_copy(turn).wait_send()

    for copy in sends:
        copy.wait_send()

    def await_weight_sends(big):
        for tensor in range(3):
            for kind in range(8) if big else (0, 1, 3, 4, 5, 6):
                weight(tensor, kind, big).wait_send()

    by_kind(await_weight_sends)
    pl.when(z < 3)(chain.wait_send)


def on_device_paired(n, m, *arrays):
    (skip, query, forget, value, emission, slack, surge, gain, projection, row_gain, switch, expansion, contraction) = arrays
    tokens, width = query.shape
    rows, model = skip.shape
    depth, units = switch.shape
    heads = width // HEAD_DIM
    many = units - units // 256 * 128
    vmem, anywhere = pl.BlockSpec(memory_space=pltpu.VMEM), pl.BlockSpec(memory_space=pl.ANY)
    dma = pltpu.SemaphoreType.DMA
    return pl.pallas_call(
        functools.partial(paired_kernel, n, m),
        out_shape=jax.ShapeDtypeStruct((rows, model), BF16),
        in_specs=[anywhere] + [vmem] * 7 + [anywhere, vmem] + [anywhere] * 3,
        out_specs=vmem,
        scratch_shapes=[
            pltpu.VMEM((model, many), BF16),
            pltpu.VMEM((model, many), BF16),
            pltpu.VMEM((n, many, depth), BF16),
            pltpu.VMEM(projection.shape, BF16),
            pltpu.VMEM((2, rows, model), BF16),
            pltpu.VMEM((2 * tokens, model), BF16),
            pltpu.VMEM((2 * tokens, many), BF16),
            pltpu.VMEM((m, m, rows, width), BF16),
            pltpu.VMEM((tokens, width), F32),
            pltpu.VMEM((tokens, width), BF16),
            pltpu.VMEM((heads, HEAD_DIM, HEAD_DIM), F32),
            pltpu.VMEM((1, width), F32),
            pltpu.VMEM((heads, STATE_ROWS, HEAD_DIM), BF16),
            pltpu.VMEM((heads, STATE_ROWS, HEAD_DIM), BF16),
            pltpu.VMEM((heads, HEAD_DIM, HEAD_DIM), BF16),
            pltpu.VMEM((heads, HEAD_DIM, HEAD_DIM), BF16),
            pltpu.VMEM((n, 2 * tokens, depth), BF16),
            pltpu.VMEM((n, tokens, depth), BF16),
            pltpu.VMEM((n, 2, rows, depth), BF16),
            pltpu.VMEM((n, 2, rows, depth), BF16),
            pltpu.VMEM((n, rows, depth), BF16),
            pltpu.VMEM((n, rows, depth), BF16),
            dma((5,)),
            dma((24,)),
            dma((24,)),
            dma((2,)),
            dma((2,)),
            dma((2,)),
            dma((6,)),
            dma((6,)),
            dma((18,)),
            dma((18,)),
            dma((n,)),
            dma((n,)),
            dma((n,)),
            dma((n,)),
            dma((n,)),
            dma((n,)),
        ],
        compiler_params=pltpu.CompilerParams(
            collective_id=0, has_side_effects=True, vmem_limit_bytes=64_000_000
        ),
    )(
        skip,
        query,
        forget,
        value,
        emission,
        slack.reshape(1, width),
        surge,
        gain.reshape(1, width),
        projection,
        row_gain.reshape(1, model),
        switch,
        expansion,
        contraction,
    )


def solution(mesh):
    in_specs = (
        P(("sp", "tp"), None),
        P("sp", "tp"),
        P("sp", "tp"),
        P("sp", "tp"),
        P("sp", "tp"),
        P("tp"),
        P("sp", "tp"),
        P("tp"),
        P(),
        P(),
        P("sp", "tp"),
        P("sp", "tp"),
        P("tp", "sp"),
    )
    n, m = mesh.shape["sp"], mesh.shape["tp"]
    return jax.shard_map(
        functools.partial(on_device_paired if (n, m) == (8, 4) else on_device, n, m),
        mesh=mesh,
        in_specs=in_specs,
        out_specs=P(("sp", "tp"), None),
        check_vma=False,
    )
```

```python
import functools

import jax
import jax.numpy as jnp
from jax import lax
from jax.experimental import pallas as pl
from jax.experimental.pallas import tpu as pltpu
from jax.sharding import PartitionSpec as P

HEAD_DIM = 128
BLOCK = 64
STATE_ROWS = HEAD_DIM + 16
EPSILON = 1e-06
MESH = pl.DeviceIdType.MESH
F32, BF16 = jnp.float32, jnp.bfloat16
LAST = (((1,), (1,)), ((), ()))
FIRST = (((0,), (0,)), ((), ()))


def weight_plan(n, me):
    out = []
    if n != 8:
        for tensor in range(3):
            for d in range(1, n):
                to, source = lax.rem(me + d, n), lax.rem(me + n - d, n)
                out.append((0, tensor, ("D", d, tensor), True, me, to, True, source, None))
        return out
    ny, nz = 2, n // 2
    z, y = me // ny, lax.rem(me, ny)

    def at(place, flip):
        return jnp.clip(place, 0, nz - 1) * ny + (1 - y if flip else y)

    def crossed(place, tensor, way):
        first, last = (1, nz - 1) if way > 0 else (nz - 2, 0)
        return (place == first) | (place == last) if tensor == 0 else place == first

    def inside(place):
        return (place >= 0) & (place < nz)

    for tensor in range(3):
        late = 1 if tensor == 2 else 0
        out.append((0, tensor, ("Y", 0, tensor), True, me, at(z, 1), True, at(z, 1), None))
        for way in (1, -1):
            for k in range(1, nz):
                to, unit = z + way, z + way - way * k
                name, above = (way, k, tensor), (way, k - 1, tensor)
                stage = 0 if k == 1 else k - 1 + late
                out.append(
                    (stage, tensor, name, inside(to) & inside(unit), at(unit, 0), at(to, 0),
                     inside(z - way * k), at(z - way * k, 0), None if k == 1 else above)
                )
                held = inside(z - way * k)
                if k == 1:
                    held = held & jnp.logical_not(crossed(z, tensor, way))
                out.append(
                    (k + late, tensor, ("Y", way * k, tensor), held, at(z - way * k, 0), at(z, 1),
                     held, at(z - way * k, 1), name)
                )
            out.append(
                (2, tensor, ("X", way, tensor), inside(z + way) & crossed(z + way, tensor, way), at(z, 1),
                 at(z + way, 0), crossed(z, tensor, way), at(z - way, 1), ("Y", 0, tensor))
            )
    return out


def kernel(
    n,
    m,
    skip_ref,
    query_ref,
    forget_ref,
    value_ref,
    emission_ref,
    slack_ref,
    surge_ref,
    gain_ref,
    projection_ref,
    row_gain_ref,
    switch_ref,
    expansion_ref,
    contraction_ref,
    out_ref,
    switch_all,
    expansion_all,
    contraction_all,
    projection,
    stream,
    normed,
    hidden,
    mixed,
    outputs,
    decayed_query,
    state,
    offset,
    state_out,
    state_in,
    part,
    from_buddy,
    cross_out,
    cross_in,
    local_sem,
    weight_send,
    weight_recv,
    skip_send,
    skip_recv,
    mixed_send,
    mixed_recv,
    state_send,
    state_recv,
    buddy_send,
    buddy_recv,
    cross_send,
    cross_recv,
):
    sp, tp = lax.axis_index("sp"), lax.axis_index("tp")
    tokens, width = query_ref.shape
    rows, model = skip_ref.shape
    depth, units = switch_ref.shape
    heads = width // HEAD_DIM
    pairs = m // 2

    barrier = pltpu.get_barrier_semaphore()
    for d in range(1, n):
        pl.semaphore_signal(barrier, inc=1, device_id=(lax.rem(sp + d, n), tp), device_id_type=MESH)
    for d in range(1, m):
        pl.semaphore_signal(barrier, inc=1, device_id=(sp, lax.rem(tp + d, m)), device_id_type=MESH)
    pl.semaphore_wait(barrier, n - 1 + m - 1)

    def remote(src, dst, send, recv, device):
        return pltpu.make_async_remote_copy(
            src_ref=src, dst_ref=dst, send_sem=send, recv_sem=recv, device_id=device, device_id_type=MESH
        )

    own_units = (switch_ref, expansion_ref, contraction_ref)

    def unit(tensor, owner):
        if tensor == 2:
            return contraction_all.at[owner]
        held = (switch_all, expansion_all)[tensor]
        return held.at[pl.ds(pl.multiple_of(owner * depth, depth), depth)]

    messages = {}
    for index, (stage, tensor, name, sent, owner, target, arrives, arriving, after) in enumerate(
        weight_plan(n, sp)
    ):
        src = own_units[tensor] if stage == 0 else unit(tensor, owner)
        args = (weight_send.at[index], weight_recv.at[index], (target, tp))
        send = remote(src, unit(tensor, owner), *args)
        arrival = remote(unit(tensor, arriving), unit(tensor, arriving), *args)
        messages[name] = (stage, sent, send, arrives, arrival, after)
    arrived = set()

    def where(condition, action):
        if condition is True:
            action()
        else:
            pl.when(condition)(action)

    def await_unit(name):
        if name not in arrived:
            arrived.add(name)
            where(messages[name][3], messages[name][4].wait_recv)

    def run_stage(wanted):
        for name, (stage, sent, send, _, _, after) in messages.items():
            if stage == wanted:
                if after is not None:
                    await_unit(after)
                where(sent, send.start)

    run_stage(0)

    def rows_of(owner):
        return pl.ds(pl.multiple_of(owner * rows, rows), rows)

    skip_sends, skip_arrivals, mixed_sends, mixed_arrivals = [], [], [], []
    for d in range(1, m):
        source, target = lax.rem(tp + m - d, m), (sp, lax.rem(tp + d, m))
        sems = (skip_send.at[d - 1], skip_recv.at[d - 1], target)
        skip_sends.append(remote(skip_ref, stream.at[rows_of(tp)], *sems))
        skip_arrivals.append(remote(stream.at[rows_of(source)], stream.at[rows_of(source)], *sems))
        sems = (mixed_send.at[d - 1], mixed_recv.at[d - 1], target)
        mixed_sends.append(remote(mixed.at[tp], mixed.at[tp], *sems))
        mixed_arrivals.append(remote(mixed.at[source], mixed.at[source], *sems))
    for copy in skip_sends:
        copy.start()
    local = [
        pltpu.make_async_copy(skip_ref, stream.at[rows_of(tp)], local_sem.at[0]),
        pltpu.make_async_copy(projection_ref, projection, local_sem.at[1]),
    ] + [pltpu.make_async_copy(own_units[t], unit(t, sp), local_sem.at[2 + t]) for t in range(3)]
    for copy in local:
        copy.start()

    state[...] = jnp.zeros_like(state)
    offset[...] = jnp.zeros_like(offset)
    before = lax.broadcasted_iota(jnp.int32, (BLOCK, BLOCK), 0) >= lax.broadcasted_iota(
        jnp.int32, (BLOCK, BLOCK), 1
    )
    lower = before.astype(F32)

    @pl.loop(0, tokens // BLOCK)
    def _(block):
        here = pl.ds(pl.multiple_of(block * BLOCK, BLOCK), BLOCK)
        raw = query_ref[here, :].astype(F32)
        query = raw * jax.nn.sigmoid(raw)
        gate = slack_ref[...] * jax.nn.sigmoid(-forget_ref[here, :].astype(F32))
        log_forget = jnp.log1p(-gate) + surge_ref[here, :]
        total = jnp.dot(lower, log_forget, precision=lax.Precision.HIGHEST, preferred_element_type=F32)
        middle, last = total[BLOCK // 2 : BLOCK // 2 + 1, :], total[BLOCK - 1 :, :]
        left = (query * jnp.exp(total - middle)).astype(BF16)
        right = (gate * jnp.exp(middle - total)).astype(BF16)
        carried = (query * jnp.exp(total)).astype(BF16)
        kept = (gate * jnp.exp(last - total)).astype(BF16)
        decayed_query[here, :] = (query * jnp.exp(total + offset[...])).astype(BF16)
        closing = jnp.exp(last)
        for head in range(heads):
            lanes = slice(head * HEAD_DIM, (head + 1) * HEAD_DIM)
            value = value_ref[here, lanes]
            scores = lax.dot_general(left[:, lanes], right[:, lanes], LAST, preferred_element_type=F32)
            scores = jnp.where(before, scores, 0.0).astype(BF16)
            held = state[head]
            outputs[here, lanes] = jnp.dot(
                scores, value, preferred_element_type=F32
            ) + lax.dot_general(carried[:, lanes], held.astype(BF16), LAST, preferred_element_type=F32)
            state[head] = closing[:, lanes] * held + lax.dot_general(
                value, kept[:, lanes], FIRST, preferred_element_type=F32
            )
        offset[...] += last

    for head in range(heads):
        lanes = slice(head * HEAD_DIM, (head + 1) * HEAD_DIM)
        state_out[head, :HEAD_DIM, :] = state[head].astype(BF16)
        decay = jnp.exp(offset[:, lanes])
        state_out[head, HEAD_DIM:, :] = jnp.broadcast_to(decay, (16, HEAD_DIM)).astype(BF16)
    state_copies = []
    for d in range(1, n):
        copy = remote(
            state_out,
            state_in.at[d - 1],
            state_send.at[d - 1],
            state_recv.at[d - 1],
            (lax.rem(sp + d, n), tp),
        )
        state_copies.append(copy)
        pl.when(sp + d < n)(copy.start)

    run_stage(1)

    for d in range(1, n):
        pl.when(sp >= d)(state_copies[d - 1].wait_recv)
    state[...] = jnp.zeros_like(state)

    @pl.loop(0, sp)
    def _(earlier):
        slot = sp - earlier - 1
        for head in range(heads):
            item = state_in[slot, head].astype(F32)
            state[head] = item[HEAD_DIM : HEAD_DIM + 1, :] * state[head] + item[:HEAD_DIM, :]

    tile = min(256, tokens)

    @pl.loop(0, tokens // tile)
    def _(turn):
        here = pl.ds(pl.multiple_of(turn * tile, tile), tile)
        for head in range(heads):
            lanes = slice(head * HEAD_DIM, (head + 1) * HEAD_DIM)
            full = outputs[here, lanes] + lax.dot_general(
                decayed_query[here, lanes], state[head].astype(BF16), LAST, preferred_element_type=F32
            )
            squares = jnp.mean(full * full, axis=-1, keepdims=True)
            raw = emission_ref[here, lanes].astype(F32)
            scaled = full * lax.rsqrt(squares + EPSILON) * gain_ref[:, lanes]
            mixed[tp, here, lanes] = (scaled * (raw * jax.nn.sigmoid(raw))).astype(BF16)

    for copy in mixed_sends:
        copy.start()
    run_stage(2)
    for copy in local:
        copy.wait()
    for copy in skip_arrivals:
        copy.wait_recv()
    for copy in mixed_arrivals:
        copy.wait_recv()

    @pl.loop(0, tokens // tile)
    def _(turn):
        here = pl.ds(pl.multiple_of(turn * tile, tile), tile)
        total = stream[here, :].astype(F32)
        for source in range(m):
            total += jnp.dot(
                mixed[source, here, :],
                projection[source * width : (source + 1) * width, :],
                preferred_element_type=F32,
            )
        rounded = total.astype(BF16)
        stream[here, :] = rounded
        total = rounded.astype(F32)
        squares = jnp.mean(total * total, axis=-1, keepdims=True)
        normed[here, :] = (total * lax.rsqrt(squares + EPSILON) * row_gain_ref[...]).astype(BF16)

    run_stage(3)
    for name in messages:
        if name[2] < 2:
            await_unit(name)

    core, pair = lax.rem(tp, 2), tp // 2
    buddy = (sp, pair * 2 + 1 - core)

    def half(number, which):
        return part.at[number, pl.ds(pl.multiple_of(which * rows, rows), rows)]

    def gate_and_up(number, owner):
        inputs = pl.ds(pl.multiple_of(owner * 2 * rows, 2 * rows), 2 * rows)

        def columns(lanes):
            value = normed[inputs, :]
            gate = jnp.dot(value, switch_all[:, lanes], preferred_element_type=F32)
            up = jnp.dot(value, expansion_all[:, lanes], preferred_element_type=F32)
            hidden[number, :, lanes] = (gate * jax.nn.sigmoid(gate) * up).astype(BF16)

        @pl.loop(0, units // 256)
        def _(turn):
            columns(pl.ds(pl.multiple_of(turn * 256, 256), 256))

        if units % 256:
            columns(slice(units // 256 * 256, units))

    def down(number):
        @pl.loop(0, n)
        def _(turn):
            lanes = pl.ds(pl.multiple_of(turn * depth, depth), depth)
            part[number, :, lanes] = jnp.dot(
                hidden[number], contraction_all[turn], preferred_element_type=F32
            ).astype(BF16)

        copy = remote(
            half(number, 1 - core),
            from_buddy.at[number],
            buddy_send.at[number],
            buddy_recv.at[number],
            buddy,
        )
        copy.start()
        return copy

    for d in [*range(1, pairs), 0]:
        gate_and_up(d, lax.rem(pair + d, pairs))
    run_stage(4)
    for name in messages:
        await_unit(name)
    tail = []
    for d in range(1, pairs):
        owner = lax.rem(pair + d, pairs)
        copy = down(d)
        copy.wait_recv()
        cross_out[d - 1] = (half(d, core)[...].astype(F32) + from_buddy[d].astype(F32)).astype(BF16)
        cross = remote(
            cross_out.at[d - 1],
            cross_in.at[d - 1],
            cross_send.at[d - 1],
            cross_recv.at[d - 1],
            (sp, owner * 2 + core),
        )
        cross.start()
        tail += [copy, cross]
    copy = down(0)
    copy.wait_recv()
    total = half(0, core)[...].astype(F32) + from_buddy[0].astype(F32) + stream[rows_of(tp), :].astype(F32)
    for d in range(1, pairs):
        tail[2 * d - 1].wait_recv()
        total += cross_in[d - 1].astype(F32)
    out_ref[...] = total.astype(BF16)

    for copy in tail + [copy] + skip_sends + mixed_sends:
        copy.wait_send()
    for _, sent, send, _, _, _ in messages.values():
        where(sent, send.wait_send)
    for d in range(1, n):
        pl.when(sp + d < n)(state_copies[d - 1].wait_send)


def on_device(n, m, *arrays):
    (skip, query, forget, value, emission, slack, surge, gain, projection, row_gain, switch, expansion, contraction) = arrays
    tokens, width = query.shape
    rows, model = skip.shape
    depth, units = switch.shape
    heads, pairs = width // HEAD_DIM, m // 2
    count = 3 * (3 * n // 2 + 3) if n == 8 else 3 * (n - 1)
    vmem, anywhere = pl.BlockSpec(memory_space=pltpu.VMEM), pl.BlockSpec(memory_space=pl.ANY)
    dma = pltpu.SemaphoreType.DMA
    return pl.pallas_call(
        functools.partial(kernel, n, m),
        out_shape=jax.ShapeDtypeStruct((rows, model), BF16),
        in_specs=[anywhere] + [vmem] * 7 + [anywhere, vmem] + [anywhere] * 3,
        out_specs=vmem,
        scratch_shapes=[
            pltpu.VMEM((model, units), BF16),
            pltpu.VMEM((model, units), BF16),
            pltpu.VMEM((n, units, depth), BF16),
            pltpu.VMEM(projection.shape, BF16),
            pltpu.VMEM((tokens, model), BF16),
            pltpu.VMEM((tokens, model), BF16),
            pltpu.VMEM((pairs, 2 * rows, units), BF16),
            pltpu.VMEM((m, tokens, width), BF16),
            pltpu.VMEM((tokens, width), F32),
            pltpu.VMEM((tokens, width), BF16),
            pltpu.VMEM((heads, HEAD_DIM, HEAD_DIM), F32),
            pltpu.VMEM((1, width), F32),
            pltpu.VMEM((heads, STATE_ROWS, HEAD_DIM), BF16),
            pltpu.VMEM((n - 1, heads, STATE_ROWS, HEAD_DIM), BF16),
            pltpu.VMEM((pairs, 2 * rows, model), BF16),
            pltpu.VMEM((pairs, rows, model), BF16),
            pltpu.VMEM((pairs - 1, rows, model), BF16),
            pltpu.VMEM((pairs - 1, rows, model), BF16),
            dma((5,)),
            dma((count,)),
            dma((count,)),
            dma((m - 1,)),
            dma((m - 1,)),
            dma((m - 1,)),
            dma((m - 1,)),
            dma((n - 1,)),
            dma((n - 1,)),
            dma((pairs,)),
            dma((pairs,)),
            dma((pairs - 1,)),
            dma((pairs - 1,)),
        ],
        compiler_params=pltpu.CompilerParams(
            collective_id=0, has_side_effects=True, vmem_limit_bytes=63_000_000
        ),
    )(
        skip,
        query,
        forget,
        value,
        emission,
        slack.reshape(1, width),
        surge,
        gain.reshape(1, width),
        projection,
        row_gain.reshape(1, model),
        switch,
        expansion,
        contraction,
    )


def paired_kernel(
    n,
    m,
    skip_ref,
    query_ref,
    forget_ref,
    value_ref,
    emission_ref,
    slack_ref,
    surge_ref,
    gain_ref,
    projection_ref,
    row_gain_ref,
    switch_ref,
    expansion_ref,
    contraction_ref,
    out_ref,
    switch_half,
    expansion_half,
    contraction_half,
    projection,
    stream,
    normed,
    hidden,
    mixed,
    outputs,
    decayed_query,
    state,
    offset,
    state_out,
    state_in,
    chain_out,
    chain_in,
    part,
    from_buddy,
    cross_out,
    cross_in,
    plane_out,
    plane_in,
    local_sem,
    weight_send,
    weight_recv,
    skip_sem,
    state_sem,
    chain_send,
    chain_recv,
    mixed_send,
    mixed_recv,
    normed_send,
    normed_recv,
    buddy_send,
    buddy_recv,
    cross_send,
    cross_recv,
    plane_send,
    plane_recv,
):
    sp, tp = lax.axis_index("sp"), lax.axis_index("tp")
    tokens, width = query_ref.shape
    rows, model = skip_ref.shape
    depth, units = switch_ref.shape
    heads = width // HEAD_DIM
    few = units // 256 * 128
    many = units - few
    z, y = sp // 2, lax.rem(sp, 2)
    x, core = tp // 2, lax.rem(tp, 2)
    planes = {0: z, 1: z + 1 - 2 * lax.rem(z, 2), 2: lax.rem(z + 2, 4), 3: 3 - z}
    outer = (z == 0) | (z == 3)
    beside = (z * 2 + 1 - y, tp)
    across = (sp, (1 - x) * 2 + core)
    buddy = (sp, x * 2 + 1 - core)
    paired = (planes[1] * 2 + y, tp)

    barrier = pltpu.get_barrier_semaphore()
    for d in range(1, n):
        pl.semaphore_signal(barrier, inc=1, device_id=(lax.rem(sp + d, n), tp), device_id_type=MESH)
    for d in range(1, m):
        pl.semaphore_signal(barrier, inc=1, device_id=(sp, lax.rem(tp + d, m)), device_id_type=MESH)
    def remote(src, dst, send, recv, device):
        return pltpu.make_async_remote_copy(
            src_ref=src, dst_ref=dst, send_sem=send, recv_sem=recv, device_id=device, device_id_type=MESH
        )

    sends = []

    def start(copy):
        copy.start()
        sends.append(copy)

    def by_kind(action):
        pl.when(outer)(lambda: action(False))
        pl.when(jnp.logical_not(outer))(lambda: action(True))

    def own(tensor, big):
        span = pl.ds(few, many) if big else pl.ds(0, few)
        if tensor == 2:
            return contraction_ref.at[span]
        return (switch_ref, expansion_ref)[tensor].at[:, span]

    def held(tensor, owner, big):
        span = pl.ds(0, many if big else few)
        if tensor == 2:
            return contraction_half.at[owner, span]
        place = pl.ds(pl.multiple_of(owner * depth, depth), depth)
        return (switch_half, expansion_half)[tensor].at[place, span]

    def weight(tensor, kind, big):
        sems = (weight_send.at[tensor * 8 + kind], weight_recv.at[tensor * 8 + kind])
        if kind == 0:
            return remote(own(tensor, big), held(tensor, sp, big), *sems, beside)
        if kind <= 3:
            wanted = big if kind == 3 else not big
            return remote(own(tensor, wanted), held(tensor, sp, wanted), *sems, (planes[kind] * 2 + y, tp))
        unit = held(tensor, planes[1 if kind == 7 else kind - 3] * 2 + y, big)
        if kind == 7:
            return remote(unit, unit, sems[0], weight_recv.at[tensor * 8 + 2], (planes[3] * 2 + y, tp))
        return remote(unit, unit, *sems, beside)

    def weight_arrival(tensor, kind, big):
        sems = (weight_send.at[tensor * 8 + kind], weight_recv.at[tensor * 8 + kind])
        if kind == 0:
            owner = z * 2 + 1 - y
        elif kind <= 3:
            owner = planes[kind] * 2 + y
        else:
            owner = planes[kind - 3] * 2 + 1 - y
        unit = held(tensor, owner, big)
        return remote(unit, unit, *sems, beside)

    def local_weight(tensor, big):
        return pltpu.make_async_copy(own(tensor, big), held(tensor, sp, big), local_sem.at[2 + tensor])

    def send_weights(*pairs):
        def action(big):
            for tensor, kind in pairs:
                if big or kind != 2:
                    weight(tensor, kind, big).start()

        by_kind(action)

    def await_weights(*pairs):
        def action(big):
            for tensor, kind in pairs:
                weight_arrival(tensor, kind, big).wait_recv()

        by_kind(action)

    def relay(tensor, kind):
        def action(big):
            weight_arrival(tensor, kind, big).wait_recv()
            weight(tensor, kind + 3, big).start()

        by_kind(action)

    local = [
        pltpu.make_async_copy(skip_ref, stream.at[0], local_sem.at[0]),
        pltpu.make_async_copy(projection_ref, projection, local_sem.at[1]),
    ]
    for copy in local:
        copy.start()

    def prepare(big):
        for tensor in range(3):
            local_weight(tensor, big).start()
        if not big and many > few:
            switch_half[:, few:] = jnp.zeros((model, many - few), BF16)
            expansion_half[:, few:] = jnp.zeros((model, many - few), BF16)
            for owner in range(n):
                contraction_half[owner, few:, :] = jnp.zeros((many - few, depth), BF16)

    by_kind(prepare)

    state[...] = jnp.zeros_like(state)
    offset[...] = jnp.zeros_like(offset)
    before = lax.broadcasted_iota(jnp.int32, (BLOCK, BLOCK), 0) >= lax.broadcasted_iota(
        jnp.int32, (BLOCK, BLOCK), 1
    )
    lower = before.astype(F32)

    def recur(block):
        here = pl.ds(pl.multiple_of(block * BLOCK, BLOCK), BLOCK)
        raw = query_ref[here, :].astype(F32)
        query = raw * jax.nn.sigmoid(raw)
        gate = slack_ref[...] * jax.nn.sigmoid(-forget_ref[here, :].astype(F32))
        log_forget = jnp.log1p(-gate) + surge_ref[here, :]
        total = jnp.dot(lower, log_forget, precision=lax.Precision.HIGHEST, preferred_element_type=F32)
        middle, last = total[BLOCK // 2 : BLOCK // 2 + 1, :], total[BLOCK - 1 :, :]
        left = (query * jnp.exp(total - middle)).astype(BF16)
        right = (gate * jnp.exp(middle - total)).astype(BF16)
        carried = (query * jnp.exp(total)).astype(BF16)
        kept = (gate * jnp.exp(last - total)).astype(BF16)
        decayed_query[here, :] = (query * jnp.exp(total + offset[...])).astype(BF16)
        closing = jnp.exp(last)
        for head in range(heads):
            lanes = slice(head * HEAD_DIM, (head + 1) * HEAD_DIM)
            value = value_ref[here, lanes]
            scores = lax.dot_general(left[:, lanes], right[:, lanes], LAST, preferred_element_type=F32)
            scores = jnp.where(before, scores, 0.0).astype(BF16)
            kept_state = state[head]
            outputs[here, lanes] = jnp.dot(
                scores, value, preferred_element_type=F32
            ) + lax.dot_general(carried[:, lanes], kept_state.astype(BF16), LAST, preferred_element_type=F32)
            state[head] = closing[:, lanes] * kept_state + lax.dot_general(
                value, kept[:, lanes], FIRST, preferred_element_type=F32
            )
        offset[...] += last

    blocks = tokens // BLOCK
    early = blocks // 4
    pl.loop(0, early)(recur)
    pl.semaphore_wait(barrier, n - 1 + m - 1)
    send_weights((0, 0))
    pl.when(z == 0)(lambda: send_weights((0, 3)))
    send_weights((0, 1))
    pl.when(z > 0)(lambda: send_weights((0, 3)))

    @pl.when(z > 1)
    def _():
        send_weights((0, 2))

    @pl.when(z == 3)
    def _():
        send_weights((1, 1), (1, 3))

    start(remote(skip_ref, stream.at[1], skip_sem.at[0], skip_sem.at[1], across))
    pl.loop(early, blocks)(recur)

    for head in range(heads):
        lanes = slice(head * HEAD_DIM, (head + 1) * HEAD_DIM)
        state_out[head, :HEAD_DIM, :] = state[head].astype(BF16)
        decay = jnp.exp(offset[:, lanes])
        state_out[head, HEAD_DIM:, :] = jnp.broadcast_to(decay, (16, HEAD_DIM)).astype(BF16)
    exchange = remote(state_out, state_in, state_sem.at[0], state_sem.at[1], beside)
    start(exchange)
    def chain(distance):
        sems = (chain_send.at[distance - 1], chain_recv.at[distance - 1])
        return remote(chain_out, chain_in.at[distance - 1], *sems, ((z + distance) * 2 + y, tp))

    exchange.wait_recv()
    for head in range(heads):
        lanes = slice(head * HEAD_DIM, (head + 1) * HEAD_DIM)
        decay = jnp.exp(offset[:, lanes])
        other = state_in[head, :HEAD_DIM, :].astype(F32)
        other_decay = state_in[head, HEAD_DIM : HEAD_DIM + 1, :].astype(F32)
        later = jnp.where(y == 0, other, state[head])
        earlier = jnp.where(y == 0, state[head], other)
        later_decay = jnp.where(y == 0, other_decay, decay)
        chain_out[head, :HEAD_DIM, :] = (later_decay * earlier + later).astype(BF16)
        chain_out[head, HEAD_DIM:, :] = jnp.broadcast_to(decay * other_decay, (16, HEAD_DIM)).astype(BF16)
    for distance in range(1, 4):
        pl.when(z + distance < 4)(chain(distance).start)

    def forward(tensor):
        pl.when(jnp.logical_not(outer))(lambda: weight(tensor, 7, True).start())

    pl.when(z == 0)(lambda: send_weights((1, 1), (1, 3)))

    @pl.when((z == 1) | (z == 2))
    def _():
        pl.when(z == 1)(lambda: send_weights((0, 2)))
        send_weights((1, 1))

    send_weights((1, 0))
    for distance in range(1, 4):
        pl.when(z >= distance)(chain(distance).wait_recv)
    for head in range(heads):
        state[head] = jnp.zeros((HEAD_DIM, HEAD_DIM), F32)
        for distance in range(3, 0, -1):

            @pl.when(z >= distance)
            def _():
                item = chain_in[distance - 1, head].astype(F32)
                state[head] = item[HEAD_DIM : HEAD_DIM + 1, :] * state[head] + item[:HEAD_DIM, :]

        @pl.when(y == 1)
        def _():
            item = state_in[head].astype(F32)
            state[head] = item[HEAD_DIM : HEAD_DIM + 1, :] * state[head] + item[:HEAD_DIM, :]

    def mixed_copy(slot, source, block, kind, device):
        place = mixed.at[source, block]
        index = kind * 2 + slot
        return remote(place, place, mixed_send.at[index], mixed_recv.at[index], device)

    for j in range(2):
        side = 1 - x if j else x
        for r in range(2):
            target = 1 - core if r else core
            block = side * 2 + target
            here = pl.ds(pl.multiple_of(block * rows, rows), rows)
            for head in range(heads):
                lanes = slice(head * HEAD_DIM, (head + 1) * HEAD_DIM)
                full = outputs[here, lanes] + lax.dot_general(
                    decayed_query[here, lanes], state[head].astype(BF16), LAST, preferred_element_type=F32
                )
                squares = jnp.mean(full * full, axis=-1, keepdims=True)
                raw = emission_ref[here, lanes].astype(F32)
                scaled = full * lax.rsqrt(squares + EPSILON) * gain_ref[:, lanes]
                mixed[tp, block, :, lanes] = (scaled * (raw * jax.nn.sigmoid(raw))).astype(BF16)
            start(mixed_copy(1 - j, tp, block, r, (sp, (1 - x) * 2 + target)))
            if r:
                start(mixed_copy(j, tp, block, 2, buddy))

    relay(0, 1)
    forward(0)
    pl.when(jnp.logical_not(outer))(lambda: send_weights((1, 3)))
    relay(0, 3)

    @pl.when(jnp.logical_not(outer))
    def _():
        relay(1, 1)
        forward(1)
        send_weights((1, 2))

    for copy in local:
        copy.wait()
    remote(stream.at[1], stream.at[1], skip_sem.at[0], skip_sem.at[1], across).wait_recv()

    pieces = 4
    fine = rows // pieces

    def place_of(plane, side, which):
        return (which * 4 + plane * 2 + side) * rows

    def normed_rows(plane, side, which, piece):
        first, count = place_of(plane, side, which), rows
        if piece is not None:
            first, count = first + piece * fine, fine
        return normed.at[pl.ds(pl.multiple_of(first, fine), count)]

    def normed_copy(index, device, plane, side, which, piece=None, target=None):
        return remote(
            normed_rows(plane, side, which, piece),
            normed_rows(plane if target is None else target, side, which, piece),
            normed_send.at[index],
            normed_recv.at[index],
            device,
        )

    for j in range(2):
        side = 1 - x if j else x
        block = side * 2 + core
        mixed_copy(j, (1 - x) * 2 + core, block, 0, across).wait_recv()
        mixed_copy(j, (1 - x) * 2 + 1 - core, block, 1, across).wait_recv()
        mixed_copy(j, x * 2 + 1 - core, block, 2, across).wait_recv()
        first = place_of(0, side, core)
        for piece in range(2):
            here = slice(piece * rows // 2, (piece + 1) * rows // 2)
            total = stream[j, here, :].astype(F32)
            for source in range(m):
                total += jnp.dot(
                    mixed[source, block, here, :],
                    projection[source * width : (source + 1) * width, :],
                    preferred_element_type=F32,
                )
            rounded = total.astype(BF16)
            stream[j, here, :] = rounded
            total = rounded.astype(F32)
            squares = jnp.mean(total * total, axis=-1, keepdims=True)
            normed[pl.ds(pl.multiple_of(first + piece * rows // 2, rows // 2), rows // 2), :] = (
                total * lax.rsqrt(squares + EPSILON) * row_gain_ref[...]
            ).astype(BF16)
            if j == 0:
                for part_of in range(piece * pieces // 2, (piece + 1) * pieces // 2):
                    start(normed_copy(2 + part_of, paired, 0, side, core, part_of, 1))
        start(normed_copy(j, buddy, 0, side, core))

    pl.when(outer)(lambda: relay(1, 1))
    pl.when(jnp.logical_not(outer))(lambda: send_weights((2, 3)))
    relay(0, 2)

    def tiles(plane, action, side=None):
        count = rows if side is not None else 2 * rows
        first = plane * 2 * rows + (0 if side is None else side * rows)

        @pl.loop(0, 2)
        def _(which):
            here = pl.ds(pl.multiple_of(which * 4 * rows + first, rows), count)

            @pl.loop(0, many // 256)
            def _(turn):
                action(here, pl.ds(pl.multiple_of(turn * 256, 256), 256))

            if many % 256:
                action(here, slice(many // 256 * 256, many))

    def gate(here, lanes):
        value = jnp.dot(normed[here, :], switch_half[:, lanes], preferred_element_type=F32)
        hidden[here, lanes] = (value * jax.nn.sigmoid(value)).astype(BF16)

    def up(here, lanes):
        value = jnp.dot(normed[here, :], expansion_half[:, lanes], preferred_element_type=F32)
        hidden[here, lanes] = (hidden[here, lanes].astype(F32) * value).astype(BF16)

    def normed_arrives(index, plane, side, which, piece=None):
        normed_copy(index, buddy, plane, side, which, piece).wait_recv()

    def pass_on(piece):
        normed_arrives(2 + piece, 1, x, core, piece)
        start(normed_copy(6 + piece, across, 1, x, core, piece))
        start(normed_copy(10 + piece, buddy, 1, x, core, piece))

    def await_local(big):
        for tensor in range(3):
            local_weight(tensor, big).wait()

    by_kind(await_local)
    pass_on(0)
    relay(1, 3)
    pass_on(1)
    for j in range(2):
        normed_arrives(j, 0, 1 - x if j else x, 1 - core)
    await_weights((0, 0), (0, 4), (0, 6), (0, 5))
    tiles(0, gate)
    pass_on(2)
    pl.when(z < 3)(lambda: relay(1, 2))
    pass_on(3)
    pl.when(z == 3)(lambda: relay(1, 2))
    send_weights((2, 1), (2, 0))
    pl.when(outer)(lambda: send_weights((2, 3)))
    send_weights((2, 2))
    for piece in range(pieces):
        normed_arrives(10 + piece, 1, x, 1 - core, piece)
    tiles(1, gate, x)
    await_weights((1, 0), (1, 4), (1, 6), (1, 5))
    tiles(0, up)
    for piece in range(pieces):
        normed_arrives(6 + piece, 1, 1 - x, core, piece)
        start(normed_copy(14 + piece, buddy, 1, 1 - x, core, piece))
    tiles(1, up, x)

    @pl.when(z < 3)
    def _():
        relay(2, 1)
        forward(2)

    for piece in range(pieces):
        normed_arrives(14 + piece, 1, 1 - x, 1 - core, piece)
    tiles(1, gate, 1 - x)
    tiles(1, up, 1 - x)
    pl.when(z == 3)(lambda: relay(2, 1))

    base = z // 2

    def owner_of(turn):
        group, even = turn // 2, lax.rem(turn, 2)
        pair = base + (group // 2) * (1 - 2 * base)
        return (pair * 2 + even) * 2 + y + lax.rem(group, 2) * (1 - 2 * y)

    mine = pl.multiple_of(core * 4 * rows, 4 * rows)
    theirs = pl.multiple_of((1 - core) * 4 * rows, 4 * rows)

    def buddy_copy(turn):
        return remote(
            part.at[turn, pl.ds(theirs, 4 * rows)],
            from_buddy.at[turn],
            buddy_send.at[turn],
            buddy_recv.at[turn],
            buddy,
        )

    def partner(odd):
        return (sp + (paired[0] - sp) * odd, across[1] + (tp - across[1]) * odd)

    def cross_copy(turn):
        sems = (cross_send.at[turn], cross_recv.at[turn])
        return remote(cross_out.at[turn], cross_in.at[turn], *sems, partner(lax.rem(turn, 2)))

    def plane_copy(turn):
        sems = (plane_send.at[turn], plane_recv.at[turn])
        return remote(plane_out.at[turn], plane_in.at[turn], *sems, partner(1 - lax.rem(turn, 2)))

    def share(turn, plane, side):
        place = (plane * 2 + side) * rows
        local_part = part[turn, pl.ds(pl.multiple_of(mine + place, rows), rows), :].astype(F32)
        return local_part + from_buddy[turn, pl.ds(pl.multiple_of(place, rows), rows), :].astype(F32)

    lag_cross, lag_plane = 3, 5

    @pl.loop(0, n + lag_plane)
    def _(step):
        @pl.when(step == 2)
        def _():
            await_weights((2, 0), (2, 4))
            relay(2, 3)

        @pl.when(step == 4)
        def _():
            relay(2, 2)

        @pl.when(step == 6)
        def _():
            await_weights((2, 5), (2, 6))

        @pl.when(step < n)
        def _():
            unit = contraction_half.at[owner_of(step)]

            @pl.loop(0, 4)
            def _(turn):
                here = pl.ds(pl.multiple_of(turn * 2 * rows, 2 * rows), 2 * rows)
                part[step, here, :] = jnp.dot(
                    hidden[here, :], unit[...], preferred_element_type=F32
                ).astype(BF16)

            buddy_copy(step).start()

        @pl.when((step >= 1) & (step < n + 1))
        def _():
            turn = step - 1
            buddy_copy(turn).wait_recv()
            odd = lax.rem(turn, 2)
            cross_out[turn, 0] = share(turn, odd, 1 - x + (2 * x - 1) * odd).astype(BF16)
            cross_out[turn, 1] = share(turn, 1, 1 - x).astype(BF16)
            cross_copy(turn).start()

        @pl.when((step >= lag_cross) & (step < n + lag_cross))
        def _():
            turn = step - lag_cross
            cross_copy(turn).wait_recv()
            odd = lax.rem(turn, 2)
            total = share(turn, 1 - odd, x + (1 - 2 * x) * odd) + cross_in[turn, 1].astype(F32)
            plane_out[turn] = total.astype(BF16)
            plane_copy(turn).start()

        @pl.when(step >= lag_plane)
        def _():
            turn = step - lag_plane
            plane_copy(turn).wait_recv()
            lanes = pl.ds(pl.multiple_of(owner_of(turn) * depth, depth), depth)
            total = stream[0, :, lanes].astype(F32) + share(turn, 0, x)
            total += cross_in[turn, 0].astype(F32) + plane_in[turn].astype(F32)
            out_ref[:, lanes] = total.astype(BF16)

    @pl.loop(0, n)
    def _(turn):
        buddy_copy(turn).wait_send()
        cross_copy(turn).wait_send()
        plane_copy(turn).wait_send()

    for copy in sends:
        copy.wait_send()

    def await_weight_sends(big):
        for tensor in range(3):
            for kind in range(8) if big else (0, 1, 3, 4, 5, 6):
                weight(tensor, kind, big).wait_send()

    by_kind(await_weight_sends)
    for distance in range(1, 4):
        pl.when(z + distance < 4)(chain(distance).wait_send)


def on_device_paired(n, m, *arrays):
    (skip, query, forget, value, emission, slack, surge, gain, projection, row_gain, switch, expansion, contraction) = arrays
    tokens, width = query.shape
    rows, model = skip.shape
    depth, units = switch.shape
    heads = width // HEAD_DIM
    many = units - units // 256 * 128
    vmem, anywhere = pl.BlockSpec(memory_space=pltpu.VMEM), pl.BlockSpec(memory_space=pl.ANY)
    dma = pltpu.SemaphoreType.DMA
    return pl.pallas_call(
        functools.partial(paired_kernel, n, m),
        out_shape=jax.ShapeDtypeStruct((rows, model), BF16),
        in_specs=[anywhere] + [vmem] * 7 + [anywhere, vmem] + [anywhere] * 3,
        out_specs=vmem,
        scratch_shapes=[
            pltpu.VMEM((model, many), BF16),
            pltpu.VMEM((model, many), BF16),
            pltpu.VMEM((n, many, depth), BF16),
            pltpu.VMEM(projection.shape, BF16),
            pltpu.VMEM((2, rows, model), BF16),
            pltpu.VMEM((2 * tokens, model), BF16),
            pltpu.VMEM((2 * tokens, many), BF16),
            pltpu.VMEM((m, m, rows, width), BF16),
            pltpu.VMEM((tokens, width), F32),
            pltpu.VMEM((tokens, width), BF16),
            pltpu.VMEM((heads, HEAD_DIM, HEAD_DIM), F32),
            pltpu.VMEM((1, width), F32),
            pltpu.VMEM((heads, STATE_ROWS, HEAD_DIM), BF16),
            pltpu.VMEM((heads, STATE_ROWS, HEAD_DIM), BF16),
            pltpu.VMEM((heads, STATE_ROWS, HEAD_DIM), BF16),
            pltpu.VMEM((3, heads, STATE_ROWS, HEAD_DIM), BF16),
            pltpu.VMEM((n, 2 * tokens, depth), BF16),
            pltpu.VMEM((n, tokens, depth), BF16),
            pltpu.VMEM((n, 2, rows, depth), BF16),
            pltpu.VMEM((n, 2, rows, depth), BF16),
            pltpu.VMEM((n, rows, depth), BF16),
            pltpu.VMEM((n, rows, depth), BF16),
            dma((5,)),
            dma((24,)),
            dma((24,)),
            dma((2,)),
            dma((2,)),
            dma((3,)),
            dma((3,)),
            dma((6,)),
            dma((6,)),
            dma((18,)),
            dma((18,)),
            dma((n,)),
            dma((n,)),
            dma((n,)),
            dma((n,)),
            dma((n,)),
            dma((n,)),
        ],
        compiler_params=pltpu.CompilerParams(
            collective_id=0, has_side_effects=True, vmem_limit_bytes=64_000_000
        ),
    )(
        skip,
        query,
        forget,
        value,
        emission,
        slack.reshape(1, width),
        surge,
        gain.reshape(1, width),
        projection,
        row_gain.reshape(1, model),
        switch,
        expansion,
        contraction,
    )


def solution(mesh):
    in_specs = (
        P(("sp", "tp"), None),
        P("sp", "tp"),
        P("sp", "tp"),
        P("sp", "tp"),
        P("sp", "tp"),
        P("tp"),
        P("sp", "tp"),
        P("tp"),
        P(),
        P(),
        P("sp", "tp"),
        P("sp", "tp"),
        P("tp", "sp"),
    )
    n, m = mesh.shape["sp"], mesh.shape["tp"]
    return jax.shard_map(
        functools.partial(on_device_paired if (n, m) == (8, 4) else on_device, n, m),
        mesh=mesh,
        in_specs=in_specs,
        out_specs=P(("sp", "tp"), None),
        check_vma=False,
    )
```

```python
import functools

import jax
import jax.numpy as jnp
from jax import lax
from jax.experimental import pallas as pl
from jax.experimental.pallas import tpu as pltpu
from jax.sharding import PartitionSpec as P

HEAD_DIM = 128
BLOCK = 64
STATE_ROWS = HEAD_DIM + 16
EPSILON = 1e-06
MESH = pl.DeviceIdType.MESH
F32, BF16 = jnp.float32, jnp.bfloat16
LAST = (((1,), (1,)), ((), ()))
FIRST = (((0,), (0,)), ((), ()))


def weight_plan(n, me):
    out = []
    if n != 8:
        for tensor in range(3):
            for d in range(1, n):
                to, source = lax.rem(me + d, n), lax.rem(me + n - d, n)
                out.append((0, tensor, ("D", d, tensor), True, me, to, True, source, None))
        return out
    ny, nz = 2, n // 2
    z, y = me // ny, lax.rem(me, ny)

    def at(place, flip):
        return jnp.clip(place, 0, nz - 1) * ny + (1 - y if flip else y)

    def crossed(place, tensor, way):
        first, last = (1, nz - 1) if way > 0 else (nz - 2, 0)
        return (place == first) | (place == last) if tensor == 0 else place == first

    def inside(place):
        return (place >= 0) & (place < nz)

    for tensor in range(3):
        late = 1 if tensor == 2 else 0
        out.append((0, tensor, ("Y", 0, tensor), True, me, at(z, 1), True, at(z, 1), None))
        for way in (1, -1):
            for k in range(1, nz):
                to, unit = z + way, z + way - way * k
                name, above = (way, k, tensor), (way, k - 1, tensor)
                stage = 0 if k == 1 else k - 1 + late
                out.append(
                    (stage, tensor, name, inside(to) & inside(unit), at(unit, 0), at(to, 0),
                     inside(z - way * k), at(z - way * k, 0), None if k == 1 else above)
                )
                held = inside(z - way * k)
                if k == 1:
                    held = held & jnp.logical_not(crossed(z, tensor, way))
                out.append(
                    (k + late, tensor, ("Y", way * k, tensor), held, at(z - way * k, 0), at(z, 1),
                     held, at(z - way * k, 1), name)
                )
            out.append(
                (2, tensor, ("X", way, tensor), inside(z + way) & crossed(z + way, tensor, way), at(z, 1),
                 at(z + way, 0), crossed(z, tensor, way), at(z - way, 1), ("Y", 0, tensor))
            )
    return out


def kernel(
    n,
    m,
    skip_ref,
    query_ref,
    forget_ref,
    value_ref,
    emission_ref,
    slack_ref,
    surge_ref,
    gain_ref,
    projection_ref,
    row_gain_ref,
    switch_ref,
    expansion_ref,
    contraction_ref,
    out_ref,
    switch_all,
    expansion_all,
    contraction_all,
    projection,
    stream,
    normed,
    hidden,
    mixed,
    outputs,
    decayed_query,
    state,
    offset,
    state_out,
    state_in,
    part,
    from_buddy,
    cross_out,
    cross_in,
    local_sem,
    weight_send,
    weight_recv,
    skip_send,
    skip_recv,
    mixed_send,
    mixed_recv,
    state_send,
    state_recv,
    buddy_send,
    buddy_recv,
    cross_send,
    cross_recv,
):
    sp, tp = lax.axis_index("sp"), lax.axis_index("tp")
    tokens, width = query_ref.shape
    rows, model = skip_ref.shape
    depth, units = switch_ref.shape
    heads = width // HEAD_DIM
    pairs = m // 2

    barrier = pltpu.get_barrier_semaphore()
    for d in range(1, n):
        pl.semaphore_signal(barrier, inc=1, device_id=(lax.rem(sp + d, n), tp), device_id_type=MESH)
    for d in range(1, m):
        pl.semaphore_signal(barrier, inc=1, device_id=(sp, lax.rem(tp + d, m)), device_id_type=MESH)
    pl.semaphore_wait(barrier, n - 1 + m - 1)

    def remote(src, dst, send, recv, device):
        return pltpu.make_async_remote_copy(
            src_ref=src, dst_ref=dst, send_sem=send, recv_sem=recv, device_id=device, device_id_type=MESH
        )

    own_units = (switch_ref, expansion_ref, contraction_ref)

    def unit(tensor, owner):
        if tensor == 2:
            return contraction_all.at[owner]
        held = (switch_all, expansion_all)[tensor]
        return held.at[pl.ds(pl.multiple_of(owner * depth, depth), depth)]

    messages = {}
    for index, (stage, tensor, name, sent, owner, target, arrives, arriving, after) in enumerate(
        weight_plan(n, sp)
    ):
        src = own_units[tensor] if stage == 0 else unit(tensor, owner)
        args = (weight_send.at[index], weight_recv.at[index], (target, tp))
        send = remote(src, unit(tensor, owner), *args)
        arrival = remote(unit(tensor, arriving), unit(tensor, arriving), *args)
        messages[name] = (stage, sent, send, arrives, arrival, after)
    arrived = set()

    def where(condition, action):
        if condition is True:
            action()
        else:
            pl.when(condition)(action)

    def await_unit(name):
        if name not in arrived:
            arrived.add(name)
            where(messages[name][3], messages[name][4].wait_recv)

    def run_stage(wanted):
        for name, (stage, sent, send, _, _, after) in messages.items():
            if stage == wanted:
                if after is not None:
                    await_unit(after)
                where(sent, send.start)

    run_stage(0)

    def rows_of(owner):
        return pl.ds(pl.multiple_of(owner * rows, rows), rows)

    skip_sends, skip_arrivals, mixed_sends, mixed_arrivals = [], [], [], []
    for d in range(1, m):
        source, target = lax.rem(tp + m - d, m), (sp, lax.rem(tp + d, m))
        sems = (skip_send.at[d - 1], skip_recv.at[d - 1], target)
        skip_sends.append(remote(skip_ref, stream.at[rows_of(tp)], *sems))
        skip_arrivals.append(remote(stream.at[rows_of(source)], stream.at[rows_of(source)], *sems))
        sems = (mixed_send.at[d - 1], mixed_recv.at[d - 1], target)
        mixed_sends.append(remote(mixed.at[tp], mixed.at[tp], *sems))
        mixed_arrivals.append(remote(mixed.at[source], mixed.at[source], *sems))
    for copy in skip_sends:
        copy.start()
    local = [
        pltpu.make_async_copy(skip_ref, stream.at[rows_of(tp)], local_sem.at[0]),
        pltpu.make_async_copy(projection_ref, projection, local_sem.at[1]),
    ] + [pltpu.make_async_copy(own_units[t], unit(t, sp), local_sem.at[2 + t]) for t in range(3)]
    for copy in local:
        copy.start()

    state[...] = jnp.zeros_like(state)
    offset[...] = jnp.zeros_like(offset)
    before = lax.broadcasted_iota(jnp.int32, (BLOCK, BLOCK), 0) >= lax.broadcasted_iota(
        jnp.int32, (BLOCK, BLOCK), 1
    )
    lower = before.astype(F32)

    @pl.loop(0, tokens // BLOCK)
    def _(block):
        here = pl.ds(pl.multiple_of(block * BLOCK, BLOCK), BLOCK)
        raw = query_ref[here, :].astype(F32)
        query = raw * jax.nn.sigmoid(raw)
        gate = slack_ref[...] * jax.nn.sigmoid(-forget_ref[here, :].astype(F32))
        log_forget = jnp.log1p(-gate) + surge_ref[here, :]
        total = jnp.dot(lower, log_forget, precision=lax.Precision.HIGHEST, preferred_element_type=F32)
        middle, last = total[BLOCK // 2 : BLOCK // 2 + 1, :], total[BLOCK - 1 :, :]
        left = (query * jnp.exp(total - middle)).astype(BF16)
        right = (gate * jnp.exp(middle - total)).astype(BF16)
        carried = (query * jnp.exp(total)).astype(BF16)
        kept = (gate * jnp.exp(last - total)).astype(BF16)
        decayed_query[here, :] = (query * jnp.exp(total + offset[...])).astype(BF16)
        closing = jnp.exp(last)
        for head in range(heads):
            lanes = slice(head * HEAD_DIM, (head + 1) * HEAD_DIM)
            value = value_ref[here, lanes]
            scores = lax.dot_general(left[:, lanes], right[:, lanes], LAST, preferred_element_type=F32)
            scores = jnp.where(before, scores, 0.0).astype(BF16)
            held = state[head]
            outputs[here, lanes] = jnp.dot(
                scores, value, preferred_element_type=F32
            ) + lax.dot_general(carried[:, lanes], held.astype(BF16), LAST, preferred_element_type=F32)
            state[head] = closing[:, lanes] * held + lax.dot_general(
                value, kept[:, lanes], FIRST, preferred_element_type=F32
            )
        offset[...] += last

    for head in range(heads):
        lanes = slice(head * HEAD_DIM, (head + 1) * HEAD_DIM)
        state_out[head, :HEAD_DIM, :] = state[head].astype(BF16)
        decay = jnp.exp(offset[:, lanes])
        state_out[head, HEAD_DIM:, :] = jnp.broadcast_to(decay, (16, HEAD_DIM)).astype(BF16)
    state_copies = []
    for d in range(1, n):
        copy = remote(
            state_out,
            state_in.at[d - 1],
            state_send.at[d - 1],
            state_recv.at[d - 1],
            (lax.rem(sp + d, n), tp),
        )
        state_copies.append(copy)
        pl.when(sp + d < n)(copy.start)

    run_stage(1)

    for d in range(1, n):
        pl.when(sp >= d)(state_copies[d - 1].wait_recv)
    state[...] = jnp.zeros_like(state)

    @pl.loop(0, sp)
    def _(earlier):
        slot = sp - earlier - 1
        for head in range(heads):
            item = state_in[slot, head].astype(F32)
            state[head] = item[HEAD_DIM : HEAD_DIM + 1, :] * state[head] + item[:HEAD_DIM, :]

    tile = min(256, tokens)

    @pl.loop(0, tokens // tile)
    def _(turn):
        here = pl.ds(pl.multiple_of(turn * tile, tile), tile)
        for head in range(heads):
            lanes = slice(head * HEAD_DIM, (head + 1) * HEAD_DIM)
            full = outputs[here, lanes] + lax.dot_general(
                decayed_query[here, lanes], state[head].astype(BF16), LAST, preferred_element_type=F32
            )
            squares = jnp.mean(full * full, axis=-1, keepdims=True)
            raw = emission_ref[here, lanes].astype(F32)
            scaled = full * lax.rsqrt(squares + EPSILON) * gain_ref[:, lanes]
            mixed[tp, here, lanes] = (scaled * (raw * jax.nn.sigmoid(raw))).astype(BF16)

    for copy in mixed_sends:
        copy.start()
    run_stage(2)
    for copy in local:
        copy.wait()
    for copy in skip_arrivals:
        copy.wait_recv()
    for copy in mixed_arrivals:
        copy.wait_recv()

    @pl.loop(0, tokens // tile)
    def _(turn):
        here = pl.ds(pl.multiple_of(turn * tile, tile), tile)
        total = stream[here, :].astype(F32)
        for source in range(m):
            total += jnp.dot(
                mixed[source, here, :],
                projection[source * width : (source + 1) * width, :],
                preferred_element_type=F32,
            )
        rounded = total.astype(BF16)
        stream[here, :] = rounded
        total = rounded.astype(F32)
        squares = jnp.mean(total * total, axis=-1, keepdims=True)
        normed[here, :] = (total * lax.rsqrt(squares + EPSILON) * row_gain_ref[...]).astype(BF16)

    run_stage(3)
    for name in messages:
        if name[2] < 2:
            await_unit(name)

    core, pair = lax.rem(tp, 2), tp // 2
    buddy = (sp, pair * 2 + 1 - core)

    def half(number, which):
        return part.at[number, pl.ds(pl.multiple_of(which * rows, rows), rows)]

    def gate_and_up(number, owner):
        inputs = pl.ds(pl.multiple_of(owner * 2 * rows, 2 * rows), 2 * rows)

        def columns(lanes):
            value = normed[inputs, :]
            gate = jnp.dot(value, switch_all[:, lanes], preferred_element_type=F32)
            up = jnp.dot(value, expansion_all[:, lanes], preferred_element_type=F32)
            hidden[number, :, lanes] = (gate * jax.nn.sigmoid(gate) * up).astype(BF16)

        @pl.loop(0, units // 256)
        def _(turn):
            columns(pl.ds(pl.multiple_of(turn * 256, 256), 256))

        if units % 256:
            columns(slice(units // 256 * 256, units))

    def down(number):
        @pl.loop(0, n)
        def _(turn):
            lanes = pl.ds(pl.multiple_of(turn * depth, depth), depth)
            part[number, :, lanes] = jnp.dot(
                hidden[number], contraction_all[turn], preferred_element_type=F32
            ).astype(BF16)

        copy = remote(
            half(number, 1 - core),
            from_buddy.at[number],
            buddy_send.at[number],
            buddy_recv.at[number],
            buddy,
        )
        copy.start()
        return copy

    for d in [*range(1, pairs), 0]:
        gate_and_up(d, lax.rem(pair + d, pairs))
    run_stage(4)
    for name in messages:
        await_unit(name)
    tail = []
    for d in range(1, pairs):
        owner = lax.rem(pair + d, pairs)
        copy = down(d)
        copy.wait_recv()
        cross_out[d - 1] = (half(d, core)[...].astype(F32) + from_buddy[d].astype(F32)).astype(BF16)
        cross = remote(
            cross_out.at[d - 1],
            cross_in.at[d - 1],
            cross_send.at[d - 1],
            cross_recv.at[d - 1],
            (sp, owner * 2 + core),
        )
        cross.start()
        tail += [copy, cross]
    copy = down(0)
    copy.wait_recv()
    total = half(0, core)[...].astype(F32) + from_buddy[0].astype(F32) + stream[rows_of(tp), :].astype(F32)
    for d in range(1, pairs):
        tail[2 * d - 1].wait_recv()
        total += cross_in[d - 1].astype(F32)
    out_ref[...] = total.astype(BF16)

    for copy in tail + [copy] + skip_sends + mixed_sends:
        copy.wait_send()
    for _, sent, send, _, _, _ in messages.values():
        where(sent, send.wait_send)
    for d in range(1, n):
        pl.when(sp + d < n)(state_copies[d - 1].wait_send)


def on_device(n, m, *arrays):
    (skip, query, forget, value, emission, slack, surge, gain, projection, row_gain, switch, expansion, contraction) = arrays
    tokens, width = query.shape
    rows, model = skip.shape
    depth, units = switch.shape
    heads, pairs = width // HEAD_DIM, m // 2
    count = 3 * (3 * n // 2 + 3) if n == 8 else 3 * (n - 1)
    vmem, anywhere = pl.BlockSpec(memory_space=pltpu.VMEM), pl.BlockSpec(memory_space=pl.ANY)
    dma = pltpu.SemaphoreType.DMA
    return pl.pallas_call(
        functools.partial(kernel, n, m),
        out_shape=jax.ShapeDtypeStruct((rows, model), BF16),
        in_specs=[anywhere] + [vmem] * 7 + [anywhere, vmem] + [anywhere] * 3,
        out_specs=vmem,
        scratch_shapes=[
            pltpu.VMEM((model, units), BF16),
            pltpu.VMEM((model, units), BF16),
            pltpu.VMEM((n, units, depth), BF16),
            pltpu.VMEM(projection.shape, BF16),
            pltpu.VMEM((tokens, model), BF16),
            pltpu.VMEM((tokens, model), BF16),
            pltpu.VMEM((pairs, 2 * rows, units), BF16),
            pltpu.VMEM((m, tokens, width), BF16),
            pltpu.VMEM((tokens, width), F32),
            pltpu.VMEM((tokens, width), BF16),
            pltpu.VMEM((heads, HEAD_DIM, HEAD_DIM), F32),
            pltpu.VMEM((1, width), F32),
            pltpu.VMEM((heads, STATE_ROWS, HEAD_DIM), BF16),
            pltpu.VMEM((n - 1, heads, STATE_ROWS, HEAD_DIM), BF16),
            pltpu.VMEM((pairs, 2 * rows, model), BF16),
            pltpu.VMEM((pairs, rows, model), BF16),
            pltpu.VMEM((pairs - 1, rows, model), BF16),
            pltpu.VMEM((pairs - 1, rows, model), BF16),
            dma((5,)),
            dma((count,)),
            dma((count,)),
            dma((m - 1,)),
            dma((m - 1,)),
            dma((m - 1,)),
            dma((m - 1,)),
            dma((n - 1,)),
            dma((n - 1,)),
            dma((pairs,)),
            dma((pairs,)),
            dma((pairs - 1,)),
            dma((pairs - 1,)),
        ],
        compiler_params=pltpu.CompilerParams(
            collective_id=0, has_side_effects=True, vmem_limit_bytes=63_000_000
        ),
    )(
        skip,
        query,
        forget,
        value,
        emission,
        slack.reshape(1, width),
        surge,
        gain.reshape(1, width),
        projection,
        row_gain.reshape(1, model),
        switch,
        expansion,
        contraction,
    )


def paired_kernel(
    n,
    m,
    skip_ref,
    query_ref,
    forget_ref,
    value_ref,
    emission_ref,
    slack_ref,
    surge_ref,
    gain_ref,
    projection_ref,
    row_gain_ref,
    switch_ref,
    expansion_ref,
    contraction_ref,
    out_ref,
    switch_half,
    expansion_half,
    contraction_half,
    projection,
    stream,
    normed,
    hidden,
    mixed,
    outputs,
    decayed_query,
    state,
    offset,
    state_out,
    state_in,
    chain_out,
    chain_in,
    part,
    from_buddy,
    cross_out,
    cross_in,
    plane_out,
    plane_in,
    local_sem,
    weight_send,
    weight_recv,
    skip_sem,
    state_sem,
    chain_send,
    chain_recv,
    mixed_send,
    mixed_recv,
    normed_send,
    normed_recv,
    buddy_send,
    buddy_recv,
    cross_send,
    cross_recv,
    plane_send,
    plane_recv,
):
    sp, tp = lax.axis_index("sp"), lax.axis_index("tp")
    tokens, width = query_ref.shape
    rows, model = skip_ref.shape
    depth, units = switch_ref.shape
    heads = width // HEAD_DIM
    few = units // 256 * 128
    many = units - few
    z, y = sp // 2, lax.rem(sp, 2)
    x, core = tp // 2, lax.rem(tp, 2)
    planes = {0: z, 1: z + 1 - 2 * lax.rem(z, 2), 2: lax.rem(z + 2, 4), 3: 3 - z}
    outer = (z == 0) | (z == 3)
    beside = (z * 2 + 1 - y, tp)
    across = (sp, (1 - x) * 2 + core)
    buddy = (sp, x * 2 + 1 - core)
    paired = (planes[1] * 2 + y, tp)

    barrier = pltpu.get_barrier_semaphore()
    for d in range(1, n):
        pl.semaphore_signal(barrier, inc=1, device_id=(lax.rem(sp + d, n), tp), device_id_type=MESH)
    for d in range(1, m):
        pl.semaphore_signal(barrier, inc=1, device_id=(sp, lax.rem(tp + d, m)), device_id_type=MESH)
    def remote(src, dst, send, recv, device):
        return pltpu.make_async_remote_copy(
            src_ref=src, dst_ref=dst, send_sem=send, recv_sem=recv, device_id=device, device_id_type=MESH
        )

    sends = []

    def start(copy):
        copy.start()
        sends.append(copy)

    def by_kind(action):
        pl.when(outer)(lambda: action(False))
        pl.when(jnp.logical_not(outer))(lambda: action(True))

    def own(tensor, big):
        span = pl.ds(few, many) if big else pl.ds(0, few)
        if tensor == 2:
            return contraction_ref.at[span]
        return (switch_ref, expansion_ref)[tensor].at[:, span]

    def held(tensor, owner, big):
        span = pl.ds(0, many if big else few)
        if tensor == 2:
            return contraction_half.at[owner, span]
        place = pl.ds(pl.multiple_of(owner * depth, depth), depth)
        return (switch_half, expansion_half)[tensor].at[place, span]

    def weight(tensor, kind, big):
        sems = (weight_send.at[tensor * 8 + kind], weight_recv.at[tensor * 8 + kind])
        if kind == 0:
            return remote(own(tensor, big), held(tensor, sp, big), *sems, beside)
        if kind <= 3:
            wanted = big if kind == 3 else not big
            return remote(own(tensor, wanted), held(tensor, sp, wanted), *sems, (planes[kind] * 2 + y, tp))
        unit = held(tensor, planes[1 if kind == 7 else kind - 3] * 2 + y, big)
        if kind == 7:
            return remote(unit, unit, sems[0], weight_recv.at[tensor * 8 + 2], (planes[3] * 2 + y, tp))
        return remote(unit, unit, *sems, beside)

    def weight_arrival(tensor, kind, big):
        sems = (weight_send.at[tensor * 8 + kind], weight_recv.at[tensor * 8 + kind])
        if kind == 0:
            owner = z * 2 + 1 - y
        elif kind <= 3:
            owner = planes[kind] * 2 + y
        else:
            owner = planes[kind - 3] * 2 + 1 - y
        unit = held(tensor, owner, big)
        return remote(unit, unit, *sems, beside)

    def local_weight(tensor, big):
        return pltpu.make_async_copy(own(tensor, big), held(tensor, sp, big), local_sem.at[2 + tensor])

    def send_weights(*pairs):
        def action(big):
            for tensor, kind in pairs:
                if big or kind != 2:
                    weight(tensor, kind, big).start()

        by_kind(action)

    def await_weights(*pairs):
        def action(big):
            for tensor, kind in pairs:
                weight_arrival(tensor, kind, big).wait_recv()

        by_kind(action)

    def relay(tensor, kind):
        def action(big):
            weight_arrival(tensor, kind, big).wait_recv()
            weight(tensor, kind + 3, big).start()

        by_kind(action)

    local = [
        pltpu.make_async_copy(skip_ref, stream.at[0], local_sem.at[0]),
        pltpu.make_async_copy(projection_ref, projection, local_sem.at[1]),
    ]
    for copy in local:
        copy.start()

    def prepare(big):
        for tensor in range(3):
            local_weight(tensor, big).start()
        if not big and many > few:
            switch_half[:, few:] = jnp.zeros((model, many - few), BF16)
            expansion_half[:, few:] = jnp.zeros((model, many - few), BF16)
            for owner in range(n):
                contraction_half[owner, few:, :] = jnp.zeros((many - few, depth), BF16)

    by_kind(prepare)

    state[...] = jnp.zeros_like(state)
    offset[...] = jnp.zeros_like(offset)
    before = lax.broadcasted_iota(jnp.int32, (BLOCK, BLOCK), 0) >= lax.broadcasted_iota(
        jnp.int32, (BLOCK, BLOCK), 1
    )
    lower = before.astype(F32)

    def recur(block):
        here = pl.ds(pl.multiple_of(block * BLOCK, BLOCK), BLOCK)
        raw = query_ref[here, :].astype(F32)
        query = raw * jax.nn.sigmoid(raw)
        gate = slack_ref[...] * jax.nn.sigmoid(-forget_ref[here, :].astype(F32))
        log_forget = jnp.log1p(-gate) + surge_ref[here, :]
        total = jnp.dot(lower, log_forget, precision=lax.Precision.HIGHEST, preferred_element_type=F32)
        middle, last = total[BLOCK // 2 : BLOCK // 2 + 1, :], total[BLOCK - 1 :, :]
        left = (query * jnp.exp(total - middle)).astype(BF16)
        right = (gate * jnp.exp(middle - total)).astype(BF16)
        carried = (query * jnp.exp(total)).astype(BF16)
        kept = (gate * jnp.exp(last - total)).astype(BF16)
        decayed_query[here, :] = (query * jnp.exp(total + offset[...])).astype(BF16)
        closing = jnp.exp(last)
        for head in range(heads):
            lanes = slice(head * HEAD_DIM, (head + 1) * HEAD_DIM)
            value = value_ref[here, lanes]
            scores = lax.dot_general(left[:, lanes], right[:, lanes], LAST, preferred_element_type=F32)
            scores = jnp.where(before, scores, 0.0).astype(BF16)
            kept_state = state[head]
            outputs[here, lanes] = jnp.dot(
                scores, value, preferred_element_type=F32
            ) + lax.dot_general(carried[:, lanes], kept_state.astype(BF16), LAST, preferred_element_type=F32)
            state[head] = closing[:, lanes] * kept_state + lax.dot_general(
                value, kept[:, lanes], FIRST, preferred_element_type=F32
            )
        offset[...] += last

    blocks = tokens // BLOCK
    early = blocks // 4
    pl.loop(0, early)(recur)
    pl.semaphore_wait(barrier, n - 1 + m - 1)
    send_weights((0, 0))
    pl.when(z == 0)(lambda: send_weights((0, 3)))
    send_weights((0, 1))
    pl.when(z > 0)(lambda: send_weights((0, 3)))

    @pl.when(z > 1)
    def _():
        send_weights((0, 2))

    @pl.when(z == 3)
    def _():
        send_weights((1, 1), (1, 3))

    start(remote(skip_ref, stream.at[1], skip_sem.at[0], skip_sem.at[1], across))
    pl.loop(early, blocks)(recur)

    for head in range(heads):
        lanes = slice(head * HEAD_DIM, (head + 1) * HEAD_DIM)
        state_out[head, :HEAD_DIM, :] = state[head].astype(BF16)
        decay = jnp.exp(offset[:, lanes])
        state_out[head, HEAD_DIM:, :] = jnp.broadcast_to(decay, (16, HEAD_DIM)).astype(BF16)
    exchange = remote(state_out, state_in, state_sem.at[0], state_sem.at[1], beside)
    start(exchange)
    def chain(distance):
        sems = (chain_send.at[distance - 1], chain_recv.at[distance - 1])
        return remote(chain_out, chain_in.at[distance - 1], *sems, ((z + distance) * 2 + y, tp))

    exchange.wait_recv()
    for head in range(heads):
        lanes = slice(head * HEAD_DIM, (head + 1) * HEAD_DIM)
        decay = jnp.exp(offset[:, lanes])
        other = state_in[head, :HEAD_DIM, :].astype(F32)
        other_decay = state_in[head, HEAD_DIM : HEAD_DIM + 1, :].astype(F32)
        later = jnp.where(y == 0, other, state[head])
        earlier = jnp.where(y == 0, state[head], other)
        later_decay = jnp.where(y == 0, other_decay, decay)
        chain_out[head, :HEAD_DIM, :] = (later_decay * earlier + later).astype(BF16)
        chain_out[head, HEAD_DIM:, :] = jnp.broadcast_to(decay * other_decay, (16, HEAD_DIM)).astype(BF16)
    for distance in range(1, 4):
        pl.when(z + distance < 4)(chain(distance).start)

    def forward(tensor):
        pl.when(jnp.logical_not(outer))(lambda: weight(tensor, 7, True).start())

    pl.when(z == 0)(lambda: send_weights((1, 1), (1, 3)))

    @pl.when((z == 1) | (z == 2))
    def _():
        pl.when(z == 1)(lambda: send_weights((0, 2)))
        send_weights((1, 1))

    send_weights((1, 0))
    for distance in range(1, 4):
        pl.when(z >= distance)(chain(distance).wait_recv)
    for head in range(heads):
        state[head] = jnp.zeros((HEAD_DIM, HEAD_DIM), F32)
        for distance in range(3, 0, -1):

            @pl.when(z >= distance)
            def _():
                item = chain_in[distance - 1, head].astype(F32)
                state[head] = item[HEAD_DIM : HEAD_DIM + 1, :] * state[head] + item[:HEAD_DIM, :]

        @pl.when(y == 1)
        def _():
            item = state_in[head].astype(F32)
            state[head] = item[HEAD_DIM : HEAD_DIM + 1, :] * state[head] + item[:HEAD_DIM, :]

    def mixed_copy(slot, source, block, kind, device):
        place = mixed.at[source, block]
        index = kind * 2 + slot
        return remote(place, place, mixed_send.at[index], mixed_recv.at[index], device)

    for j in range(2):
        side = 1 - x if j else x
        for r in range(2):
            target = 1 - core if r else core
            block = side * 2 + target
            here = pl.ds(pl.multiple_of(block * rows, rows), rows)
            for head in range(heads):
                lanes = slice(head * HEAD_DIM, (head + 1) * HEAD_DIM)
                full = outputs[here, lanes] + lax.dot_general(
                    decayed_query[here, lanes], state[head].astype(BF16), LAST, preferred_element_type=F32
                )
                squares = jnp.mean(full * full, axis=-1, keepdims=True)
                raw = emission_ref[here, lanes].astype(F32)
                scaled = full * lax.rsqrt(squares + EPSILON) * gain_ref[:, lanes]
                mixed[tp, block, :, lanes] = (scaled * (raw * jax.nn.sigmoid(raw))).astype(BF16)
            start(mixed_copy(1 - j, tp, block, r, (sp, (1 - x) * 2 + target)))
            if r:
                start(mixed_copy(j, tp, block, 2, buddy))

    relay(0, 1)
    forward(0)
    pl.when(jnp.logical_not(outer))(lambda: send_weights((1, 3)))
    relay(0, 3)

    @pl.when(jnp.logical_not(outer))
    def _():
        relay(1, 1)
        forward(1)
        send_weights((1, 2))

    for copy in local:
        copy.wait()
    remote(stream.at[1], stream.at[1], skip_sem.at[0], skip_sem.at[1], across).wait_recv()

    pieces = 4
    fine = rows // pieces

    def place_of(plane, side, which):
        return (which * 4 + plane * 2 + side) * rows

    def normed_rows(plane, side, which, piece):
        first, count = place_of(plane, side, which), rows
        if piece is not None:
            first, count = first + piece * fine, fine
        return normed.at[pl.ds(pl.multiple_of(first, fine), count)]

    def normed_copy(index, device, plane, side, which, piece=None, target=None):
        return remote(
            normed_rows(plane, side, which, piece),
            normed_rows(plane if target is None else target, side, which, piece),
            normed_send.at[index],
            normed_recv.at[index],
            device,
        )

    for j in range(2):
        side = 1 - x if j else x
        block = side * 2 + core
        mixed_copy(j, (1 - x) * 2 + core, block, 0, across).wait_recv()
        mixed_copy(j, (1 - x) * 2 + 1 - core, block, 1, across).wait_recv()
        mixed_copy(j, x * 2 + 1 - core, block, 2, across).wait_recv()
        first = place_of(0, side, core)
        for piece in range(2):
            here = slice(piece * rows // 2, (piece + 1) * rows // 2)
            total = stream[j, here, :].astype(F32)
            for source in range(m):
                total += jnp.dot(
                    mixed[source, block, here, :],
                    projection[source * width : (source + 1) * width, :],
                    preferred_element_type=F32,
                )
            rounded = total.astype(BF16)
            stream[j, here, :] = rounded
            total = rounded.astype(F32)
            squares = jnp.mean(total * total, axis=-1, keepdims=True)
            normed[pl.ds(pl.multiple_of(first + piece * rows // 2, rows // 2), rows // 2), :] = (
                total * lax.rsqrt(squares + EPSILON) * row_gain_ref[...]
            ).astype(BF16)
            if j == 0:
                for part_of in range(piece * pieces // 2, (piece + 1) * pieces // 2):
                    start(normed_copy(2 + part_of, paired, 0, side, core, part_of, 1))
        start(normed_copy(j, buddy, 0, side, core))

    pl.when(outer)(lambda: relay(1, 1))
    pl.when(jnp.logical_not(outer))(lambda: send_weights((2, 3)))
    relay(0, 2)

    def tiles(plane, action, side=None):
        count = rows if side is not None else 2 * rows
        first = plane * 2 * rows + (0 if side is None else side * rows)

        @pl.loop(0, 2)
        def _(which):
            here = pl.ds(pl.multiple_of(which * 4 * rows + first, rows), count)

            @pl.loop(0, many // 256)
            def _(turn):
                action(here, pl.ds(pl.multiple_of(turn * 256, 256), 256))

            if many % 256:
                action(here, slice(many // 256 * 256, many))

    def gate(here, lanes):
        value = jnp.dot(normed[here, :], switch_half[:, lanes], preferred_element_type=F32)
        hidden[here, lanes] = (value * jax.nn.sigmoid(value)).astype(BF16)

    def up(here, lanes):
        value = jnp.dot(normed[here, :], expansion_half[:, lanes], preferred_element_type=F32)
        hidden[here, lanes] = (hidden[here, lanes].astype(F32) * value).astype(BF16)

    def normed_arrives(index, plane, side, which, piece=None):
        normed_copy(index, buddy, plane, side, which, piece).wait_recv()

    def pass_on(piece):
        normed_arrives(2 + piece, 1, x, core, piece)
        start(normed_copy(6 + piece, across, 1, x, core, piece))
        start(normed_copy(10 + piece, buddy, 1, x, core, piece))

    def await_local(big):
        for tensor in range(3):
            local_weight(tensor, big).wait()

    by_kind(await_local)
    pass_on(0)
    relay(1, 3)
    pass_on(1)
    for j in range(2):
        normed_arrives(j, 0, 1 - x if j else x, 1 - core)
    await_weights((0, 0), (0, 4), (0, 6), (0, 5))
    tiles(0, gate)
    pass_on(2)
    pl.when(z < 3)(lambda: relay(1, 2))
    pass_on(3)
    pl.when(z == 3)(lambda: relay(1, 2))
    send_weights((2, 1), (2, 0))
    pl.when(outer)(lambda: send_weights((2, 3)))
    send_weights((2, 2))
    for piece in range(pieces):
        normed_arrives(10 + piece, 1, x, 1 - core, piece)
    tiles(1, gate, x)
    def collect():
        for piece in range(pieces):
            normed_arrives(6 + piece, 1, 1 - x, core, piece)
            normed_copy(14 + piece, buddy, 1, 1 - x, core, piece).start()

    def collected():
        for piece in range(pieces):
            normed_arrives(14 + piece, 1, 1 - x, 1 - core, piece)

    @pl.when(z == 3)
    def _():
        collect()
        collected()
        tiles(1, gate, 1 - x)
        await_weights((1, 0), (1, 4), (1, 6), (1, 5))
        tiles(0, up)
        tiles(1, up)

    @pl.when(z < 3)
    def _():
        await_weights((1, 0), (1, 4), (1, 6), (1, 5))
        tiles(0, up)
        collect()
        tiles(1, up, x)

        @pl.when(z > 0)
        def _():
            relay(2, 1)
            weight(2, 7, True).start()
            relay(2, 3)

        collected()
        tiles(1, gate, 1 - x)
        tiles(1, up, 1 - x)

    base = z // 2

    def owner_of(turn):
        far, second = turn // 4, lax.rem(turn, 4) // 2
        pair = base + far * (1 - 2 * base)
        plane = 1 + pair + (1 - lax.rem(far + second, 2)) * (2 * pair - 1)
        return plane * 2 + y + lax.rem(turn, 2) * (1 - 2 * y)

    mine = pl.multiple_of(core * 4 * rows, 4 * rows)
    theirs = pl.multiple_of((1 - core) * 4 * rows, 4 * rows)

    def buddy_copy(turn):
        return remote(
            part.at[turn, pl.ds(theirs, 4 * rows)],
            from_buddy.at[turn],
            buddy_send.at[turn],
            buddy_recv.at[turn],
            buddy,
        )

    def partner(odd):
        return (sp + (paired[0] - sp) * odd, across[1] + (tp - across[1]) * odd)

    def cross_copy(turn):
        sems = (cross_send.at[turn], cross_recv.at[turn])
        return remote(cross_out.at[turn], cross_in.at[turn], *sems, partner(lax.rem(turn, 2)))

    def plane_copy(turn):
        sems = (plane_send.at[turn], plane_recv.at[turn])
        return remote(plane_out.at[turn], plane_in.at[turn], *sems, partner(1 - lax.rem(turn, 2)))

    def share(turn, plane, side):
        place = (plane * 2 + side) * rows
        local_part = part[turn, pl.ds(pl.multiple_of(mine + place, rows), rows), :].astype(F32)
        return local_part + from_buddy[turn, pl.ds(pl.multiple_of(place, rows), rows), :].astype(F32)

    lag_cross, lag_plane = 3, 5

    @pl.loop(0, n + lag_plane)
    def _(step):
        @pl.when((step >= 1) & (step < n + 1))
        def _():
            turn = step - 1
            buddy_copy(turn).wait_recv()
            odd = lax.rem(turn, 2)
            cross_out[turn, 0] = share(turn, odd, 1 - x + (2 * x - 1) * odd).astype(BF16)
            cross_out[turn, 1] = share(turn, 1, 1 - x).astype(BF16)
            cross_copy(turn).start()

        def ready(at, outer_needs, inner_needs):
            def action(big):
                for kind in inner_needs if big else outer_needs:
                    if kind in (1, 2, 3):
                        weight_arrival(2, kind, big).wait_recv()
                        weight(2, kind + 3, big).start()
                    else:
                        weight_arrival(2, kind, big).wait_recv()

            pl.when(step == at)(lambda: by_kind(action))

        ready(1, (0, 1), (4,))
        ready(2, (2,), ())
        ready(3, (4, 3), (0, 2))
        ready(5, (5,), (6,))
        ready(7, (6,), (5,))

        @pl.when(step < n)
        def _():
            unit = contraction_half.at[owner_of(step)]

            @pl.loop(0, 4)
            def _(turn):
                here = pl.ds(pl.multiple_of(turn * 2 * rows, 2 * rows), 2 * rows)
                part[step, here, :] = jnp.dot(
                    hidden[here, :], unit[...], preferred_element_type=F32
                ).astype(BF16)

            buddy_copy(step).start()

        @pl.when((step >= lag_cross) & (step < n + lag_cross))
        def _():
            turn = step - lag_cross
            cross_copy(turn).wait_recv()
            odd = lax.rem(turn, 2)
            total = share(turn, 1 - odd, x + (1 - 2 * x) * odd) + cross_in[turn, 1].astype(F32)
            plane_out[turn] = total.astype(BF16)
            plane_copy(turn).start()

        @pl.when(step >= lag_plane)
        def _():
            turn = step - lag_plane
            plane_copy(turn).wait_recv()
            lanes = pl.ds(pl.multiple_of(owner_of(turn) * depth, depth), depth)
            total = stream[0, :, lanes].astype(F32) + share(turn, 0, x)
            total += cross_in[turn, 0].astype(F32) + plane_in[turn].astype(F32)
            out_ref[:, lanes] = total.astype(BF16)

    @pl.loop(0, n)
    def _(turn):
        buddy_copy(turn).wait_send()
        cross_copy(turn).wait_send()
        plane_copy(turn).wait_send()

    for copy in sends:
        copy.wait_send()
    for piece in range(pieces):
        normed_copy(14 + piece, buddy, 1, 1 - x, core, piece).wait_send()

    def await_weight_sends(big):
        for tensor in range(3):
            for kind in range(8) if big else (0, 1, 3, 4, 5, 6):
                weight(tensor, kind, big).wait_send()

    by_kind(await_weight_sends)
    for distance in range(1, 4):
        pl.when(z + distance < 4)(chain(distance).wait_send)


def on_device_paired(n, m, *arrays):
    (skip, query, forget, value, emission, slack, surge, gain, projection, row_gain, switch, expansion, contraction) = arrays
    tokens, width = query.shape
    rows, model = skip.shape
    depth, units = switch.shape
    heads = width // HEAD_DIM
    many = units - units // 256 * 128
    vmem, anywhere = pl.BlockSpec(memory_space=pltpu.VMEM), pl.BlockSpec(memory_space=pl.ANY)
    dma = pltpu.SemaphoreType.DMA
    return pl.pallas_call(
        functools.partial(paired_kernel, n, m),
        out_shape=jax.ShapeDtypeStruct((rows, model), BF16),
        in_specs=[anywhere] + [vmem] * 7 + [anywhere, vmem] + [anywhere] * 3,
        out_specs=vmem,
        scratch_shapes=[
            pltpu.VMEM((model, many), BF16),
            pltpu.VMEM((model, many), BF16),
            pltpu.VMEM((n, many, depth), BF16),
            pltpu.VMEM(projection.shape, BF16),
            pltpu.VMEM((2, rows, model), BF16),
            pltpu.VMEM((2 * tokens, model), BF16),
            pltpu.VMEM((2 * tokens, many), BF16),
            pltpu.VMEM((m, m, rows, width), BF16),
            pltpu.VMEM((tokens, width), F32),
            pltpu.VMEM((tokens, width), BF16),
            pltpu.VMEM((heads, HEAD_DIM, HEAD_DIM), F32),
            pltpu.VMEM((1, width), F32),
            pltpu.VMEM((heads, STATE_ROWS, HEAD_DIM), BF16),
            pltpu.VMEM((heads, STATE_ROWS, HEAD_DIM), BF16),
            pltpu.VMEM((heads, STATE_ROWS, HEAD_DIM), BF16),
            pltpu.VMEM((3, heads, STATE_ROWS, HEAD_DIM), BF16),
            pltpu.VMEM((n, 2 * tokens, depth), BF16),
            pltpu.VMEM((n, tokens, depth), BF16),
            pltpu.VMEM((n, 2, rows, depth), BF16),
            pltpu.VMEM((n, 2, rows, depth), BF16),
            pltpu.VMEM((n, rows, depth), BF16),
            pltpu.VMEM((n, rows, depth), BF16),
            dma((5,)),
            dma((24,)),
            dma((24,)),
            dma((2,)),
            dma((2,)),
            dma((3,)),
            dma((3,)),
            dma((6,)),
            dma((6,)),
            dma((18,)),
            dma((18,)),
            dma((n,)),
            dma((n,)),
            dma((n,)),
            dma((n,)),
            dma((n,)),
            dma((n,)),
        ],
        compiler_params=pltpu.CompilerParams(
            collective_id=0, has_side_effects=True, vmem_limit_bytes=64_000_000
        ),
    )(
        skip,
        query,
        forget,
        value,
        emission,
        slack.reshape(1, width),
        surge,
        gain.reshape(1, width),
        projection,
        row_gain.reshape(1, model),
        switch,
        expansion,
        contraction,
    )


def solution(mesh):
    in_specs = (
        P(("sp", "tp"), None),
        P("sp", "tp"),
        P("sp", "tp"),
        P("sp", "tp"),
        P("sp", "tp"),
        P("tp"),
        P("sp", "tp"),
        P("tp"),
        P(),
        P(),
        P("sp", "tp"),
        P("sp", "tp"),
        P("tp", "sp"),
    )
    n, m = mesh.shape["sp"], mesh.shape["tp"]
    return jax.shard_map(
        functools.partial(on_device_paired if (n, m) == (8, 4) else on_device, n, m),
        mesh=mesh,
        in_specs=in_specs,
        out_specs=P(("sp", "tp"), None),
        check_vma=False,
    )
```

```python
import functools

import jax
import jax.numpy as jnp
from jax import lax
from jax.experimental import pallas as pl
from jax.experimental.pallas import tpu as pltpu
from jax.sharding import PartitionSpec as P

HEAD_DIM = 128
BLOCK = 64
STATE_ROWS = HEAD_DIM + 16
EPSILON = 1e-06
MESH = pl.DeviceIdType.MESH
F32, BF16 = jnp.float32, jnp.bfloat16
LAST = (((1,), (1,)), ((), ()))
FIRST = (((0,), (0,)), ((), ()))


def weight_plan(n, me):
    out = []
    if n != 8:
        for tensor in range(3):
            for d in range(1, n):
                to, source = lax.rem(me + d, n), lax.rem(me + n - d, n)
                out.append((0, tensor, ("D", d, tensor), True, me, to, True, source, None))
        return out
    ny, nz = 2, n // 2
    z, y = me // ny, lax.rem(me, ny)

    def at(place, flip):
        return jnp.clip(place, 0, nz - 1) * ny + (1 - y if flip else y)

    def crossed(place, tensor, way):
        first, last = (1, nz - 1) if way > 0 else (nz - 2, 0)
        return (place == first) | (place == last) if tensor == 0 else place == first

    def inside(place):
        return (place >= 0) & (place < nz)

    for tensor in range(3):
        late = 1 if tensor == 2 else 0
        out.append((0, tensor, ("Y", 0, tensor), True, me, at(z, 1), True, at(z, 1), None))
        for way in (1, -1):
            for k in range(1, nz):
                to, unit = z + way, z + way - way * k
                name, above = (way, k, tensor), (way, k - 1, tensor)
                stage = 0 if k == 1 else k - 1 + late
                out.append(
                    (stage, tensor, name, inside(to) & inside(unit), at(unit, 0), at(to, 0),
                     inside(z - way * k), at(z - way * k, 0), None if k == 1 else above)
                )
                held = inside(z - way * k)
                if k == 1:
                    held = held & jnp.logical_not(crossed(z, tensor, way))
                out.append(
                    (k + late, tensor, ("Y", way * k, tensor), held, at(z - way * k, 0), at(z, 1),
                     held, at(z - way * k, 1), name)
                )
            out.append(
                (2, tensor, ("X", way, tensor), inside(z + way) & crossed(z + way, tensor, way), at(z, 1),
                 at(z + way, 0), crossed(z, tensor, way), at(z - way, 1), ("Y", 0, tensor))
            )
    return out


def kernel(
    n,
    m,
    skip_ref,
    query_ref,
    forget_ref,
    value_ref,
    emission_ref,
    slack_ref,
    surge_ref,
    gain_ref,
    projection_ref,
    row_gain_ref,
    switch_ref,
    expansion_ref,
    contraction_ref,
    out_ref,
    switch_all,
    expansion_all,
    contraction_all,
    projection,
    stream,
    normed,
    hidden,
    mixed,
    outputs,
    decayed_query,
    state,
    offset,
    state_out,
    state_in,
    part,
    from_buddy,
    cross_out,
    cross_in,
    local_sem,
    weight_send,
    weight_recv,
    skip_send,
    skip_recv,
    mixed_send,
    mixed_recv,
    state_send,
    state_recv,
    buddy_send,
    buddy_recv,
    cross_send,
    cross_recv,
):
    sp, tp = lax.axis_index("sp"), lax.axis_index("tp")
    tokens, width = query_ref.shape
    rows, model = skip_ref.shape
    depth, units = switch_ref.shape
    heads = width // HEAD_DIM
    pairs = m // 2

    barrier = pltpu.get_barrier_semaphore()
    for d in range(1, n):
        pl.semaphore_signal(barrier, inc=1, device_id=(lax.rem(sp + d, n), tp), device_id_type=MESH)
    for d in range(1, m):
        pl.semaphore_signal(barrier, inc=1, device_id=(sp, lax.rem(tp + d, m)), device_id_type=MESH)
    pl.semaphore_wait(barrier, n - 1 + m - 1)

    def remote(src, dst, send, recv, device):
        return pltpu.make_async_remote_copy(
            src_ref=src, dst_ref=dst, send_sem=send, recv_sem=recv, device_id=device, device_id_type=MESH
        )

    own_units = (switch_ref, expansion_ref, contraction_ref)

    def unit(tensor, owner):
        if tensor == 2:
            return contraction_all.at[owner]
        held = (switch_all, expansion_all)[tensor]
        return held.at[pl.ds(pl.multiple_of(owner * depth, depth), depth)]

    messages = {}
    for index, (stage, tensor, name, sent, owner, target, arrives, arriving, after) in enumerate(
        weight_plan(n, sp)
    ):
        src = own_units[tensor] if stage == 0 else unit(tensor, owner)
        args = (weight_send.at[index], weight_recv.at[index], (target, tp))
        send = remote(src, unit(tensor, owner), *args)
        arrival = remote(unit(tensor, arriving), unit(tensor, arriving), *args)
        messages[name] = (stage, sent, send, arrives, arrival, after)
    arrived = set()

    def where(condition, action):
        if condition is True:
            action()
        else:
            pl.when(condition)(action)

    def await_unit(name):
        if name not in arrived:
            arrived.add(name)
            where(messages[name][3], messages[name][4].wait_recv)

    def run_stage(wanted):
        for name, (stage, sent, send, _, _, after) in messages.items():
            if stage == wanted:
                if after is not None:
                    await_unit(after)
                where(sent, send.start)

    run_stage(0)

    def rows_of(owner):
        return pl.ds(pl.multiple_of(owner * rows, rows), rows)

    skip_sends, skip_arrivals, mixed_sends, mixed_arrivals = [], [], [], []
    for d in range(1, m):
        source, target = lax.rem(tp + m - d, m), (sp, lax.rem(tp + d, m))
        sems = (skip_send.at[d - 1], skip_recv.at[d - 1], target)
        skip_sends.append(remote(skip_ref, stream.at[rows_of(tp)], *sems))
        skip_arrivals.append(remote(stream.at[rows_of(source)], stream.at[rows_of(source)], *sems))
        sems = (mixed_send.at[d - 1], mixed_recv.at[d - 1], target)
        mixed_sends.append(remote(mixed.at[tp], mixed.at[tp], *sems))
        mixed_arrivals.append(remote(mixed.at[source], mixed.at[source], *sems))
    for copy in skip_sends:
        copy.start()
    local = [
        pltpu.make_async_copy(skip_ref, stream.at[rows_of(tp)], local_sem.at[0]),
        pltpu.make_async_copy(projection_ref, projection, local_sem.at[1]),
    ] + [pltpu.make_async_copy(own_units[t], unit(t, sp), local_sem.at[2 + t]) for t in range(3)]
    for copy in local:
        copy.start()

    state[...] = jnp.zeros_like(state)
    offset[...] = jnp.zeros_like(offset)
    before = lax.broadcasted_iota(jnp.int32, (BLOCK, BLOCK), 0) >= lax.broadcasted_iota(
        jnp.int32, (BLOCK, BLOCK), 1
    )
    lower = before.astype(F32)

    @pl.loop(0, tokens // BLOCK)
    def _(block):
        here = pl.ds(pl.multiple_of(block * BLOCK, BLOCK), BLOCK)
        raw = query_ref[here, :].astype(F32)
        query = raw * jax.nn.sigmoid(raw)
        gate = slack_ref[...] * jax.nn.sigmoid(-forget_ref[here, :].astype(F32))
        log_forget = jnp.log1p(-gate) + surge_ref[here, :]
        total = jnp.dot(lower, log_forget, precision=lax.Precision.HIGHEST, preferred_element_type=F32)
        middle, last = total[BLOCK // 2 : BLOCK // 2 + 1, :], total[BLOCK - 1 :, :]
        left = (query * jnp.exp(total - middle)).astype(BF16)
        right = (gate * jnp.exp(middle - total)).astype(BF16)
        carried = (query * jnp.exp(total)).astype(BF16)
        kept = (gate * jnp.exp(last - total)).astype(BF16)
        decayed_query[here, :] = (query * jnp.exp(total + offset[...])).astype(BF16)
        closing = jnp.exp(last)
        for head in range(heads):
            lanes = slice(head * HEAD_DIM, (head + 1) * HEAD_DIM)
            value = value_ref[here, lanes]
            scores = lax.dot_general(left[:, lanes], right[:, lanes], LAST, preferred_element_type=F32)
            scores = jnp.where(before, scores, 0.0).astype(BF16)
            held = state[head]
            outputs[here, lanes] = jnp.dot(
                scores, value, preferred_element_type=F32
            ) + lax.dot_general(carried[:, lanes], held.astype(BF16), LAST, preferred_element_type=F32)
            state[head] = closing[:, lanes] * held + lax.dot_general(
                value, kept[:, lanes], FIRST, preferred_element_type=F32
            )
        offset[...] += last

    for head in range(heads):
        lanes = slice(head * HEAD_DIM, (head + 1) * HEAD_DIM)
        state_out[head, :HEAD_DIM, :] = state[head].astype(BF16)
        decay = jnp.exp(offset[:, lanes])
        state_out[head, HEAD_DIM:, :] = jnp.broadcast_to(decay, (16, HEAD_DIM)).astype(BF16)
    state_copies = []
    for d in range(1, n):
        copy = remote(
            state_out,
            state_in.at[d - 1],
            state_send.at[d - 1],
            state_recv.at[d - 1],
            (lax.rem(sp + d, n), tp),
        )
        state_copies.append(copy)
        pl.when(sp + d < n)(copy.start)

    run_stage(1)

    for d in range(1, n):
        pl.when(sp >= d)(state_copies[d - 1].wait_recv)
    state[...] = jnp.zeros_like(state)

    @pl.loop(0, sp)
    def _(earlier):
        slot = sp - earlier - 1
        for head in range(heads):
            item = state_in[slot, head].astype(F32)
            state[head] = item[HEAD_DIM : HEAD_DIM + 1, :] * state[head] + item[:HEAD_DIM, :]

    tile = min(256, tokens)

    @pl.loop(0, tokens // tile)
    def _(turn):
        here = pl.ds(pl.multiple_of(turn * tile, tile), tile)
        for head in range(heads):
            lanes = slice(head * HEAD_DIM, (head + 1) * HEAD_DIM)
            full = outputs[here, lanes] + lax.dot_general(
                decayed_query[here, lanes], state[head].astype(BF16), LAST, preferred_element_type=F32
            )
            squares = jnp.mean(full * full, axis=-1, keepdims=True)
            raw = emission_ref[here, lanes].astype(F32)
            scaled = full * lax.rsqrt(squares + EPSILON) * gain_ref[:, lanes]
            mixed[tp, here, lanes] = (scaled * (raw * jax.nn.sigmoid(raw))).astype(BF16)

    for copy in mixed_sends:
        copy.start()
    run_stage(2)
    for copy in local:
        copy.wait()
    for copy in skip_arrivals:
        copy.wait_recv()
    for copy in mixed_arrivals:
        copy.wait_recv()

    @pl.loop(0, tokens // tile)
    def _(turn):
        here = pl.ds(pl.multiple_of(turn * tile, tile), tile)
        total = stream[here, :].astype(F32)
        for source in range(m):
            total += jnp.dot(
                mixed[source, here, :],
                projection[source * width : (source + 1) * width, :],
                preferred_element_type=F32,
            )
        rounded = total.astype(BF16)
        stream[here, :] = rounded
        total = rounded.astype(F32)
        squares = jnp.mean(total * total, axis=-1, keepdims=True)
        normed[here, :] = (total * lax.rsqrt(squares + EPSILON) * row_gain_ref[...]).astype(BF16)

    run_stage(3)
    for name in messages:
        if name[2] < 2:
            await_unit(name)

    core, pair = lax.rem(tp, 2), tp // 2
    buddy = (sp, pair * 2 + 1 - core)

    def half(number, which):
        return part.at[number, pl.ds(pl.multiple_of(which * rows, rows), rows)]

    def gate_and_up(number, owner):
        inputs = pl.ds(pl.multiple_of(owner * 2 * rows, 2 * rows), 2 * rows)

        def columns(lanes):
            value = normed[inputs, :]
            gate = jnp.dot(value, switch_all[:, lanes], preferred_element_type=F32)
            up = jnp.dot(value, expansion_all[:, lanes], preferred_element_type=F32)
            hidden[number, :, lanes] = (gate * jax.nn.sigmoid(gate) * up).astype(BF16)

        @pl.loop(0, units // 256)
        def _(turn):
            columns(pl.ds(pl.multiple_of(turn * 256, 256), 256))

        if units % 256:
            columns(slice(units // 256 * 256, units))

    def down(number):
        @pl.loop(0, n)
        def _(turn):
            lanes = pl.ds(pl.multiple_of(turn * depth, depth), depth)
            part[number, :, lanes] = jnp.dot(
                hidden[number], contraction_all[turn], preferred_element_type=F32
            ).astype(BF16)

        copy = remote(
            half(number, 1 - core),
            from_buddy.at[number],
            buddy_send.at[number],
            buddy_recv.at[number],
            buddy,
        )
        copy.start()
        return copy

    for d in [*range(1, pairs), 0]:
        gate_and_up(d, lax.rem(pair + d, pairs))
    run_stage(4)
    for name in messages:
        await_unit(name)
    tail = []
    for d in range(1, pairs):
        owner = lax.rem(pair + d, pairs)
        copy = down(d)
        copy.wait_recv()
        cross_out[d - 1] = (half(d, core)[...].astype(F32) + from_buddy[d].astype(F32)).astype(BF16)
        cross = remote(
            cross_out.at[d - 1],
            cross_in.at[d - 1],
            cross_send.at[d - 1],
            cross_recv.at[d - 1],
            (sp, owner * 2 + core),
        )
        cross.start()
        tail += [copy, cross]
    copy = down(0)
    copy.wait_recv()
    total = half(0, core)[...].astype(F32) + from_buddy[0].astype(F32) + stream[rows_of(tp), :].astype(F32)
    for d in range(1, pairs):
        tail[2 * d - 1].wait_recv()
        total += cross_in[d - 1].astype(F32)
    out_ref[...] = total.astype(BF16)

    for copy in tail + [copy] + skip_sends + mixed_sends:
        copy.wait_send()
    for _, sent, send, _, _, _ in messages.values():
        where(sent, send.wait_send)
    for d in range(1, n):
        pl.when(sp + d < n)(state_copies[d - 1].wait_send)


def on_device(n, m, *arrays):
    (skip, query, forget, value, emission, slack, surge, gain, projection, row_gain, switch, expansion, contraction) = arrays
    tokens, width = query.shape
    rows, model = skip.shape
    depth, units = switch.shape
    heads, pairs = width // HEAD_DIM, m // 2
    count = 3 * (3 * n // 2 + 3) if n == 8 else 3 * (n - 1)
    vmem, anywhere = pl.BlockSpec(memory_space=pltpu.VMEM), pl.BlockSpec(memory_space=pl.ANY)
    dma = pltpu.SemaphoreType.DMA
    return pl.pallas_call(
        functools.partial(kernel, n, m),
        out_shape=jax.ShapeDtypeStruct((rows, model), BF16),
        in_specs=[anywhere] + [vmem] * 7 + [anywhere, vmem] + [anywhere] * 3,
        out_specs=vmem,
        scratch_shapes=[
            pltpu.VMEM((model, units), BF16),
            pltpu.VMEM((model, units), BF16),
            pltpu.VMEM((n, units, depth), BF16),
            pltpu.VMEM(projection.shape, BF16),
            pltpu.VMEM((tokens, model), BF16),
            pltpu.VMEM((tokens, model), BF16),
            pltpu.VMEM((pairs, 2 * rows, units), BF16),
            pltpu.VMEM((m, tokens, width), BF16),
            pltpu.VMEM((tokens, width), F32),
            pltpu.VMEM((tokens, width), BF16),
            pltpu.VMEM((heads, HEAD_DIM, HEAD_DIM), F32),
            pltpu.VMEM((1, width), F32),
            pltpu.VMEM((heads, STATE_ROWS, HEAD_DIM), BF16),
            pltpu.VMEM((n - 1, heads, STATE_ROWS, HEAD_DIM), BF16),
            pltpu.VMEM((pairs, 2 * rows, model), BF16),
            pltpu.VMEM((pairs, rows, model), BF16),
            pltpu.VMEM((pairs - 1, rows, model), BF16),
            pltpu.VMEM((pairs - 1, rows, model), BF16),
            dma((5,)),
            dma((count,)),
            dma((count,)),
            dma((m - 1,)),
            dma((m - 1,)),
            dma((m - 1,)),
            dma((m - 1,)),
            dma((n - 1,)),
            dma((n - 1,)),
            dma((pairs,)),
            dma((pairs,)),
            dma((pairs - 1,)),
            dma((pairs - 1,)),
        ],
        compiler_params=pltpu.CompilerParams(
            collective_id=0, has_side_effects=True, vmem_limit_bytes=63_000_000
        ),
    )(
        skip,
        query,
        forget,
        value,
        emission,
        slack.reshape(1, width),
        surge,
        gain.reshape(1, width),
        projection,
        row_gain.reshape(1, model),
        switch,
        expansion,
        contraction,
    )


def paired_kernel(
    n,
    m,
    skip_ref,
    query_in,
    forget_in,
    value_in,
    emission_in,
    slack_ref,
    surge_in,
    gain_ref,
    projection_ref,
    row_gain_ref,
    switch_ref,
    expansion_ref,
    contraction_ref,
    out_ref,
    switch_half,
    expansion_half,
    contraction_half,
    projection,
    stream,
    normed,
    hidden,
    mixed,
    outputs,
    decayed_query,
    state,
    offset,
    state_out,
    state_in,
    chain_out,
    chain_in,
    part,
    from_buddy,
    cross_out,
    cross_in,
    plane_out,
    plane_in,
    local_sem,
    weight_send,
    weight_recv,
    skip_sem,
    state_sem,
    chain_send,
    chain_recv,
    mixed_send,
    mixed_recv,
    normed_send,
    normed_recv,
    buddy_send,
    buddy_recv,
    cross_send,
    cross_recv,
    plane_send,
    plane_recv,
    first_send,
    first_recv,
    result,
    result_sem,
    query_ref,
    forget_ref,
    value_ref,
    emission_ref,
    surge_ref,
    input_sem,
):
    sp, tp = lax.axis_index("sp"), lax.axis_index("tp")
    tokens, width = query_ref.shape
    rows, model = skip_ref.shape
    depth, units = switch_ref.shape
    heads = width // HEAD_DIM
    few = units // 256 * 128
    many = units - few
    z, y = sp // 2, lax.rem(sp, 2)
    x, core = tp // 2, lax.rem(tp, 2)
    planes = {0: z, 1: z + 1 - 2 * lax.rem(z, 2), 2: lax.rem(z + 2, 4), 3: 3 - z}
    outer = (z == 0) | (z == 3)
    beside = (z * 2 + 1 - y, tp)
    across = (sp, (1 - x) * 2 + core)
    buddy = (sp, x * 2 + 1 - core)
    paired = (planes[1] * 2 + y, tp)

    first_rows = tokens // 4
    inputs = [(query_in, query_ref), (forget_in, forget_ref), (surge_in, surge_ref), (value_in, value_ref)]
    opening, rest = [], []
    for index, (source, place) in enumerate(inputs):
        span = pl.ds(0, first_rows)
        opening.append(pltpu.make_async_copy(source.at[span], place.at[span], input_sem.at[index]))
        span = pl.ds(first_rows, tokens - first_rows)
        rest.append(pltpu.make_async_copy(source.at[span], place.at[span], input_sem.at[4 + index]))
    rest.append(pltpu.make_async_copy(emission_in, emission_ref, input_sem.at[8]))
    for copy in opening + rest:
        copy.start()

    barrier = pltpu.get_barrier_semaphore()
    for d in range(1, n):
        pl.semaphore_signal(barrier, inc=1, device_id=(lax.rem(sp + d, n), tp), device_id_type=MESH)
    for d in range(1, m):
        pl.semaphore_signal(barrier, inc=1, device_id=(sp, lax.rem(tp + d, m)), device_id_type=MESH)
    def remote(src, dst, send, recv, device):
        return pltpu.make_async_remote_copy(
            src_ref=src, dst_ref=dst, send_sem=send, recv_sem=recv, device_id=device, device_id_type=MESH
        )

    sends = []

    def start(copy):
        copy.start()
        sends.append(copy)

    def by_kind(action):
        pl.when(outer)(lambda: action(False))
        pl.when(jnp.logical_not(outer))(lambda: action(True))

    def own(tensor, big):
        span = pl.ds(few, many) if big else pl.ds(0, few)
        if tensor == 2:
            return contraction_ref.at[span]
        return (switch_ref, expansion_ref)[tensor].at[:, span]

    def held(tensor, owner, big):
        span = pl.ds(0, many if big else few)
        if tensor == 2:
            return contraction_half.at[owner, span]
        place = pl.ds(pl.multiple_of(owner * depth, depth), depth)
        return (switch_half, expansion_half)[tensor].at[place, span]

    def weight(tensor, kind, big):
        sems = (weight_send.at[tensor * 8 + kind], weight_recv.at[tensor * 8 + kind])
        if kind == 0:
            return remote(own(tensor, big), held(tensor, sp, big), *sems, beside)
        if kind <= 3:
            wanted = big if kind == 3 else not big
            return remote(own(tensor, wanted), held(tensor, sp, wanted), *sems, (planes[kind] * 2 + y, tp))
        unit = held(tensor, planes[1 if kind == 7 else kind - 3] * 2 + y, big)
        if kind == 7:
            return remote(unit, unit, sems[0], weight_recv.at[tensor * 8 + 2], (planes[3] * 2 + y, tp))
        return remote(unit, unit, *sems, beside)

    def weight_arrival(tensor, kind, big):
        sems = (weight_send.at[tensor * 8 + kind], weight_recv.at[tensor * 8 + kind])
        if kind == 0:
            owner = z * 2 + 1 - y
        elif kind <= 3:
            owner = planes[kind] * 2 + y
        else:
            owner = planes[kind - 3] * 2 + 1 - y
        unit = held(tensor, owner, big)
        return remote(unit, unit, *sems, beside)

    def local_weight(tensor, big):
        return pltpu.make_async_copy(own(tensor, big), held(tensor, sp, big), local_sem.at[2 + tensor])

    def send_weights(*pairs):
        def action(big):
            for tensor, kind in pairs:
                if big or kind != 2:
                    weight(tensor, kind, big).start()

        by_kind(action)

    def await_weights(*pairs):
        def action(big):
            for tensor, kind in pairs:
                weight_arrival(tensor, kind, big).wait_recv()

        by_kind(action)

    def relay(tensor, kind):
        def action(big):
            weight_arrival(tensor, kind, big).wait_recv()
            weight(tensor, kind + 3, big).start()

        by_kind(action)

    local = [
        pltpu.make_async_copy(skip_ref, stream.at[0], local_sem.at[0]),
        pltpu.make_async_copy(projection_ref, projection, local_sem.at[1]),
    ]
    for copy in local:
        copy.start()

    def prepare(big):
        for tensor in range(3):
            local_weight(tensor, big).start()
        if not big and many > few:
            switch_half[:, few:] = jnp.zeros((model, many - few), BF16)
            expansion_half[:, few:] = jnp.zeros((model, many - few), BF16)
            for owner in range(n):
                contraction_half[owner, few:, :] = jnp.zeros((many - few, depth), BF16)

    by_kind(prepare)

    state[...] = jnp.zeros_like(state)
    offset[...] = jnp.zeros_like(offset)
    before = lax.broadcasted_iota(jnp.int32, (BLOCK, BLOCK), 0) >= lax.broadcasted_iota(
        jnp.int32, (BLOCK, BLOCK), 1
    )
    lower = before.astype(F32)

    def recur(block):
        here = pl.ds(pl.multiple_of(block * BLOCK, BLOCK), BLOCK)
        raw = query_ref[here, :].astype(F32)
        query = raw * jax.nn.sigmoid(raw)
        gate = slack_ref[...] * jax.nn.sigmoid(-forget_ref[here, :].astype(F32))
        log_forget = jnp.log1p(-gate) + surge_ref[here, :]
        total = jnp.dot(lower, log_forget, precision=lax.Precision.HIGHEST, preferred_element_type=F32)
        middle, last = total[BLOCK // 2 : BLOCK // 2 + 1, :], total[BLOCK - 1 :, :]
        left = (query * jnp.exp(total - middle)).astype(BF16)
        right = (gate * jnp.exp(middle - total)).astype(BF16)
        carried = (query * jnp.exp(total)).astype(BF16)
        kept = (gate * jnp.exp(last - total)).astype(BF16)
        decayed_query[here, :] = (query * jnp.exp(total + offset[...])).astype(BF16)
        closing = jnp.exp(last)
        for head in range(heads):
            lanes = slice(head * HEAD_DIM, (head + 1) * HEAD_DIM)
            value = value_ref[here, lanes]
            scores = lax.dot_general(left[:, lanes], right[:, lanes], LAST, preferred_element_type=F32)
            scores = jnp.where(before, scores, 0.0).astype(BF16)
            kept_state = state[head]
            outputs[here, lanes] = jnp.dot(
                scores, value, preferred_element_type=F32
            ) + lax.dot_general(carried[:, lanes], kept_state.astype(BF16), LAST, preferred_element_type=F32)
            state[head] = closing[:, lanes] * kept_state + lax.dot_general(
                value, kept[:, lanes], FIRST, preferred_element_type=F32
            )
        offset[...] += last

    blocks = tokens // BLOCK
    early = blocks // 4
    for copy in opening:
        copy.wait()
    pl.loop(0, early)(recur)
    pl.semaphore_wait(barrier, n - 1 + m - 1)
    send_weights((0, 0))
    pl.when(z == 0)(lambda: send_weights((0, 3)))
    send_weights((0, 1))
    pl.when(z > 0)(lambda: send_weights((0, 3)))

    @pl.when(z > 1)
    def _():
        send_weights((0, 2))

    @pl.when(z == 3)
    def _():
        send_weights((1, 1), (1, 3))

    start(remote(skip_ref, stream.at[1], skip_sem.at[0], skip_sem.at[1], across))
    for copy in rest:
        copy.wait()
    pl.loop(early, blocks)(recur)

    for head in range(heads):
        lanes = slice(head * HEAD_DIM, (head + 1) * HEAD_DIM)
        state_out[head, :HEAD_DIM, :] = state[head].astype(BF16)
        decay = jnp.exp(offset[:, lanes])
        state_out[head, HEAD_DIM:, :] = jnp.broadcast_to(decay, (16, HEAD_DIM)).astype(BF16)
    exchange = remote(state_out, state_in, state_sem.at[0], state_sem.at[1], beside)
    start(exchange)
    def chain(distance):
        sems = (chain_send.at[distance - 1], chain_recv.at[distance - 1])
        return remote(chain_out, chain_in.at[distance - 1], *sems, ((z + distance) * 2 + y, tp))

    exchange.wait_recv()
    for head in range(heads):
        lanes = slice(head * HEAD_DIM, (head + 1) * HEAD_DIM)
        decay = jnp.exp(offset[:, lanes])
        other = state_in[head, :HEAD_DIM, :].astype(F32)
        other_decay = state_in[head, HEAD_DIM : HEAD_DIM + 1, :].astype(F32)
        later = jnp.where(y == 0, other, state[head])
        earlier = jnp.where(y == 0, state[head], other)
        later_decay = jnp.where(y == 0, other_decay, decay)
        chain_out[head, :HEAD_DIM, :] = (later_decay * earlier + later).astype(BF16)
        chain_out[head, HEAD_DIM:, :] = jnp.broadcast_to(decay * other_decay, (16, HEAD_DIM)).astype(BF16)
    for distance in range(1, 4):
        pl.when(z + distance < 4)(chain(distance).start)

    def forward(tensor):
        pl.when(jnp.logical_not(outer))(lambda: weight(tensor, 7, True).start())

    pl.when(z == 0)(lambda: send_weights((1, 1), (1, 3)))

    @pl.when((z == 1) | (z == 2))
    def _():
        pl.when(z == 1)(lambda: send_weights((0, 2)))
        send_weights((1, 1))

    send_weights((1, 0))
    for distance in range(1, 4):
        pl.when(z >= distance)(chain(distance).wait_recv)
    for head in range(heads):
        state[head] = jnp.zeros((HEAD_DIM, HEAD_DIM), F32)
        for distance in range(3, 0, -1):

            @pl.when(z >= distance)
            def _():
                item = chain_in[distance - 1, head].astype(F32)
                state[head] = item[HEAD_DIM : HEAD_DIM + 1, :] * state[head] + item[:HEAD_DIM, :]

        @pl.when(y == 1)
        def _():
            item = state_in[head].astype(F32)
            state[head] = item[HEAD_DIM : HEAD_DIM + 1, :] * state[head] + item[:HEAD_DIM, :]

    def mixed_copy(slot, source, block, kind, device):
        place = mixed.at[source, block]
        index = kind * 2 + slot
        return remote(place, place, mixed_send.at[index], mixed_recv.at[index], device)

    for j in range(2):
        side = 1 - x if j else x
        for r in range(2):
            target = 1 - core if r else core
            block = side * 2 + target
            here = pl.ds(pl.multiple_of(block * rows, rows), rows)
            for head in range(heads):
                lanes = slice(head * HEAD_DIM, (head + 1) * HEAD_DIM)
                full = outputs[here, lanes] + lax.dot_general(
                    decayed_query[here, lanes], state[head].astype(BF16), LAST, preferred_element_type=F32
                )
                squares = jnp.mean(full * full, axis=-1, keepdims=True)
                raw = emission_ref[here, lanes].astype(F32)
                scaled = full * lax.rsqrt(squares + EPSILON) * gain_ref[:, lanes]
                mixed[tp, block, :, lanes] = (scaled * (raw * jax.nn.sigmoid(raw))).astype(BF16)
            start(mixed_copy(1 - j, tp, block, r, (sp, (1 - x) * 2 + target)))
            if r:
                start(mixed_copy(j, tp, block, 2, buddy))

    relay(0, 1)
    forward(0)
    pl.when(jnp.logical_not(outer))(lambda: send_weights((1, 3)))
    relay(0, 3)

    @pl.when(jnp.logical_not(outer))
    def _():
        relay(1, 1)
        forward(1)
        send_weights((1, 2))

    for copy in local:
        copy.wait()
    remote(stream.at[1], stream.at[1], skip_sem.at[0], skip_sem.at[1], across).wait_recv()

    pieces = 4
    fine = rows // pieces

    def place_of(plane, side, which):
        return (which * 4 + plane * 2 + side) * rows

    def normed_rows(plane, side, which, piece):
        first, count = place_of(plane, side, which), rows
        if piece is not None:
            first, count = first + piece * fine, fine
        return normed.at[pl.ds(pl.multiple_of(first, fine), count)]

    def normed_copy(index, device, plane, side, which, piece=None, target=None):
        return remote(
            normed_rows(plane, side, which, piece),
            normed_rows(plane if target is None else target, side, which, piece),
            normed_send.at[index],
            normed_recv.at[index],
            device,
        )

    for j in range(2):
        side = 1 - x if j else x
        block = side * 2 + core
        mixed_copy(j, (1 - x) * 2 + core, block, 0, across).wait_recv()
        mixed_copy(j, (1 - x) * 2 + 1 - core, block, 1, across).wait_recv()
        mixed_copy(j, x * 2 + 1 - core, block, 2, across).wait_recv()
        first = place_of(0, side, core)
        for piece in range(2):
            here = slice(piece * rows // 2, (piece + 1) * rows // 2)
            total = stream[j, here, :].astype(F32)
            for source in range(m):
                total += jnp.dot(
                    mixed[source, block, here, :],
                    projection[source * width : (source + 1) * width, :],
                    preferred_element_type=F32,
                )
            rounded = total.astype(BF16)
            stream[j, here, :] = rounded
            total = rounded.astype(F32)
            squares = jnp.mean(total * total, axis=-1, keepdims=True)
            normed[pl.ds(pl.multiple_of(first + piece * rows // 2, rows // 2), rows // 2), :] = (
                total * lax.rsqrt(squares + EPSILON) * row_gain_ref[...]
            ).astype(BF16)
            if j == 0:
                for part_of in range(piece * pieces // 2, (piece + 1) * pieces // 2):
                    start(normed_copy(2 + part_of, paired, 0, side, core, part_of, 1))
        start(normed_copy(j, buddy, 0, side, core))

    pl.when(outer)(lambda: relay(1, 1))
    pl.when(jnp.logical_not(outer))(lambda: send_weights((2, 3)))
    relay(0, 2)

    def tiles(plane, action, side=None):
        count = rows if side is not None else 2 * rows
        first = plane * 2 * rows + (0 if side is None else side * rows)

        @pl.loop(0, 2)
        def _(which):
            here = pl.ds(pl.multiple_of(which * 4 * rows + first, rows), count)

            @pl.loop(0, many // 256)
            def _(turn):
                action(here, pl.ds(pl.multiple_of(turn * 256, 256), 256))

            if many % 256:
                action(here, slice(many // 256 * 256, many))

    def gate(here, lanes):
        value = jnp.dot(normed[here, :], switch_half[:, lanes], preferred_element_type=F32)
        hidden[here, lanes] = (value * jax.nn.sigmoid(value)).astype(BF16)

    def up(here, lanes):
        value = jnp.dot(normed[here, :], expansion_half[:, lanes], preferred_element_type=F32)
        hidden[here, lanes] = (hidden[here, lanes].astype(F32) * value).astype(BF16)

    def normed_arrives(index, plane, side, which, piece=None):
        normed_copy(index, buddy, plane, side, which, piece).wait_recv()

    def pass_on(piece):
        normed_arrives(2 + piece, 1, x, core, piece)
        start(normed_copy(6 + piece, across, 1, x, core, piece))
        start(normed_copy(10 + piece, buddy, 1, x, core, piece))

    def await_local(big):
        for tensor in range(3):
            local_weight(tensor, big).wait()

    by_kind(await_local)
    pass_on(0)
    relay(1, 3)
    pass_on(1)
    for j in range(2):
        normed_arrives(j, 0, 1 - x if j else x, 1 - core)
    await_weights((0, 0), (0, 4), (0, 6), (0, 5))
    tiles(0, gate)
    pass_on(2)
    pl.when(z < 3)(lambda: relay(1, 2))
    pass_on(3)
    pl.when(z == 3)(lambda: relay(1, 2))
    send_weights((2, 1), (2, 0))
    pl.when(outer)(lambda: send_weights((2, 3)))
    send_weights((2, 2))
    for piece in range(pieces):
        normed_arrives(10 + piece, 1, x, 1 - core, piece)
    tiles(1, gate, x)
    base = z // 2

    def owner_of(turn):
        far, second = turn // 4, lax.rem(turn, 4) // 2
        pair = base + far * (1 - 2 * base)
        plane = 1 + pair + (1 - lax.rem(far + second, 2)) * (2 * pair - 1)
        return plane * 2 + y + lax.rem(turn, 2) * (1 - 2 * y)

    mine = pl.multiple_of(core * 4 * rows, 4 * rows)
    theirs = pl.multiple_of((1 - core) * 4 * rows, 4 * rows)

    def buddy_copy(turn):
        return remote(
            part.at[turn, pl.ds(theirs, 4 * rows)],
            from_buddy.at[turn],
            buddy_send.at[turn],
            buddy_recv.at[turn],
            buddy,
        )

    def partner(odd):
        return (sp + (paired[0] - sp) * odd, across[1] + (tp - across[1]) * odd)

    def cross_copy(turn, which):
        sems = (cross_send.at[turn * 2 + which], cross_recv.at[turn * 2 + which])
        return remote(cross_out.at[turn, which], cross_in.at[turn, which], *sems, partner(lax.rem(turn, 2)))

    def plane_copy(turn):
        sems = (plane_send.at[turn], plane_recv.at[turn])
        return remote(plane_out.at[turn], plane_in.at[turn], *sems, partner(1 - lax.rem(turn, 2)))

    def share(turn, plane, side):
        place = (plane * 2 + side) * rows
        local_part = part[turn, pl.ds(pl.multiple_of(mine + place, rows), rows), :].astype(F32)
        return local_part + from_buddy[turn, pl.ds(pl.multiple_of(place, rows), rows), :].astype(F32)

    def result_copy(turn):
        lanes = pl.ds(pl.multiple_of(owner_of(turn) * depth, depth), depth)
        return pltpu.make_async_copy(result.at[turn], out_ref.at[:, lanes], result_sem.at[turn])

    def down(turn, tile):
        here = pl.ds(pl.multiple_of(tile * 2 * rows, 2 * rows), 2 * rows)
        unit = contraction_half.at[owner_of(turn)]
        part[turn, here, :] = jnp.dot(hidden[here, :], unit[...], preferred_element_type=F32).astype(BF16)

    def first_buddy(plane):
        place = pl.multiple_of((1 - core) * 4 * rows + plane * 2 * rows, 2 * rows)
        return remote(
            part.at[0, pl.ds(place, 2 * rows)],
            from_buddy.at[0, pl.ds(plane * 2 * rows, 2 * rows)],
            first_send.at[plane],
            first_recv.at[plane],
            buddy,
        )

    def first_cross(plane):
        sems = (first_send.at[2 + plane], first_recv.at[2 + plane])
        return remote(cross_out.at[0, plane], cross_in.at[0, plane], *sems, across)

    def open_first(plane):
        @pl.loop(0, 2)
        def _(which):
            down(0, which * 2 + plane)

        first_buddy(plane).start()

    def close_first(plane):
        first_buddy(plane).wait_recv()
        cross_out[0, plane] = share(0, plane, 1 - x).astype(BF16)
        first_cross(plane).start()

    def collect():
        for piece in range(pieces):
            normed_arrives(6 + piece, 1, 1 - x, core, piece)
            normed_copy(14 + piece, buddy, 1, 1 - x, core, piece).start()

    def collected():
        for piece in range(pieces):
            normed_arrives(14 + piece, 1, 1 - x, 1 - core, piece)

    @pl.when(z == 3)
    def _():
        collect()
        collected()
        tiles(1, gate, 1 - x)
        await_weights((1, 0), (1, 4), (1, 6), (1, 5))
        tiles(0, up)
        open_first(0)
        tiles(1, up, x)
        close_first(0)
        tiles(1, up, 1 - x)

    @pl.when(z < 3)
    def _():
        await_weights((1, 0), (1, 4), (1, 6), (1, 5))
        tiles(0, up)
        collect()
        tiles(1, up, x)

        @pl.when(z > 0)
        def _():
            relay(2, 1)
            weight(2, 7, True).start()
            relay(2, 3)

        open_first(0)
        collected()
        tiles(1, gate, 1 - x)
        close_first(0)
        tiles(1, up, 1 - x)

    lag_cross, lag_plane = 2, 4

    open_first(1)

    @pl.loop(1, n + lag_plane)
    def _(step):
        pl.when(step == 1)(lambda: close_first(1))

        @pl.when((step >= 2) & (step < n + 1))
        def _():
            turn = step - 1
            buddy_copy(turn).wait_recv()
            odd = lax.rem(turn, 2)
            cross_out[turn, 1] = share(turn, 1, 1 - x).astype(BF16)
            cross_copy(turn, 1).start()
            cross_out[turn, 0] = share(turn, odd, 1 - x + (2 * x - 1) * odd).astype(BF16)
            cross_copy(turn, 0).start()

        def ready(at, outer_needs, inner_needs):
            def action(big):
                for kind in inner_needs if big else outer_needs:
                    if kind in (1, 2, 3):
                        weight_arrival(2, kind, big).wait_recv()
                        weight(2, kind + 3, big).start()
                    else:
                        weight_arrival(2, kind, big).wait_recv()

            pl.when(step == at)(lambda: by_kind(action))

        ready(1, (0, 1), (4,))
        ready(2, (2,), ())
        ready(3, (4, 3), (0, 2))
        ready(5, (5,), (6,))
        ready(7, (6,), (5,))

        @pl.when(step < n)
        def _():
            @pl.loop(0, 4)
            def _(tile):
                down(step, tile)

            buddy_copy(step).start()

        @pl.when((step >= lag_cross) & (step < n + lag_cross))
        def _():
            turn = step - lag_cross

            pl.when(turn == 0)(lambda: first_cross(1).wait_recv())
            pl.when(turn > 0)(lambda: cross_copy(turn, 1).wait_recv())
            odd = lax.rem(turn, 2)
            total = share(turn, 1 - odd, x + (1 - 2 * x) * odd) + cross_in[turn, 1].astype(F32)
            plane_out[turn] = total.astype(BF16)
            plane_copy(turn).start()

        @pl.when(step >= lag_plane)
        def _():
            turn = step - lag_plane
            pl.when(turn == 0)(lambda: first_cross(0).wait_recv())
            pl.when(turn > 0)(lambda: cross_copy(turn, 0).wait_recv())
            plane_copy(turn).wait_recv()
            lanes = pl.ds(pl.multiple_of(owner_of(turn) * depth, depth), depth)
            total = stream[0, :, lanes].astype(F32) + share(turn, 0, x)
            total += cross_in[turn, 0].astype(F32) + plane_in[turn].astype(F32)
            result[turn] = total.astype(BF16)
            result_copy(turn).start()

    @pl.loop(0, n)
    def _(turn):
        @pl.when(turn > 0)
        def _():
            buddy_copy(turn).wait_send()
            cross_copy(turn, 0).wait_send()
            cross_copy(turn, 1).wait_send()

        plane_copy(turn).wait_send()
        result_copy(turn).wait()

    for plane in range(2):
        first_buddy(plane).wait_send()
        first_cross(plane).wait_send()

    for copy in sends:
        copy.wait_send()
    for piece in range(pieces):
        normed_copy(14 + piece, buddy, 1, 1 - x, core, piece).wait_send()

    def await_weight_sends(big):
        for tensor in range(3):
            for kind in range(8) if big else (0, 1, 3, 4, 5, 6):
                weight(tensor, kind, big).wait_send()

    by_kind(await_weight_sends)
    for distance in range(1, 4):
        pl.when(z + distance < 4)(chain(distance).wait_send)


def on_device_paired(n, m, *arrays):
    (skip, query, forget, value, emission, slack, surge, gain, projection, row_gain, switch, expansion, contraction) = arrays
    tokens, width = query.shape
    rows, model = skip.shape
    depth, units = switch.shape
    heads = width // HEAD_DIM
    many = units - units // 256 * 128
    vmem, anywhere = pl.BlockSpec(memory_space=pltpu.VMEM), pl.BlockSpec(memory_space=pl.ANY)
    dma = pltpu.SemaphoreType.DMA
    return pl.pallas_call(
        functools.partial(paired_kernel, n, m),
        out_shape=jax.ShapeDtypeStruct((rows, model), BF16),
        in_specs=[anywhere] * 5 + [vmem, anywhere, vmem] + [anywhere, vmem] + [anywhere] * 3,
        out_specs=anywhere,
        scratch_shapes=[
            pltpu.VMEM((model, many), BF16),
            pltpu.VMEM((model, many), BF16),
            pltpu.VMEM((n, many, depth), BF16),
            pltpu.VMEM(projection.shape, BF16),
            pltpu.VMEM((2, rows, model), BF16),
            pltpu.VMEM((2 * tokens, model), BF16),
            pltpu.VMEM((2 * tokens, many), BF16),
            pltpu.VMEM((m, m, rows, width), BF16),
            pltpu.VMEM((tokens, width), F32),
            pltpu.VMEM((tokens, width), BF16),
            pltpu.VMEM((heads, HEAD_DIM, HEAD_DIM), F32),
            pltpu.VMEM((1, width), F32),
            pltpu.VMEM((heads, STATE_ROWS, HEAD_DIM), BF16),
            pltpu.VMEM((heads, STATE_ROWS, HEAD_DIM), BF16),
            pltpu.VMEM((heads, STATE_ROWS, HEAD_DIM), BF16),
            pltpu.VMEM((3, heads, STATE_ROWS, HEAD_DIM), BF16),
            pltpu.VMEM((n, 2 * tokens, depth), BF16),
            pltpu.VMEM((n, tokens, depth), BF16),
            pltpu.VMEM((n, 2, rows, depth), BF16),
            pltpu.VMEM((n, 2, rows, depth), BF16),
            pltpu.VMEM((n, rows, depth), BF16),
            pltpu.VMEM((n, rows, depth), BF16),
            dma((5,)),
            dma((24,)),
            dma((24,)),
            dma((2,)),
            dma((2,)),
            dma((3,)),
            dma((3,)),
            dma((6,)),
            dma((6,)),
            dma((18,)),
            dma((18,)),
            dma((n,)),
            dma((n,)),
            dma((2 * n,)),
            dma((2 * n,)),
            dma((n,)),
            dma((n,)),
            dma((4,)),
            dma((4,)),
            pltpu.VMEM((n, rows, depth), BF16),
            dma((n,)),
            pltpu.VMEM((tokens, width), BF16),
            pltpu.VMEM((tokens, width), BF16),
            pltpu.VMEM((tokens, width), BF16),
            pltpu.VMEM((tokens, width), BF16),
            pltpu.VMEM((tokens, width), F32),
            dma((9,)),
        ],
        compiler_params=pltpu.CompilerParams(
            collective_id=0, has_side_effects=True, vmem_limit_bytes=64_000_000
        ),
    )(
        skip,
        query,
        forget,
        value,
        emission,
        slack.reshape(1, width),
        surge,
        gain.reshape(1, width),
        projection,
        row_gain.reshape(1, model),
        switch,
        expansion,
        contraction,
    )


def solution(mesh):
    in_specs = (
        P(("sp", "tp"), None),
        P("sp", "tp"),
        P("sp", "tp"),
        P("sp", "tp"),
        P("sp", "tp"),
        P("tp"),
        P("sp", "tp"),
        P("tp"),
        P(),
        P(),
        P("sp", "tp"),
        P("sp", "tp"),
        P("tp", "sp"),
    )
    n, m = mesh.shape["sp"], mesh.shape["tp"]
    return jax.shard_map(
        functools.partial(on_device_paired if (n, m) == (8, 4) else on_device, n, m),
        mesh=mesh,
        in_specs=in_specs,
        out_specs=P(("sp", "tp"), None),
        check_vma=False,
    )
```

```python
import functools

import jax
import jax.numpy as jnp
from jax import lax
from jax.experimental import pallas as pl
from jax.experimental.pallas import tpu as pltpu
from jax.sharding import PartitionSpec as P

HEAD_DIM = 128
BLOCK = 64
STATE_ROWS = HEAD_DIM + 16
EPSILON = 1e-06
MESH = pl.DeviceIdType.MESH
F32, BF16 = jnp.float32, jnp.bfloat16
LAST = (((1,), (1,)), ((), ()))
FIRST = (((0,), (0,)), ((), ()))


def weight_plan(n, me):
    out = []
    if n != 8:
        for tensor in range(3):
            for d in range(1, n):
                to, source = lax.rem(me + d, n), lax.rem(me + n - d, n)
                out.append((0, tensor, ("D", d, tensor), True, me, to, True, source, None))
        return out
    ny, nz = 2, n // 2
    z, y = me // ny, lax.rem(me, ny)

    def at(place, flip):
        return jnp.clip(place, 0, nz - 1) * ny + (1 - y if flip else y)

    def crossed(place, tensor, way):
        first, last = (1, nz - 1) if way > 0 else (nz - 2, 0)
        return (place == first) | (place == last) if tensor == 0 else place == first

    def inside(place):
        return (place >= 0) & (place < nz)

    for tensor in range(3):
        late = 1 if tensor == 2 else 0
        out.append((0, tensor, ("Y", 0, tensor), True, me, at(z, 1), True, at(z, 1), None))
        for way in (1, -1):
            for k in range(1, nz):
                to, unit = z + way, z + way - way * k
                name, above = (way, k, tensor), (way, k - 1, tensor)
                stage = 0 if k == 1 else k - 1 + late
                out.append(
                    (stage, tensor, name, inside(to) & inside(unit), at(unit, 0), at(to, 0),
                     inside(z - way * k), at(z - way * k, 0), None if k == 1 else above)
                )
                held = inside(z - way * k)
                if k == 1:
                    held = held & jnp.logical_not(crossed(z, tensor, way))
                out.append(
                    (k + late, tensor, ("Y", way * k, tensor), held, at(z - way * k, 0), at(z, 1),
                     held, at(z - way * k, 1), name)
                )
            out.append(
                (2, tensor, ("X", way, tensor), inside(z + way) & crossed(z + way, tensor, way), at(z, 1),
                 at(z + way, 0), crossed(z, tensor, way), at(z - way, 1), ("Y", 0, tensor))
            )
    return out


def kernel(
    n,
    m,
    skip_ref,
    query_ref,
    forget_ref,
    value_ref,
    emission_ref,
    slack_ref,
    surge_ref,
    gain_ref,
    projection_ref,
    row_gain_ref,
    switch_ref,
    expansion_ref,
    contraction_ref,
    out_ref,
    switch_all,
    expansion_all,
    contraction_all,
    projection,
    stream,
    normed,
    hidden,
    mixed,
    outputs,
    decayed_query,
    state,
    offset,
    state_out,
    state_in,
    part,
    from_buddy,
    cross_out,
    cross_in,
    local_sem,
    weight_send,
    weight_recv,
    skip_send,
    skip_recv,
    mixed_send,
    mixed_recv,
    state_send,
    state_recv,
    buddy_send,
    buddy_recv,
    cross_send,
    cross_recv,
):
    sp, tp = lax.axis_index("sp"), lax.axis_index("tp")
    tokens, width = query_ref.shape
    rows, model = skip_ref.shape
    depth, units = switch_ref.shape
    heads = width // HEAD_DIM
    pairs = m // 2

    barrier = pltpu.get_barrier_semaphore()
    for d in range(1, n):
        pl.semaphore_signal(barrier, inc=1, device_id=(lax.rem(sp + d, n), tp), device_id_type=MESH)
    for d in range(1, m):
        pl.semaphore_signal(barrier, inc=1, device_id=(sp, lax.rem(tp + d, m)), device_id_type=MESH)
    pl.semaphore_wait(barrier, n - 1 + m - 1)

    def remote(src, dst, send, recv, device):
        return pltpu.make_async_remote_copy(
            src_ref=src, dst_ref=dst, send_sem=send, recv_sem=recv, device_id=device, device_id_type=MESH
        )

    own_units = (switch_ref, expansion_ref, contraction_ref)

    def unit(tensor, owner):
        if tensor == 2:
            return contraction_all.at[owner]
        held = (switch_all, expansion_all)[tensor]
        return held.at[pl.ds(pl.multiple_of(owner * depth, depth), depth)]

    messages = {}
    for index, (stage, tensor, name, sent, owner, target, arrives, arriving, after) in enumerate(
        weight_plan(n, sp)
    ):
        src = own_units[tensor] if stage == 0 else unit(tensor, owner)
        args = (weight_send.at[index], weight_recv.at[index], (target, tp))
        send = remote(src, unit(tensor, owner), *args)
        arrival = remote(unit(tensor, arriving), unit(tensor, arriving), *args)
        messages[name] = (stage, sent, send, arrives, arrival, after)
    arrived = set()

    def where(condition, action):
        if condition is True:
            action()
        else:
            pl.when(condition)(action)

    def await_unit(name):
        if name not in arrived:
            arrived.add(name)
            where(messages[name][3], messages[name][4].wait_recv)

    def run_stage(wanted):
        for name, (stage, sent, send, _, _, after) in messages.items():
            if stage == wanted:
                if after is not None:
                    await_unit(after)
                where(sent, send.start)

    run_stage(0)

    def rows_of(owner):
        return pl.ds(pl.multiple_of(owner * rows, rows), rows)

    skip_sends, skip_arrivals, mixed_sends, mixed_arrivals = [], [], [], []
    for d in range(1, m):
        source, target = lax.rem(tp + m - d, m), (sp, lax.rem(tp + d, m))
        sems = (skip_send.at[d - 1], skip_recv.at[d - 1], target)
        skip_sends.append(remote(skip_ref, stream.at[rows_of(tp)], *sems))
        skip_arrivals.append(remote(stream.at[rows_of(source)], stream.at[rows_of(source)], *sems))
        sems = (mixed_send.at[d - 1], mixed_recv.at[d - 1], target)
        mixed_sends.append(remote(mixed.at[tp], mixed.at[tp], *sems))
        mixed_arrivals.append(remote(mixed.at[source], mixed.at[source], *sems))
    for copy in skip_sends:
        copy.start()
    local = [
        pltpu.make_async_copy(skip_ref, stream.at[rows_of(tp)], local_sem.at[0]),
        pltpu.make_async_copy(projection_ref, projection, local_sem.at[1]),
    ] + [pltpu.make_async_copy(own_units[t], unit(t, sp), local_sem.at[2 + t]) for t in range(3)]
    for copy in local:
        copy.start()

    state[...] = jnp.zeros_like(state)
    offset[...] = jnp.zeros_like(offset)
    before = lax.broadcasted_iota(jnp.int32, (BLOCK, BLOCK), 0) >= lax.broadcasted_iota(
        jnp.int32, (BLOCK, BLOCK), 1
    )
    lower = before.astype(F32)

    @pl.loop(0, tokens // BLOCK)
    def _(block):
        here = pl.ds(pl.multiple_of(block * BLOCK, BLOCK), BLOCK)
        raw = query_ref[here, :].astype(F32)
        query = raw * jax.nn.sigmoid(raw)
        gate = slack_ref[...] * jax.nn.sigmoid(-forget_ref[here, :].astype(F32))
        log_forget = jnp.log1p(-gate) + surge_ref[here, :]
        total = jnp.dot(lower, log_forget, precision=lax.Precision.HIGHEST, preferred_element_type=F32)
        middle, last = total[BLOCK // 2 : BLOCK // 2 + 1, :], total[BLOCK - 1 :, :]
        left = (query * jnp.exp(total - middle)).astype(BF16)
        right = (gate * jnp.exp(middle - total)).astype(BF16)
        carried = (query * jnp.exp(total)).astype(BF16)
        kept = (gate * jnp.exp(last - total)).astype(BF16)
        decayed_query[here, :] = (query * jnp.exp(total + offset[...])).astype(BF16)
        closing = jnp.exp(last)
        for head in range(heads):
            lanes = slice(head * HEAD_DIM, (head + 1) * HEAD_DIM)
            value = value_ref[here, lanes]
            scores = lax.dot_general(left[:, lanes], right[:, lanes], LAST, preferred_element_type=F32)
            scores = jnp.where(before, scores, 0.0).astype(BF16)
            held = state[head]
            outputs[here, lanes] = jnp.dot(
                scores, value, preferred_element_type=F32
            ) + lax.dot_general(carried[:, lanes], held.astype(BF16), LAST, preferred_element_type=F32)
            state[head] = closing[:, lanes] * held + lax.dot_general(
                value, kept[:, lanes], FIRST, preferred_element_type=F32
            )
        offset[...] += last

    for head in range(heads):
        lanes = slice(head * HEAD_DIM, (head + 1) * HEAD_DIM)
        state_out[head, :HEAD_DIM, :] = state[head].astype(BF16)
        decay = jnp.exp(offset[:, lanes])
        state_out[head, HEAD_DIM:, :] = jnp.broadcast_to(decay, (16, HEAD_DIM)).astype(BF16)
    state_copies = []
    for d in range(1, n):
        copy = remote(
            state_out,
            state_in.at[d - 1],
            state_send.at[d - 1],
            state_recv.at[d - 1],
            (lax.rem(sp + d, n), tp),
        )
        state_copies.append(copy)
        pl.when(sp + d < n)(copy.start)

    run_stage(1)

    for d in range(1, n):
        pl.when(sp >= d)(state_copies[d - 1].wait_recv)
    state[...] = jnp.zeros_like(state)

    @pl.loop(0, sp)
    def _(earlier):
        slot = sp - earlier - 1
        for head in range(heads):
            item = state_in[slot, head].astype(F32)
            state[head] = item[HEAD_DIM : HEAD_DIM + 1, :] * state[head] + item[:HEAD_DIM, :]

    tile = min(256, tokens)

    @pl.loop(0, tokens // tile)
    def _(turn):
        here = pl.ds(pl.multiple_of(turn * tile, tile), tile)
        for head in range(heads):
            lanes = slice(head * HEAD_DIM, (head + 1) * HEAD_DIM)
            full = outputs[here, lanes] + lax.dot_general(
                decayed_query[here, lanes], state[head].astype(BF16), LAST, preferred_element_type=F32
            )
            squares = jnp.mean(full * full, axis=-1, keepdims=True)
            raw = emission_ref[here, lanes].astype(F32)
            scaled = full * lax.rsqrt(squares + EPSILON) * gain_ref[:, lanes]
            mixed[tp, here, lanes] = (scaled * (raw * jax.nn.sigmoid(raw))).astype(BF16)

    for copy in mixed_sends:
        copy.start()
    run_stage(2)
    for copy in local:
        copy.wait()
    for copy in skip_arrivals:
        copy.wait_recv()
    for copy in mixed_arrivals:
        copy.wait_recv()

    @pl.loop(0, tokens // tile)
    def _(turn):
        here = pl.ds(pl.multiple_of(turn * tile, tile), tile)
        total = stream[here, :].astype(F32)
        for source in range(m):
            total += jnp.dot(
                mixed[source, here, :],
                projection[source * width : (source + 1) * width, :],
                preferred_element_type=F32,
            )
        rounded = total.astype(BF16)
        stream[here, :] = rounded
        total = rounded.astype(F32)
        squares = jnp.mean(total * total, axis=-1, keepdims=True)
        normed[here, :] = (total * lax.rsqrt(squares + EPSILON) * row_gain_ref[...]).astype(BF16)

    run_stage(3)
    for name in messages:
        if name[2] < 2:
            await_unit(name)

    core, pair = lax.rem(tp, 2), tp // 2
    buddy = (sp, pair * 2 + 1 - core)

    def half(number, which):
        return part.at[number, pl.ds(pl.multiple_of(which * rows, rows), rows)]

    def gate_and_up(number, owner):
        inputs = pl.ds(pl.multiple_of(owner * 2 * rows, 2 * rows), 2 * rows)

        def columns(lanes):
            value = normed[inputs, :]
            gate = jnp.dot(value, switch_all[:, lanes], preferred_element_type=F32)
            up = jnp.dot(value, expansion_all[:, lanes], preferred_element_type=F32)
            hidden[number, :, lanes] = (gate * jax.nn.sigmoid(gate) * up).astype(BF16)

        @pl.loop(0, units // 256)
        def _(turn):
            columns(pl.ds(pl.multiple_of(turn * 256, 256), 256))

        if units % 256:
            columns(slice(units // 256 * 256, units))

    def down(number):
        @pl.loop(0, n)
        def _(turn):
            lanes = pl.ds(pl.multiple_of(turn * depth, depth), depth)
            part[number, :, lanes] = jnp.dot(
                hidden[number], contraction_all[turn], preferred_element_type=F32
            ).astype(BF16)

        copy = remote(
            half(number, 1 - core),
            from_buddy.at[number],
            buddy_send.at[number],
            buddy_recv.at[number],
            buddy,
        )
        copy.start()
        return copy

    for d in [*range(1, pairs), 0]:
        gate_and_up(d, lax.rem(pair + d, pairs))
    run_stage(4)
    for name in messages:
        await_unit(name)
    tail = []
    for d in range(1, pairs):
        owner = lax.rem(pair + d, pairs)
        copy = down(d)
        copy.wait_recv()
        cross_out[d - 1] = (half(d, core)[...].astype(F32) + from_buddy[d].astype(F32)).astype(BF16)
        cross = remote(
            cross_out.at[d - 1],
            cross_in.at[d - 1],
            cross_send.at[d - 1],
            cross_recv.at[d - 1],
            (sp, owner * 2 + core),
        )
        cross.start()
        tail += [copy, cross]
    copy = down(0)
    copy.wait_recv()
    total = half(0, core)[...].astype(F32) + from_buddy[0].astype(F32) + stream[rows_of(tp), :].astype(F32)
    for d in range(1, pairs):
        tail[2 * d - 1].wait_recv()
        total += cross_in[d - 1].astype(F32)
    out_ref[...] = total.astype(BF16)

    for copy in tail + [copy] + skip_sends + mixed_sends:
        copy.wait_send()
    for _, sent, send, _, _, _ in messages.values():
        where(sent, send.wait_send)
    for d in range(1, n):
        pl.when(sp + d < n)(state_copies[d - 1].wait_send)


def on_device(n, m, *arrays):
    (skip, query, forget, value, emission, slack, surge, gain, projection, row_gain, switch, expansion, contraction) = arrays
    tokens, width = query.shape
    rows, model = skip.shape
    depth, units = switch.shape
    heads, pairs = width // HEAD_DIM, m // 2
    count = 3 * (3 * n // 2 + 3) if n == 8 else 3 * (n - 1)
    vmem, anywhere = pl.BlockSpec(memory_space=pltpu.VMEM), pl.BlockSpec(memory_space=pl.ANY)
    dma = pltpu.SemaphoreType.DMA
    return pl.pallas_call(
        functools.partial(kernel, n, m),
        out_shape=jax.ShapeDtypeStruct((rows, model), BF16),
        in_specs=[anywhere] + [vmem] * 7 + [anywhere, vmem] + [anywhere] * 3,
        out_specs=vmem,
        scratch_shapes=[
            pltpu.VMEM((model, units), BF16),
            pltpu.VMEM((model, units), BF16),
            pltpu.VMEM((n, units, depth), BF16),
            pltpu.VMEM(projection.shape, BF16),
            pltpu.VMEM((tokens, model), BF16),
            pltpu.VMEM((tokens, model), BF16),
            pltpu.VMEM((pairs, 2 * rows, units), BF16),
            pltpu.VMEM((m, tokens, width), BF16),
            pltpu.VMEM((tokens, width), F32),
            pltpu.VMEM((tokens, width), BF16),
            pltpu.VMEM((heads, HEAD_DIM, HEAD_DIM), F32),
            pltpu.VMEM((1, width), F32),
            pltpu.VMEM((heads, STATE_ROWS, HEAD_DIM), BF16),
            pltpu.VMEM((n - 1, heads, STATE_ROWS, HEAD_DIM), BF16),
            pltpu.VMEM((pairs, 2 * rows, model), BF16),
            pltpu.VMEM((pairs, rows, model), BF16),
            pltpu.VMEM((pairs - 1, rows, model), BF16),
            pltpu.VMEM((pairs - 1, rows, model), BF16),
            dma((5,)),
            dma((count,)),
            dma((count,)),
            dma((m - 1,)),
            dma((m - 1,)),
            dma((m - 1,)),
            dma((m - 1,)),
            dma((n - 1,)),
            dma((n - 1,)),
            dma((pairs,)),
            dma((pairs,)),
            dma((pairs - 1,)),
            dma((pairs - 1,)),
        ],
        compiler_params=pltpu.CompilerParams(
            collective_id=0, has_side_effects=True, vmem_limit_bytes=63_000_000
        ),
    )(
        skip,
        query,
        forget,
        value,
        emission,
        slack.reshape(1, width),
        surge,
        gain.reshape(1, width),
        projection,
        row_gain.reshape(1, model),
        switch,
        expansion,
        contraction,
    )


def paired_kernel(
    n,
    m,
    skip_ref,
    query_in,
    forget_in,
    value_in,
    emission_in,
    slack_ref,
    surge_in,
    gain_ref,
    projection_ref,
    row_gain_ref,
    switch_ref,
    expansion_ref,
    contraction_ref,
    out_ref,
    switch_half,
    expansion_half,
    contraction_half,
    projection,
    stream,
    normed,
    hidden,
    mixed,
    outputs,
    decayed_query,
    state,
    offset,
    state_out,
    state_in,
    chain_out,
    chain_in,
    part,
    from_buddy,
    cross_out,
    cross_in,
    plane_out,
    plane_in,
    local_sem,
    weight_send,
    weight_recv,
    skip_sem,
    state_sem,
    chain_send,
    chain_recv,
    mixed_send,
    mixed_recv,
    normed_send,
    normed_recv,
    buddy_send,
    buddy_recv,
    cross_send,
    cross_recv,
    plane_send,
    plane_recv,
    first_send,
    first_recv,
    result,
    result_sem,
    query_ref,
    forget_ref,
    value_ref,
    emission_ref,
    surge_ref,
    input_sem,
):
    sp, tp = lax.axis_index("sp"), lax.axis_index("tp")
    tokens, width = query_ref.shape
    rows, model = skip_ref.shape
    depth, units = switch_ref.shape
    heads = width // HEAD_DIM
    few = units // 256 * 128
    many = units - few
    z, y = sp // 2, lax.rem(sp, 2)
    x, core = tp // 2, lax.rem(tp, 2)
    planes = {0: z, 1: z + 1 - 2 * lax.rem(z, 2), 2: lax.rem(z + 2, 4), 3: 3 - z}
    outer = (z == 0) | (z == 3)
    beside = (z * 2 + 1 - y, tp)
    across = (sp, (1 - x) * 2 + core)
    buddy = (sp, x * 2 + 1 - core)
    paired = (planes[1] * 2 + y, tp)

    first_rows = tokens // 4
    inputs = [(query_in, query_ref), (forget_in, forget_ref), (surge_in, surge_ref), (value_in, value_ref)]
    opening, rest = [], []
    for index, (source, place) in enumerate(inputs):
        span = pl.ds(0, first_rows)
        opening.append(pltpu.make_async_copy(source.at[span], place.at[span], input_sem.at[index]))
        span = pl.ds(first_rows, tokens - first_rows)
        rest.append(pltpu.make_async_copy(source.at[span], place.at[span], input_sem.at[4 + index]))
    rest.append(pltpu.make_async_copy(emission_in, emission_ref, input_sem.at[8]))
    for copy in opening + rest:
        copy.start()

    barrier = pltpu.get_barrier_semaphore()
    for d in range(1, n):
        pl.semaphore_signal(barrier, inc=1, device_id=(lax.rem(sp + d, n), tp), device_id_type=MESH)
    for d in range(1, m):
        pl.semaphore_signal(barrier, inc=1, device_id=(sp, lax.rem(tp + d, m)), device_id_type=MESH)
    def remote(src, dst, send, recv, device):
        return pltpu.make_async_remote_copy(
            src_ref=src, dst_ref=dst, send_sem=send, recv_sem=recv, device_id=device, device_id_type=MESH
        )

    sends = []

    def start(copy):
        copy.start()
        sends.append(copy)

    def by_kind(action):
        pl.when(outer)(lambda: action(False))
        pl.when(jnp.logical_not(outer))(lambda: action(True))

    def own(tensor, big):
        span = pl.ds(few, many) if big else pl.ds(0, few)
        if tensor == 2:
            return contraction_ref.at[span]
        return (switch_ref, expansion_ref)[tensor].at[:, span]

    def held(tensor, owner, big):
        span = pl.ds(0, many if big else few)
        if tensor == 2:
            return contraction_half.at[owner, span]
        place = pl.ds(pl.multiple_of(owner * depth, depth), depth)
        return (switch_half, expansion_half)[tensor].at[place, span]

    def weight(tensor, kind, big):
        sems = (weight_send.at[tensor * 8 + kind], weight_recv.at[tensor * 8 + kind])
        if kind == 0:
            return remote(own(tensor, big), held(tensor, sp, big), *sems, beside)
        if kind <= 3:
            wanted = big if kind == 3 else not big
            return remote(own(tensor, wanted), held(tensor, sp, wanted), *sems, (planes[kind] * 2 + y, tp))
        unit = held(tensor, planes[1 if kind == 7 else kind - 3] * 2 + y, big)
        if kind == 7:
            return remote(unit, unit, sems[0], weight_recv.at[tensor * 8 + 2], (planes[3] * 2 + y, tp))
        return remote(unit, unit, *sems, beside)

    def weight_arrival(tensor, kind, big):
        sems = (weight_send.at[tensor * 8 + kind], weight_recv.at[tensor * 8 + kind])
        if kind == 0:
            owner = z * 2 + 1 - y
        elif kind <= 3:
            owner = planes[kind] * 2 + y
        else:
            owner = planes[kind - 3] * 2 + 1 - y
        unit = held(tensor, owner, big)
        return remote(unit, unit, *sems, beside)

    def local_weight(tensor, big):
        return pltpu.make_async_copy(own(tensor, big), held(tensor, sp, big), local_sem.at[2 + tensor])

    def send_weights(*pairs):
        def action(big):
            for tensor, kind in pairs:
                if big or kind != 2:
                    weight(tensor, kind, big).start()

        by_kind(action)

    def await_weights(*pairs):
        def action(big):
            for tensor, kind in pairs:
                weight_arrival(tensor, kind, big).wait_recv()

        by_kind(action)

    def relay(tensor, kind):
        def action(big):
            weight_arrival(tensor, kind, big).wait_recv()
            weight(tensor, kind + 3, big).start()

        by_kind(action)

    local = [
        pltpu.make_async_copy(skip_ref, stream.at[0], local_sem.at[0]),
        pltpu.make_async_copy(projection_ref, projection, local_sem.at[1]),
    ]
    for copy in local:
        copy.start()

    def prepare(big):
        for tensor in range(3):
            local_weight(tensor, big).start()
        if not big and many > few:
            switch_half[:, few:] = jnp.zeros((model, many - few), BF16)
            expansion_half[:, few:] = jnp.zeros((model, many - few), BF16)
            for owner in range(n):
                contraction_half[owner, few:, :] = jnp.zeros((many - few, depth), BF16)

    by_kind(prepare)

    state[...] = jnp.zeros_like(state)
    offset[...] = jnp.zeros_like(offset)
    before = lax.broadcasted_iota(jnp.int32, (BLOCK, BLOCK), 0) >= lax.broadcasted_iota(
        jnp.int32, (BLOCK, BLOCK), 1
    )
    lower = before.astype(F32)

    def recur(block):
        here = pl.ds(pl.multiple_of(block * BLOCK, BLOCK), BLOCK)
        raw = query_ref[here, :].astype(F32)
        query = raw * jax.nn.sigmoid(raw)
        gate = slack_ref[...] * jax.nn.sigmoid(-forget_ref[here, :].astype(F32))
        log_forget = jnp.log1p(-gate) + surge_ref[here, :]
        total = jnp.dot(lower, log_forget, precision=lax.Precision.HIGHEST, preferred_element_type=F32)
        middle, last = total[BLOCK // 2 : BLOCK // 2 + 1, :], total[BLOCK - 1 :, :]
        left = (query * jnp.exp(total - middle)).astype(BF16)
        right = (gate * jnp.exp(middle - total)).astype(BF16)
        carried = (query * jnp.exp(total)).astype(BF16)
        kept = (gate * jnp.exp(last - total)).astype(BF16)
        decayed_query[here, :] = (query * jnp.exp(total + offset[...])).astype(BF16)
        closing = jnp.exp(last)
        for head in range(heads):
            lanes = slice(head * HEAD_DIM, (head + 1) * HEAD_DIM)
            value = value_ref[here, lanes]
            scores = lax.dot_general(left[:, lanes], right[:, lanes], LAST, preferred_element_type=F32)
            scores = jnp.where(before, scores, 0.0).astype(BF16)
            kept_state = state[head]
            outputs[here, lanes] = jnp.dot(
                scores, value, preferred_element_type=F32
            ) + lax.dot_general(carried[:, lanes], kept_state.astype(BF16), LAST, preferred_element_type=F32)
            state[head] = closing[:, lanes] * kept_state + lax.dot_general(
                value, kept[:, lanes], FIRST, preferred_element_type=F32
            )
        offset[...] += last

    blocks = tokens // BLOCK
    early = blocks // 4
    for copy in opening:
        copy.wait()
    pl.loop(0, early)(recur)
    pl.semaphore_wait(barrier, n - 1 + m - 1)
    send_weights((0, 0))
    pl.when(z == 0)(lambda: send_weights((0, 3)))
    send_weights((0, 1))
    pl.when(z > 0)(lambda: send_weights((0, 3)))

    @pl.when(z > 1)
    def _():
        send_weights((0, 2))

    @pl.when(z == 3)
    def _():
        send_weights((1, 1), (1, 3))

    start(remote(skip_ref, stream.at[1], skip_sem.at[0], skip_sem.at[1], across))
    for copy in rest:
        copy.wait()
    pl.loop(early, blocks)(recur)

    for head in range(heads):
        lanes = slice(head * HEAD_DIM, (head + 1) * HEAD_DIM)
        state_out[head, :HEAD_DIM, :] = state[head].astype(BF16)
        decay = jnp.exp(offset[:, lanes])
        state_out[head, HEAD_DIM:, :] = jnp.broadcast_to(decay, (16, HEAD_DIM)).astype(BF16)
    exchange = remote(state_out, state_in, state_sem.at[0], state_sem.at[1], beside)
    start(exchange)
    def chain(distance):
        sems = (chain_send.at[distance - 1], chain_recv.at[distance - 1])
        return remote(chain_out, chain_in.at[distance - 1], *sems, ((z + distance) * 2 + y, tp))

    exchange.wait_recv()
    for head in range(heads):
        lanes = slice(head * HEAD_DIM, (head + 1) * HEAD_DIM)
        decay = jnp.exp(offset[:, lanes])
        other = state_in[head, :HEAD_DIM, :].astype(F32)
        other_decay = state_in[head, HEAD_DIM : HEAD_DIM + 1, :].astype(F32)
        later = jnp.where(y == 0, other, state[head])
        earlier = jnp.where(y == 0, state[head], other)
        later_decay = jnp.where(y == 0, other_decay, decay)
        chain_out[head, :HEAD_DIM, :] = (later_decay * earlier + later).astype(BF16)
        chain_out[head, HEAD_DIM:, :] = jnp.broadcast_to(decay * other_decay, (16, HEAD_DIM)).astype(BF16)
    for distance in range(1, 4):
        pl.when(z + distance < 4)(chain(distance).start)

    def forward(tensor):
        pl.when(jnp.logical_not(outer))(lambda: weight(tensor, 7, True).start())

    pl.when(z == 0)(lambda: send_weights((1, 1), (1, 3)))

    @pl.when((z == 1) | (z == 2))
    def _():
        pl.when(z == 1)(lambda: send_weights((0, 2)))
        send_weights((1, 1))

    send_weights((1, 0))
    for distance in range(1, 4):
        pl.when(z >= distance)(chain(distance).wait_recv)
    for head in range(heads):
        state[head] = jnp.zeros((HEAD_DIM, HEAD_DIM), F32)
        for distance in range(3, 0, -1):

            @pl.when(z >= distance)
            def _():
                item = chain_in[distance - 1, head].astype(F32)
                state[head] = item[HEAD_DIM : HEAD_DIM + 1, :] * state[head] + item[:HEAD_DIM, :]

        @pl.when(y == 1)
        def _():
            item = state_in[head].astype(F32)
            state[head] = item[HEAD_DIM : HEAD_DIM + 1, :] * state[head] + item[:HEAD_DIM, :]

    def mixed_copy(slot, source, block, kind, device):
        place = mixed.at[source, block]
        index = kind * 2 + slot
        return remote(place, place, mixed_send.at[index], mixed_recv.at[index], device)

    for j in range(2):
        side = 1 - x if j else x
        for r in range(2):
            target = 1 - core if r else core
            block = side * 2 + target
            here = pl.ds(pl.multiple_of(block * rows, rows), rows)
            for head in range(heads):
                lanes = slice(head * HEAD_DIM, (head + 1) * HEAD_DIM)
                full = outputs[here, lanes] + lax.dot_general(
                    decayed_query[here, lanes], state[head].astype(BF16), LAST, preferred_element_type=F32
                )
                squares = jnp.mean(full * full, axis=-1, keepdims=True)
                raw = emission_ref[here, lanes].astype(F32)
                scaled = full * lax.rsqrt(squares + EPSILON) * gain_ref[:, lanes]
                mixed[tp, block, :, lanes] = (scaled * (raw * jax.nn.sigmoid(raw))).astype(BF16)
            start(mixed_copy(1 - j, tp, block, r, (sp, (1 - x) * 2 + target)))
            if r:
                start(mixed_copy(j, tp, block, 2, buddy))

    relay(0, 1)
    forward(0)
    pl.when(jnp.logical_not(outer))(lambda: send_weights((1, 3)))
    relay(0, 3)

    @pl.when(jnp.logical_not(outer))
    def _():
        relay(1, 1)
        forward(1)
        send_weights((1, 2))

    for copy in local:
        copy.wait()
    remote(stream.at[1], stream.at[1], skip_sem.at[0], skip_sem.at[1], across).wait_recv()

    pieces = 4
    fine = rows // pieces

    def place_of(plane, side, which):
        return (which * 4 + plane * 2 + side) * rows

    def normed_rows(plane, side, which, piece):
        first, count = place_of(plane, side, which), rows
        if piece is not None:
            first, count = first + piece * fine, fine
        return normed.at[pl.ds(pl.multiple_of(first, fine), count)]

    def normed_copy(index, device, plane, side, which, piece=None, target=None):
        return remote(
            normed_rows(plane, side, which, piece),
            normed_rows(plane if target is None else target, side, which, piece),
            normed_send.at[index],
            normed_recv.at[index],
            device,
        )

    for j in range(2):
        side = 1 - x if j else x
        block = side * 2 + core
        mixed_copy(j, (1 - x) * 2 + core, block, 0, across).wait_recv()
        mixed_copy(j, (1 - x) * 2 + 1 - core, block, 1, across).wait_recv()
        mixed_copy(j, x * 2 + 1 - core, block, 2, across).wait_recv()
        first = place_of(0, side, core)
        for piece in range(2):
            here = slice(piece * rows // 2, (piece + 1) * rows // 2)
            total = stream[j, here, :].astype(F32)
            for source in range(m):
                total += jnp.dot(
                    mixed[source, block, here, :],
                    projection[source * width : (source + 1) * width, :],
                    preferred_element_type=F32,
                )
            rounded = total.astype(BF16)
            stream[j, here, :] = rounded
            total = rounded.astype(F32)
            squares = jnp.mean(total * total, axis=-1, keepdims=True)
            normed[pl.ds(pl.multiple_of(first + piece * rows // 2, rows // 2), rows // 2), :] = (
                total * lax.rsqrt(squares + EPSILON) * row_gain_ref[...]
            ).astype(BF16)
            if j == 0:
                for part_of in range(piece * pieces // 2, (piece + 1) * pieces // 2):
                    start(normed_copy(2 + part_of, paired, 0, side, core, part_of, 1))
        start(normed_copy(j, buddy, 0, side, core))

    pl.when(outer)(lambda: relay(1, 1))
    pl.when(jnp.logical_not(outer))(lambda: send_weights((2, 3)))
    relay(0, 2)

    def tiles(plane, action, side=None):
        count = rows if side is not None else 2 * rows
        first = plane * 2 * rows + (0 if side is None else side * rows)

        @pl.loop(0, 2)
        def _(which):
            here = pl.ds(pl.multiple_of(which * 4 * rows + first, rows), count)

            @pl.loop(0, many // 256)
            def _(turn):
                action(here, pl.ds(pl.multiple_of(turn * 256, 256), 256))

            if many % 256:
                action(here, slice(many // 256 * 256, many))

    def gate(here, lanes):
        value = jnp.dot(normed[here, :], switch_half[:, lanes], preferred_element_type=F32)
        hidden[here, lanes] = (value * jax.nn.sigmoid(value)).astype(BF16)

    def up(here, lanes):
        value = jnp.dot(normed[here, :], expansion_half[:, lanes], preferred_element_type=F32)
        hidden[here, lanes] = (hidden[here, lanes].astype(F32) * value).astype(BF16)

    def normed_arrives(index, plane, side, which, piece=None):
        normed_copy(index, buddy, plane, side, which, piece).wait_recv()

    def pass_on(piece):
        normed_arrives(2 + piece, 1, x, core, piece)
        start(normed_copy(6 + piece, across, 1, x, core, piece))
        start(normed_copy(10 + piece, buddy, 1, x, core, piece))

    def await_local(big):
        for tensor in range(3):
            local_weight(tensor, big).wait()

    by_kind(await_local)
    pass_on(0)
    relay(1, 3)
    pass_on(1)
    for j in range(2):
        normed_arrives(j, 0, 1 - x if j else x, 1 - core)
    await_weights((0, 0), (0, 4), (0, 6), (0, 5))
    tiles(0, gate)
    pass_on(2)
    pl.when(z < 3)(lambda: relay(1, 2))
    pass_on(3)
    pl.when(z == 3)(lambda: relay(1, 2))
    send_weights((2, 1), (2, 0))
    for piece in range(pieces):
        normed_arrives(10 + piece, 1, x, 1 - core, piece)
    tiles(1, gate, x)
    pl.when(outer)(lambda: send_weights((2, 3)))
    send_weights((2, 2))
    base = z // 2

    def owner_of(turn):
        far, second = turn // 4, lax.rem(turn, 4) // 2
        pair = base + far * (1 - 2 * base)
        plane = 1 + pair + (1 - lax.rem(far + second, 2)) * (2 * pair - 1)
        return plane * 2 + y + lax.rem(turn, 2) * (1 - 2 * y)

    mine = pl.multiple_of(core * 4 * rows, 4 * rows)
    theirs = pl.multiple_of((1 - core) * 4 * rows, 4 * rows)

    def buddy_copy(turn):
        return remote(
            part.at[turn, pl.ds(theirs, 4 * rows)],
            from_buddy.at[turn],
            buddy_send.at[turn],
            buddy_recv.at[turn],
            buddy,
        )

    def partner(odd):
        return (sp + (paired[0] - sp) * odd, across[1] + (tp - across[1]) * odd)

    def cross_copy(turn, which):
        sems = (cross_send.at[turn * 2 + which], cross_recv.at[turn * 2 + which])
        return remote(cross_out.at[turn, which], cross_in.at[turn, which], *sems, partner(lax.rem(turn, 2)))

    def plane_copy(turn):
        sems = (plane_send.at[turn], plane_recv.at[turn])
        return remote(plane_out.at[turn], plane_in.at[turn], *sems, partner(1 - lax.rem(turn, 2)))

    def share(turn, plane, side):
        place = (plane * 2 + side) * rows
        local_part = part[turn, pl.ds(pl.multiple_of(mine + place, rows), rows), :].astype(F32)
        return local_part + from_buddy[turn, pl.ds(pl.multiple_of(place, rows), rows), :].astype(F32)

    def result_copy(turn):
        lanes = pl.ds(pl.multiple_of(owner_of(turn) * depth, depth), depth)
        return pltpu.make_async_copy(result.at[turn], out_ref.at[:, lanes], result_sem.at[turn])

    def down(turn, tile):
        here = pl.ds(pl.multiple_of(tile * 2 * rows, 2 * rows), 2 * rows)
        unit = contraction_half.at[owner_of(turn)]
        part[turn, here, :] = jnp.dot(hidden[here, :], unit[...], preferred_element_type=F32).astype(BF16)

    def first_buddy(plane):
        place = pl.multiple_of((1 - core) * 4 * rows + plane * 2 * rows, 2 * rows)
        return remote(
            part.at[0, pl.ds(place, 2 * rows)],
            from_buddy.at[0, pl.ds(plane * 2 * rows, 2 * rows)],
            first_send.at[plane],
            first_recv.at[plane],
            buddy,
        )

    def first_cross(plane):
        sems = (first_send.at[2 + plane], first_recv.at[2 + plane])
        return remote(cross_out.at[0, plane], cross_in.at[0, plane], *sems, across)

    def open_first(plane):
        @pl.loop(0, 2)
        def _(which):
            down(0, which * 2 + plane)

        first_buddy(plane).start()

    def close_first(plane):
        first_buddy(plane).wait_recv()
        cross_out[0, plane] = share(0, plane, 1 - x).astype(BF16)
        first_cross(plane).start()

    def collect():
        for piece in range(pieces):
            normed_arrives(6 + piece, 1, 1 - x, core, piece)
            normed_copy(14 + piece, buddy, 1, 1 - x, core, piece).start()

    def collected():
        for piece in range(pieces):
            normed_arrives(14 + piece, 1, 1 - x, 1 - core, piece)

    @pl.when(z == 3)
    def _():
        collect()
        collected()
        tiles(1, gate, 1 - x)
        await_weights((1, 0), (1, 4), (1, 6), (1, 5))
        tiles(0, up)
        open_first(0)
        tiles(1, up, x)
        close_first(0)
        tiles(1, up, 1 - x)

    @pl.when(z < 3)
    def _():
        await_weights((1, 0), (1, 4), (1, 6), (1, 5))
        tiles(0, up)
        collect()
        tiles(1, up, x)

        @pl.when(z > 0)
        def _():
            relay(2, 1)
            weight(2, 7, True).start()
            relay(2, 3)

        open_first(0)
        collected()
        tiles(1, gate, 1 - x)
        close_first(0)
        tiles(1, up, 1 - x)

    lag_cross, lag_plane = 3, 5

    open_first(1)

    @pl.loop(1, n + lag_plane)
    def _(step):
        pl.when(step == 1)(lambda: close_first(1))

        @pl.when((step >= 2) & (step < n + 1))
        def _():
            turn = step - 1
            buddy_copy(turn).wait_recv()
            odd = lax.rem(turn, 2)
            cross_out[turn, 1] = share(turn, 1, 1 - x).astype(BF16)
            cross_copy(turn, 1).start()
            cross_out[turn, 0] = share(turn, odd, 1 - x + (2 * x - 1) * odd).astype(BF16)
            cross_copy(turn, 0).start()

        @pl.when((step >= lag_cross) & (step < n + lag_cross))
        def _():
            turn = step - lag_cross

            pl.when(turn == 0)(lambda: first_cross(1).wait_recv())
            pl.when(turn > 0)(lambda: cross_copy(turn, 1).wait_recv())
            odd = lax.rem(turn, 2)
            total = share(turn, 1 - odd, x + (1 - 2 * x) * odd) + cross_in[turn, 1].astype(F32)
            plane_out[turn] = total.astype(BF16)
            plane_copy(turn).start()

        def ready(at, outer_needs, inner_needs):
            def action(big):
                for kind in inner_needs if big else outer_needs:
                    if kind in (1, 2, 3):
                        weight_arrival(2, kind, big).wait_recv()
                        weight(2, kind + 3, big).start()
                    else:
                        weight_arrival(2, kind, big).wait_recv()

            pl.when(step == at)(lambda: by_kind(action))

        ready(1, (0, 1), (4,))
        ready(2, (2,), ())
        ready(3, (4, 3), (0, 2))
        ready(5, (5,), (6,))
        ready(7, (6,), (5,))

        @pl.when(step < n)
        def _():
            @pl.loop(0, 4)
            def _(tile):
                down(step, tile)

            buddy_copy(step).start()

        @pl.when(step >= lag_plane)
        def _():
            turn = step - lag_plane
            pl.when(turn == 0)(lambda: first_cross(0).wait_recv())
            pl.when(turn > 0)(lambda: cross_copy(turn, 0).wait_recv())
            plane_copy(turn).wait_recv()
            lanes = pl.ds(pl.multiple_of(owner_of(turn) * depth, depth), depth)
            total = stream[0, :, lanes].astype(F32) + share(turn, 0, x)
            total += cross_in[turn, 0].astype(F32) + plane_in[turn].astype(F32)
            result[turn] = total.astype(BF16)
            result_copy(turn).start()

    @pl.loop(0, n)
    def _(turn):
        @pl.when(turn > 0)
        def _():
            buddy_copy(turn).wait_send()
            cross_copy(turn, 0).wait_send()
            cross_copy(turn, 1).wait_send()

        plane_copy(turn).wait_send()
        result_copy(turn).wait()

    for plane in range(2):
        first_buddy(plane).wait_send()
        first_cross(plane).wait_send()

    for copy in sends:
        copy.wait_send()
    for piece in range(pieces):
        normed_copy(14 + piece, buddy, 1, 1 - x, core, piece).wait_send()

    def await_weight_sends(big):
        for tensor in range(3):
            for kind in range(8) if big else (0, 1, 3, 4, 5, 6):
                weight(tensor, kind, big).wait_send()

    by_kind(await_weight_sends)
    for distance in range(1, 4):
        pl.when(z + distance < 4)(chain(distance).wait_send)


def on_device_paired(n, m, *arrays):
    (skip, query, forget, value, emission, slack, surge, gain, projection, row_gain, switch, expansion, contraction) = arrays
    tokens, width = query.shape
    rows, model = skip.shape
    depth, units = switch.shape
    heads = width // HEAD_DIM
    many = units - units // 256 * 128
    vmem, anywhere = pl.BlockSpec(memory_space=pltpu.VMEM), pl.BlockSpec(memory_space=pl.ANY)
    dma = pltpu.SemaphoreType.DMA
    return pl.pallas_call(
        functools.partial(paired_kernel, n, m),
        out_shape=jax.ShapeDtypeStruct((rows, model), BF16),
        in_specs=[anywhere] * 5 + [vmem, anywhere, vmem] + [anywhere, vmem] + [anywhere] * 3,
        out_specs=anywhere,
        scratch_shapes=[
            pltpu.VMEM((model, many), BF16),
            pltpu.VMEM((model, many), BF16),
            pltpu.VMEM((n, many, depth), BF16),
            pltpu.VMEM(projection.shape, BF16),
            pltpu.VMEM((2, rows, model), BF16),
            pltpu.VMEM((2 * tokens, model), BF16),
            pltpu.VMEM((2 * tokens, many), BF16),
            pltpu.VMEM((m, m, rows, width), BF16),
            pltpu.VMEM((tokens, width), F32),
            pltpu.VMEM((tokens, width), BF16),
            pltpu.VMEM((heads, HEAD_DIM, HEAD_DIM), F32),
            pltpu.VMEM((1, width), F32),
            pltpu.VMEM((heads, STATE_ROWS, HEAD_DIM), BF16),
            pltpu.VMEM((heads, STATE_ROWS, HEAD_DIM), BF16),
            pltpu.VMEM((heads, STATE_ROWS, HEAD_DIM), BF16),
            pltpu.VMEM((3, heads, STATE_ROWS, HEAD_DIM), BF16),
            pltpu.VMEM((n, 2 * tokens, depth), BF16),
            pltpu.VMEM((n, tokens, depth), BF16),
            pltpu.VMEM((n, 2, rows, depth), BF16),
            pltpu.VMEM((n, 2, rows, depth), BF16),
            pltpu.VMEM((n, rows, depth), BF16),
            pltpu.VMEM((n, rows, depth), BF16),
            dma((5,)),
            dma((24,)),
            dma((24,)),
            dma((2,)),
            dma((2,)),
            dma((3,)),
            dma((3,)),
            dma((6,)),
            dma((6,)),
            dma((18,)),
            dma((18,)),
            dma((n,)),
            dma((n,)),
            dma((2 * n,)),
            dma((2 * n,)),
            dma((n,)),
            dma((n,)),
            dma((4,)),
            dma((4,)),
            pltpu.VMEM((n, rows, depth), BF16),
            dma((n,)),
            pltpu.VMEM((tokens, width), BF16),
            pltpu.VMEM((tokens, width), BF16),
            pltpu.VMEM((tokens, width), BF16),
            pltpu.VMEM((tokens, width), BF16),
            pltpu.VMEM((tokens, width), F32),
            dma((9,)),
        ],
        compiler_params=pltpu.CompilerParams(
            collective_id=0, has_side_effects=True, vmem_limit_bytes=64_000_000
        ),
    )(
        skip,
        query,
        forget,
        value,
        emission,
        slack.reshape(1, width),
        surge,
        gain.reshape(1, width),
        projection,
        row_gain.reshape(1, model),
        switch,
        expansion,
        contraction,
    )


def solution(mesh):
    in_specs = (
        P(("sp", "tp"), None),
        P("sp", "tp"),
        P("sp", "tp"),
        P("sp", "tp"),
        P("sp", "tp"),
        P("tp"),
        P("sp", "tp"),
        P("tp"),
        P(),
        P(),
        P("sp", "tp"),
        P("sp", "tp"),
        P("tp", "sp"),
    )
    n, m = mesh.shape["sp"], mesh.shape["tp"]
    return jax.shard_map(
        functools.partial(on_device_paired if (n, m) == (8, 4) else on_device, n, m),
        mesh=mesh,
        in_specs=in_specs,
        out_specs=P(("sp", "tp"), None),
        check_vma=False,
    )
```
